32 devices in a mesh: sp: 8 (over z, x), tp: 4 (over y, core).
Axes of the slice: x: 2, y: 2, z: 4, core: 2. Of those that a mesh axis runs over, the one named last changes fastest.
Arguments:
- latent: bfloat16 [2, 4096, 2048], P(None, ('sp', 'tp')), may hold values from -6 to 6
- context: bfloat16 [2, 512, 2048], P(None, 'sp'), may hold values from -6 to 6
- cond: bfloat16 [2, 2048], replicated, may hold values from -6 to 6
- ctx_cond: bfloat16 [2048], replicated, may hold values from -6 to 6
- w_shift: bfloat16 [2048, 2048], P('sp', 'tp'), may hold values from -0.125 to 0.125
- w_scale: bfloat16 [2048, 2048], P('sp', 'tp'), may hold values from -0.125 to 0.125
- w_gate: bfloat16 [2048, 2048], P('sp', 'tp'), may hold values from -0.125 to 0.125
- norm_gain: float32 [2048], replicated, may hold values from 0.1 to 1.9
- w_query: bfloat16 [2048, 2048], P(None, 'tp'), may hold values from -1.08275726 to 1.08275726
- w_key: bfloat16 [2048, 2048], P(None, 'tp'), may hold values from -0.090598056 to 0.090598056
- w_value: bfloat16 [2048, 2048], P(None, 'tp'), may hold values from -0.125 to 0.125
- w_out: bfloat16 [2048, 2048], P('tp'), may hold values from -1.5 to 1.5
- rel_bias: float32 [32, 15, 31], P('tp'), may hold values from -4 to 4
- ctx_bias: float32 [32], P('tp'), may hold values from -3.5 to -2
Outputs:
- mixed: bfloat16 [2, 4096, 2048], P(None, ('sp', 'tp'))
The draws below stay inside these ranges and needn't reach their ends.
All inputs are finite; a program needn't handle non-finite values.
Results may differ from the reference program's by a relative error of at most 0.0154.
Values may be sent and summed in bfloat16 or wider, within the bound.
A program may use at most 128 MiB of HBM per device.

```python
import jax
import jax.numpy as jnp
from jax import lax

D = 2048
HEADS = 32
HEAD_DIM = 64
GRID_W = 64
WIN_ROWS = 8
WIN_COLS = 16
SAMPLES = 2
ROWS = 64
TOKENS = 4096
CTX = 512
N_TP = 4


def shared_keys(key):
    base = jax.random.normal(jax.random.fold_in(key, 11), (D, D), jnp.float32)
    return jnp.clip(base, -4.0, 4.0) * D ** (-0.5)


def draw_w_key(key, part):
    return shared_keys(key).astype(jnp.bfloat16)


def draw_w_query(key, part):
    own = jax.random.normal(jax.random.fold_in(key, 12), (D, D), jnp.float32)
    own = jnp.clip(own, -4.0, 4.0) * D ** (-0.5)
    return own.astype(jnp.bfloat16)


def levels(own_key, extent, pieces, smallest, high):
    loudness, own = 1.0, jax.random.fold_in(own_key, 6)
    for axis_at, parts in pieces:
        steps = jnp.exp(jax.random.uniform(jax.random.fold_in(own, axis_at), (parts,), jnp.float32, smallest / len(pieces), high / len(pieces)))
        loudness = loudness * jnp.repeat(steps, extent[axis_at] // parts).reshape([-1 if axis == axis_at else 1 for axis in range(len(extent))])
    return loudness


def noise(stream_key, extent, width, limit, shards=(), kind=jnp.bfloat16):
    entries = jax.random.normal(stream_key, extent, jnp.float32) * width
    if len(shards) > 0:
        entries = levels(stream_key, extent, shards, -0.22, 0.18) * entries
    return jnp.clip(entries, min=-limit, max=limit).astype(kind)


def setup_inputs(seed: int = 0) -> dict:
    key_list = jax.random.split(jax.random.key(seed), 15)
    return {
        "latent": noise(key_list[0], (SAMPLES, TOKENS, D), 1.0, 6.0, ((1, 32),)),
        "context": noise(key_list[1], (SAMPLES, CTX, D), 1.0, 6.0, ((1, 8),)),
        "cond": noise(key_list[2], (SAMPLES, D), 1.0, 6.0),
        "ctx_cond": noise(key_list[3], (D,), 1.0, 6.0),
        "w_shift": noise(key_list[4], (D, D), D ** -0.5, 0.125, ((0, 8), (1, 4))),
        "w_scale": noise(key_list[5], (D, D), D ** -0.5, 0.125, ((0, 8), (1, 4))),
        "w_gate": noise(key_list[6], (D, D), D ** -0.5, 0.125, ((0, 8), (1, 4))),
        "norm_gain": jnp.clip(1.0 + 0.18 * jax.random.normal(key_list[7], (D,), jnp.float32), 0.1, 1.9),
        "w_query": draw_w_query(jax.random.fold_in(key_list[14], 71), 0),
        "w_key": draw_w_key(jax.random.fold_in(key_list[14], 71), 0),
        "w_value": noise(key_list[10], (D, D), D ** -0.5, 0.125, ((1, 4),)),
        "w_out": noise(key_list[11], (D, D), 16 ** -0.5, 1.5, ((0, 4),)),
        "rel_bias": noise(key_list[12], (HEADS, 2 * WIN_ROWS - 1, 2 * WIN_COLS - 1), 1.0, 4.0, ((0, 4),), jnp.float32),
        "ctx_bias": jnp.clip(-3.5 + 1.5 * jax.random.uniform(key_list[13], (HEADS,), jnp.float32) ** levels(key_list[13], (HEADS,), ((0, 4),), -0.2, 0.2), -3.5, -2.0),
    }


EPSILON = 1e-06

def modulate_rows(rows, gain, shift, scale):
    floats = rows.astype(jnp.float32)
    inverse = lax.rsqrt(lax.optimization_barrier(jnp.mean(floats * floats, axis=-1, keepdims=True)) + EPSILON)
    return (floats * inverse * gain * (1.0 + scale) + shift).astype(jnp.bfloat16)

def project(rows, weight):
    return jnp.dot(rows, weight, preferred_element_type=jnp.float32).astype(jnp.bfloat16)

def reference(latent, context, cond, ctx_cond, w_shift, w_scale, w_gate, norm_gain, w_query, w_key, w_value, w_out, rel_bias, ctx_bias):
    ada = jax.nn.silu(cond.astype(jnp.float32)).astype(jnp.bfloat16)
    ada_ctx = jax.nn.silu(ctx_cond.astype(jnp.float32)).astype(jnp.bfloat16)[None, :]
    shift = jnp.dot(ada, w_shift, preferred_element_type=jnp.float32)
    scale = jnp.dot(ada, w_scale, preferred_element_type=jnp.float32)
    gate = jnp.dot(ada, w_gate, preferred_element_type=jnp.float32)
    ctx_shift = jnp.dot(ada_ctx, w_shift, preferred_element_type=jnp.float32)[0]
    ctx_scale = jnp.dot(ada_ctx, w_scale, preferred_element_type=jnp.float32)[0]
    hidden = modulate_rows(latent, norm_gain, shift[:, None, :], scale[:, None, :])
    ctx_hidden = modulate_rows(context, norm_gain, ctx_shift, ctx_scale)
    query = project(hidden, w_query).reshape(SAMPLES, ROWS, GRID_W, HEADS, HEAD_DIM)
    key = project(hidden, w_key).reshape(SAMPLES, ROWS, GRID_W, HEADS, HEAD_DIM)
    value = project(hidden, w_value).reshape(SAMPLES, ROWS, GRID_W, HEADS, HEAD_DIM)
    ctx_key = project(ctx_hidden, w_key).reshape(SAMPLES, CTX, HEADS, HEAD_DIM).astype(jnp.float32)
    ctx_value = project(ctx_hidden, w_value).reshape(SAMPLES, CTX, HEADS, HEAD_DIM).astype(jnp.float32)
    factor = HEAD_DIM ** (-0.5)
    columns = jnp.arange(GRID_W, dtype=jnp.int32)
    col_start = jnp.clip(columns - WIN_COLS // 2, 0, GRID_W - WIN_COLS)
    col_mask = (columns[None, :] >= col_start[:, None]) & (columns[None, :] < col_start[:, None] + WIN_COLS)
    col_index = jnp.clip(columns[None, :] - columns[:, None] + WIN_COLS - 1, 0, 2 * WIN_COLS - 2)

    def one_row(row):
        first = jnp.clip(row - WIN_ROWS // 2, 0, ROWS - WIN_ROWS).astype(jnp.int32)
        query_row = lax.dynamic_index_in_dim(query, row, axis=1, keepdims=False).astype(jnp.float32)
        key_rows = lax.dynamic_slice_in_dim(key, first, WIN_ROWS, axis=1).astype(jnp.float32)
        value_rows = lax.dynamic_slice_in_dim(value, first, WIN_ROWS, axis=1).astype(jnp.float32)
        row_index = first + jnp.arange(WIN_ROWS, dtype=jnp.int32) - row + WIN_ROWS - 1
        bias = rel_bias[:, row_index][:, :, col_index]
        near = jnp.einsum('sqhd,siwhd->shqiw', query_row, key_rows) * factor + bias.transpose(0, 2, 1, 3)[None]
        near = jnp.where(col_mask[None, None, :, None, :], near, -jnp.inf).reshape(SAMPLES, HEADS, GRID_W, WIN_ROWS * GRID_W)
        far = jnp.einsum('sqhd,schd->shqc', query_row, ctx_key) * factor + ctx_bias[None, :, None, None]
        top = jnp.maximum(lax.optimization_barrier(jnp.max(near, axis=-1)), lax.optimization_barrier(jnp.max(far, axis=-1)))[..., None]
        near_exp = jnp.exp(near - top)
        far_exp = jnp.exp(far - top)
        total = lax.optimization_barrier(jnp.sum(near_exp, axis=-1, keepdims=True)) + lax.optimization_barrier(jnp.sum(far_exp, axis=-1, keepdims=True))
        near_weight = (near_exp / total).astype(jnp.bfloat16).astype(jnp.float32)
        far_weight = (far_exp / total).astype(jnp.bfloat16).astype(jnp.float32)
        near_weight = near_weight.reshape(SAMPLES, HEADS, GRID_W, WIN_ROWS, GRID_W)
        mixed = jnp.einsum('shqiw,siwhd->sqhd', near_weight, value_rows) + jnp.einsum('shqc,schd->sqhd', far_weight, ctx_value)
        return mixed.astype(jnp.bfloat16)
    attended = lax.map(one_row, jnp.arange(ROWS, dtype=jnp.int32))
    attended = attended.transpose(1, 0, 2, 3, 4).reshape(SAMPLES, TOKENS, D)
    group = D // N_TP
    update = jnp.zeros((SAMPLES, TOKENS, D), jnp.float32)
    for index in range(N_TP):
        part = jnp.dot(attended[..., index * group:(index + 1) * group], w_out[index * group:(index + 1) * group], preferred_element_type=jnp.float32).astype(jnp.bfloat16)
        part = lax.optimization_barrier(part)
        update = update + part.astype(jnp.float32)
    mixed_out = latent.astype(jnp.float32) + gate[:, None, :] * update
    return mixed_out.astype(jnp.bfloat16)
```

```python
import functools

import jax
import jax.numpy as jnp
from jax import lax
from jax.experimental import pallas as pl
from jax.experimental.pallas import tpu as pltpu
from jax.sharding import PartitionSpec as P

HEAD_DIM = 64
GRID_W = 64
WIN_ROWS = 8
WIN_COLS = 16


EPSILON = 1e-06


def extended(shard, sides, width):
    for axis, dim in sides:
        size, length = (lax.axis_size(axis), shard.shape[dim])
        up = [(i, (i + 1) % size) for i in range(size - 1)]
        down = [(j, i) for i, j in up]
        last = lax.slice_in_dim(shard, length - width, length, axis=dim)
        first = lax.slice_in_dim(shard, 0, width, axis=dim)
        before = lax.ppermute(last, axis, up)
        after = lax.ppermute(first, axis, down)
        shard = jnp.concatenate([before, shard, after], axis=dim)
    return shard


def silu_rows(values):
    return jax.nn.silu(values.astype(jnp.float32)).astype(jnp.bfloat16)


def modulate_rows(rows, gain, shift, scale):
    floats = rows.astype(jnp.float32)
    inverse = lax.rsqrt(jnp.mean(floats * floats, axis=-1, keepdims=True) + EPSILON)
    return (floats * inverse * gain * (1.0 + scale) + shift).astype(jnp.bfloat16)

LOG2E = 1.4426950408889634


def attention_kernel(bias_ref, far_ref, q_ref, k_ref, v_ref, ck_ref, cv_ref, out_ref, table):
    pair = pl.program_id(0)
    rows_dev = q_ref.shape[1]
    padded = k_ref.shape[1]
    span = 2 * WIN_COLS
    half = WIN_COLS // 2
    reach = WIN_ROWS // 2
    nq, nk = rows_dev * WIN_COLS, padded * span
    lanes = 2 * HEAD_DIM

    @pl.when(pl.program_id(1) == 0)
    def _():
        sp = lax.axis_index("sp")
        rows_all = rows_dev * lax.axis_size("sp")
        at = lax.broadcasted_iota(jnp.int32, (WIN_COLS, nk), 1)
        p = lax.broadcasted_iota(jnp.int32, (WIN_COLS, nk), 0)
        key_row = sp * rows_dev - reach + at // span
        k = at % span
        inner = (k - p >= 0) & (k - p < WIN_COLS)
        edge = (p < half) == (k < WIN_COLS)
        for r in range(rows_dev):
            row = sp * rows_dev + r
            first = jnp.clip(row - reach, 0, rows_all - WIN_ROWS)
            inside = (key_row >= first) & (key_row < first + WIN_ROWS)
            shift = span * (r + reach - WIN_ROWS + 1) - half + 1
            for h in range(2):
                line = jnp.broadcast_to(bias_ref[0, h : h + 1, :], (WIN_COLS, nk))
                line = pltpu.roll(line, shift % nk, 1, stride=1, stride_axis=0) * LOG2E
                at_rows = pl.ds(r * WIN_COLS, WIN_COLS)
                table[h, 0, at_rows, :] = jnp.where(inside & edge, line, -jnp.inf)
                table[h, 1, at_rows, :] = jnp.where(inside & inner, line, -jnp.inf)

    factor = HEAD_DIM ** (-0.5) * LOG2E
    ck = ck_ref[...].reshape(-1, lanes)
    ctx_count = ck.shape[0]
    cv = jnp.concatenate([cv_ref[...].reshape(-1, lanes), jnp.ones((ctx_count, lanes), jnp.bfloat16)], axis=1)
    ones = jnp.ones((nk, lanes), jnp.bfloat16)
    low = lax.broadcasted_iota(jnp.int32, (nq, lanes), 1) < HEAD_DIM
    contract = (((1,), (1,)), ((), ()))
    every = q_ref[0].astype(jnp.float32)
    outs = []
    for block in range(GRID_W // WIN_COLS):
        if block == 0:
            q = jnp.concatenate([every[:, GRID_W - half :], every[:, :half]], axis=1)
        else:
            q = every[:, WIN_COLS * block - half : WIN_COLS * (block + 1) - half]
        q = q.astype(jnp.bfloat16).reshape(nq, lanes)

        def keys(ref):
            if block == 0:
                got = jnp.concatenate([ref[0, :, GRID_W - WIN_COLS :, :], ref[0, :, :WIN_COLS, :]], 1)
            else:
                got = ref[0, :, WIN_COLS * (block - 1) : WIN_COLS * (block + 1), :]
            return got.reshape(nk, lanes)

        k = keys(k_ref)
        v = jnp.concatenate([keys(v_ref), ones], axis=1)
        halves = []
        for h in range(2):
            mine = low if h == 0 else jnp.logical_not(low)
            one = jnp.where(mine, q, jnp.zeros_like(q))
            near = lax.dot_general(one, k, contract, preferred_element_type=jnp.float32)
            near = near * factor + table[h, min(block, 1)]
            far = lax.dot_general(one, ck, contract, preferred_element_type=jnp.float32)
            far = far * factor + far_ref[2 * pair + h] * LOG2E
            top = jnp.maximum(
                jnp.max(near, axis=-1, keepdims=True), jnp.max(far, axis=-1, keepdims=True)
            )
            near = jnp.exp2(near - top).astype(jnp.bfloat16)
            far = jnp.exp2(far - top).astype(jnp.bfloat16)
            got = jnp.dot(near, v, preferred_element_type=jnp.float32) + jnp.dot(
                far, cv, preferred_element_type=jnp.float32
            )
            halves.append(got[:, :lanes] / got[:, lanes:])
        outs.append(jnp.where(low, halves[0], halves[1]).reshape(rows_dev, WIN_COLS, lanes))
    outs = [outs[0][:, half:]] + outs[1:] + [outs[0][:, :half]]
    out_ref[0] = jnp.concatenate(outs, axis=1).astype(jnp.bfloat16)


def attention(query, pair, ctx_pair, rel_bias, ctx_bias):
    samples, rows_dev, _, cols = query.shape
    padded, ctx_count = pair.shape[1], ctx_pair.shape[0] * ctx_pair.shape[2]
    heads = cols // HEAD_DIM
    lanes = 2 * HEAD_DIM
    pairs = cols // lanes
    nq, nk = rows_dev * WIN_COLS, padded * 2 * WIN_COLS
    flat = jnp.pad(rel_bias, ((0, 0), (0, 1), (0, 1))).reshape(heads, -1)
    flat = jnp.pad(flat, ((0, 0), (0, nk - flat.shape[1]))).reshape(pairs, 2, nk)
    token = lambda at: pl.BlockSpec((1, padded, GRID_W, lanes), lambda p, s: (s, 0, 0, p + at))
    far = lambda at: pl.BlockSpec(
        (ctx_pair.shape[0], 1, ctx_pair.shape[2], lanes), lambda p, s: (0, s, 0, p + at)
    )
    own = pl.BlockSpec((1, rows_dev, GRID_W, lanes), lambda p, s: (s, 0, 0, p))
    scores = samples * heads * 4 * nq * (nk + ctx_count)
    return pl.pallas_call(
        attention_kernel,
        grid=(pairs, samples),
        out_shape=jax.ShapeDtypeStruct(query.shape, jnp.bfloat16),
        in_specs=[
            pl.BlockSpec((1, 2, nk), lambda p, s: (p, 0, 0)),
            pl.BlockSpec(memory_space=pltpu.SMEM),
            own,
            token(0),
            token(pairs),
            far(0),
            far(pairs),
        ],
        out_specs=own,
        scratch_shapes=[pltpu.VMEM((2, 2, nq, nk), jnp.float32)],
        cost_estimate=pl.CostEstimate(
            flops=scores * 512, bytes_accessed=8 * query.size * 2, transcendentals=scores
        ),
    )(flat, ctx_bias, query, pair, pair, ctx_pair, ctx_pair)


def on_device(
    latent,
    context,
    cond,
    ctx_cond,
    w_shift,
    w_scale,
    w_gate,
    norm_gain,
    w_query,
    w_key,
    w_value,
    w_out,
    rel_bias,
    ctx_bias,
):
    samples = latent.shape[0]
    rows_sp = w_shift.shape[0]
    local_cols = w_shift.shape[1]
    sp_index = lax.axis_index("sp")
    ada = silu_rows(jnp.concatenate([cond, ctx_cond[None, :]], axis=0))
    ada_rows = lax.dynamic_slice_in_dim(ada, sp_index * rows_sp, rows_sp, 1)
    partial_value = jnp.stack(
        [
            jnp.dot(ada_rows, weight, preferred_element_type=jnp.float32)
            for weight in (w_shift, w_scale, w_gate)
        ]
    )
    summed = lax.psum(partial_value, "sp")
    modulation = lax.all_gather(summed, "tp", axis=2, tiled=True)
    hidden = modulate_rows(
        latent, norm_gain, modulation[0, :samples, None, :], modulation[1, :samples, None, :]
    )
    w_triple = jnp.concatenate([w_query, w_key, w_value], axis=1)
    triple = jnp.dot(
        lax.all_gather(hidden, "tp", axis=1, tiled=True),
        w_triple,
        preferred_element_type=jnp.float32,
    ).astype(jnp.bfloat16)
    ctx_hidden = modulate_rows(context, norm_gain, modulation[0, samples], modulation[1, samples])
    w_pair = jnp.concatenate([w_key, w_value], axis=1)
    own_pair = jnp.dot(ctx_hidden, w_pair, preferred_element_type=jnp.float32).astype(jnp.bfloat16)
    ctx_pair = lax.all_gather(own_pair, "sp", axis=1, tiled=True)
    heads = local_cols // HEAD_DIM
    tokens_sp = triple.shape[1]
    rows_dev = tokens_sp // GRID_W
    rows_all = rows_dev * lax.axis_size("sp")
    reach = WIN_ROWS // 2
    query = triple[..., :local_cols].reshape(samples, rows_dev, GRID_W, local_cols)
    pair = triple[..., local_cols:].reshape(samples, rows_dev, GRID_W, 2 * local_cols)
    padded_pair = extended(pair, (("sp", 1),), reach)
    mixed = attention(query, padded_pair, ctx_pair[None], rel_bias, ctx_bias)
    attended = mixed.reshape(samples, tokens_sp, local_cols)
    attended = attended.transpose(1, 0, 2)
    update = lax.psum_scatter(
        jnp.einsum("tsc,cd->tsd", attended, w_out, preferred_element_type=jnp.float32).astype(
            jnp.bfloat16
        ),
        "tp",
        scatter_dimension=0,
        tiled=True,
    ).astype(jnp.float32)
    gate = modulation[2, :samples, None, :]
    result = latent.astype(jnp.float32) + gate * update.transpose(1, 0, 2)
    return result.astype(jnp.bfloat16)


MESH = pl.DeviceIdType.MESH


def entry_barrier(peers):
    barrier = pltpu.get_barrier_semaphore()
    for device in peers:
        pl.semaphore_signal(barrier, inc=1, device_id=device, device_id_type=MESH)
    pl.semaphore_wait(barrier, len(peers))


def block_kernel(
    far_ref, flat_ref, gain_ref, cond_ref, ctx_cond_ref,
    ws_ref, wc_ref, wg_ref, latent_ref, ctx_ref, wq_ref, wk_ref, wv_ref, wo_ref,
    out_ref,
    ada, wm, part, got, total, full, buf, other, cx, cs, wq, wkv, wo, kv, qs, ckv, table,
    att, att_in, parts, y_in, fwd, x_in,
    own_sem, s1, r1, s2, r2, s_c, r_c, s_x, r_x, s_y, r_y, s_d, r_d, s_z, r_z, s_h, r_h,
    s_w, r_w, s_a, r_a, s_p, r_p, s_f, r_f,
):
    sp, tp = lax.axis_index("sp"), lax.axis_index("tp")
    n_sp, n_tp = lax.axis_size("sp"), lax.axis_size("tp")
    y, c = tp // 2, lax.rem(tp, 2)
    z, x = sp // 2, lax.rem(sp, 2)
    n_z = n_sp // 2
    same = x == y
    differs = x != y
    tokens, width = other.shape
    cols = wq.shape[1]
    rows_mod = wm.shape[1]
    lanes = 2 * HEAD_DIM
    pairs = cols // lanes
    half = WIN_COLS // 2
    reach = WIN_ROWS // 2
    own_rows = tokens // GRID_W
    group_rows = 2 * own_rows
    layer_rows = 4 * group_rows
    chunks = s_x.shape[0]
    size = tokens // chunks
    over_sp = [lax.rem(sp + k, n_sp) for k in range(1, n_sp)]
    over_tp = [lax.rem(tp + k, n_tp) for k in range(1, n_tp)]
    sib, across = (sp, tp + 1 - 2 * c), (sp, (1 - y) * 2 + c)
    beside = (sp + 1 - 2 * x, tp)
    g_own, g_x, g_y, g_d = 2 * x + y, 2 * (1 - x) + y, 2 * x + 1 - y, 2 * (1 - x) + 1 - y
    drain = []

    def remote(src, dst, s, r, device):
        return pltpu.make_async_remote_copy(
            src_ref=src, dst_ref=dst, send_sem=s, recv_sem=r, device_id=device, device_id_type=MESH
        )

    def begin(make, cond=None):
        drain.append((make, cond))
        if cond is None:
            make().start()
        else:
            @pl.when(cond)
            def _():
                make().start()

    def local(k, src, dst):
        copy = pltpu.make_async_copy(src, dst, own_sem.at[k])
        copy.start()
        return copy

    mod_copies = [local(k, w, wm.at[k]) for k, w in enumerate((ws_ref, wc_ref, wg_ref))]
    other_copy = local(3, latent_ref.at[1 - x], other)
    own_copy = local(4, latent_ref.at[x], buf.at[2 * g_own + c])
    ctx_half = cs.shape[0]
    ctx_part = lambda k: pl.ds(pl.multiple_of(k * ctx_half, ctx_half), ctx_half)
    stage_copy = local(5, ctx_ref.at[1 - x, ctx_part(c)], cs)
    ctx_copy = local(6, ctx_ref.at[x], cx.at[x])
    weight_copies = [
        local(7, wk_ref, wkv.at[:, pl.ds(0, cols)]),
        local(8, wv_ref, wkv.at[:, pl.ds(cols, cols)]),
        local(9, wq_ref, wq),
        local(10, wo_ref, wo.at[0]),
    ]
    entry_barrier([(p, tp) for p in over_sp] + [(sp, p) for p in over_tp])

    def piece(g, h):
        return buf.at[2 * g + c, pl.ds(h * size, size)]

    def to_beside(h):
        return remote(other.at[pl.ds(h * size, size)], piece(g_own, h), s_x.at[h], r_x.at[h], beside)

    def from_beside(h):
        return remote(other.at[pl.ds(h * size, size)], piece(g_x, h), s_x.at[h], r_x.at[h], beside)

    def over_y(g, flow, h):
        return remote(piece(g, h), piece(g, h), s_y.at[flow, h], r_y.at[flow, h], across)

    def to_sib(k, g, h):
        return remote(piece(g, h), piece(g, h), s_d.at[k, h], r_d.at[k, h], sib)

    def from_sib(k, g, h):
        there = buf.at[2 * g + 1 - c, pl.ds(h * size, size)]
        return remote(there, there, s_d.at[k, h], r_d.at[k, h], sib)

    mine = pl.ds(pl.multiple_of(sp * rows_mod, rows_mod), rows_mod)
    ada[...] = jnp.zeros_like(ada)
    ada[0:2, :] = cond_ref[:, mine].astype(jnp.float32)
    ada[2:3, :] = ctx_cond_ref[:, mine].astype(jnp.float32)
    values = ada[...]
    values = (values / (1.0 + jnp.exp(-values))).astype(jnp.bfloat16)
    at = 0
    for k, count in enumerate((3, 3, 2)):
        mod_copies[k].wait()
        value = jnp.dot(values, wm[k], preferred_element_type=jnp.float32)
        part[at : at + count, :] = value[:count]
        at += count
    for k, peer in enumerate(over_sp):
        begin(functools.partial(remote, part, got.at[k], s1.at[k], r1.at[k], (peer, tp)))

    stage_copy.wait()
    begin(lambda: remote(cs, cx.at[x, ctx_part(c)], s_c.at[0], r_c.at[0], beside))
    other_copy.wait()
    own_copy.wait()
    for h in range(chunks):
        if h < 2:
            begin(functools.partial(over_y, g_own, 0, h))
        begin(functools.partial(to_beside, h))
    for h in range(chunks):
        begin(functools.partial(to_sib, 0, g_own, h))

    span = 2 * WIN_COLS
    nk = table.shape[-1]
    nq = table.shape[-2] // 2
    rows_all = layer_rows * n_z
    lane = lax.broadcasted_iota(jnp.int32, (WIN_COLS, nk), 1)
    p = lax.broadcasted_iota(jnp.int32, (WIN_COLS, nk), 0)
    k_row, k_col = lane // span, lane % span
    inner = (k_col - p >= 0) & (k_col - p < WIN_COLS)
    edge = (p < half) == (k_col < WIN_COLS)

    def tables(pair, carry):
        for h in range(2):
            line = flat_ref[pl.ds(2 * pair + h, 1), :]
            line = jnp.broadcast_to(line, (WIN_COLS, line.shape[1]))
            for r in range(group_rows):
                shift = (span * (r + reach - WIN_ROWS + 1) - half + 1) % line.shape[1]
                rolled = pltpu.roll(line, shift, 1, stride=1, stride_axis=0)[:, :nk] * LOG2E
                at_rows = pl.ds(h * nq + r * WIN_COLS, WIN_COLS)
                for kind in range(3):
                    row = z * layer_rows + r + (0, 0, layer_rows - group_rows)[kind]
                    first = row - reach
                    if kind:
                        first = jnp.clip(first, 0, rows_all - WIN_ROWS)
                    key_row = k_row + (row - r - reach)
                    inside = (key_row >= first) & (key_row < first + WIN_ROWS)
                    table[kind, pair, 0, at_rows, :] = jnp.where(inside & edge, rolled, -jnp.inf)
                    table[kind, pair, 1, at_rows, :] = jnp.where(inside & inner, rolled, -jnp.inf)
        return carry

    last_row = kv.shape[0] - 1
    kv[last_row] = jnp.zeros(kv.shape[1:], jnp.bfloat16)

    @pl.when(z == 0)
    def _():
        kv[0:reach] = jnp.zeros((reach,) + kv.shape[1:], jnp.bfloat16)

    @pl.when(z == n_z - 1)
    def _():
        kv[last_row - reach + 1 : last_row] = jnp.zeros((reach - 1,) + kv.shape[1:], jnp.bfloat16)

    lax.fori_loop(0, pairs // 2, tables, 0)

    value = part[...]
    for k, peer in enumerate(over_sp):
        remote(part, got.at[k], s1.at[k], r1.at[k], (peer, tp)).wait_recv()
        value = value + got[k]
    total[...] = value
    columns = pl.ds(pl.multiple_of(tp * cols, cols), cols)
    full[:, columns] = value
    for k, peer in enumerate(over_tp):
        begin(
            functools.partial(remote, total, full.at[:, columns], s2.at[k], r2.at[k], (sp, peer))
        )
    begin(functools.partial(over_y, g_own, 0, 2))
    last_own = functools.partial(over_y, g_own, 0, 3)
    drain.append((last_own, None))

    @pl.when(same)
    def _():
        last_own().start()

    remote(cs, cx.at[1 - x, ctx_part(c)], s_c.at[0], r_c.at[0], beside).wait_recv()
    ctx_sib = lambda k: remote(
        cx.at[1 - x, ctx_part(k)], cx.at[1 - x, ctx_part(k)], s_c.at[1], r_c.at[1], sib
    )
    begin(lambda: ctx_sib(c))
    lax.fori_loop(pairs // 2, pairs, tables, 0)
    ctx_copy.wait()
    ctx_sib(1 - c).wait_recv()
    for copy in weight_copies:
        copy.wait()
    for k, peer in enumerate(over_tp):
        there = pl.ds(pl.multiple_of(peer * cols, cols), cols)
        remote(total, full.at[:, there], s2.at[k], r2.at[k], (sp, peer)).wait_recv()
    begin(lambda: remote(wo.at[0], wo.at[1], s_w.at[0], r_w.at[0], sib))

    def relay(h):
        from_beside(h).wait_recv()
        over_y(g_x, 1, h).start()
        to_sib(1, g_x, h).start()

    for h in range(chunks):
        drain.append((functools.partial(over_y, g_x, 1, h), None))
        drain.append((functools.partial(to_sib, 1, g_x, h), None))
    relay(0)

    def normed(rows, which):
        rows = rows.astype(jnp.float32)
        inverse = lax.rsqrt(jnp.mean(rows * rows, axis=-1, keepdims=True) + EPSILON)
        lift = gain_ref[...] * (1.0 + full[pl.ds(3 + which, 1), :])
        return (rows * inverse * lift + full[pl.ds(which, 1), :]).astype(jnp.bfloat16)

    hidden = jnp.concatenate([normed(cx[0], 2), normed(cx[1], 2)], axis=0)
    ckv[z] = jnp.dot(hidden, wkv[...], preferred_element_type=jnp.float32).astype(jnp.bfloat16)

    def layer_copy(zb, k, up):
        return remote(ckv.at[zb], ckv.at[zb], s_z.at[k], r_z.at[zb], (sp + 2 * up, tp))

    for k, up in enumerate((2, -2, 1, -1)):
        begin(functools.partial(layer_copy, z, k, up), (z + up >= 0) & (z + up < n_z))
    far_up, far_down = z == n_z - 2, z == 1

    def ctx_relay():
        for cond, zb, k, up in ((far_up, 0, 4, 1), (far_down, n_z - 1, 5, -1)):
            @pl.when(cond)
            def _():
                layer_copy(zb, k, up).wait_recv()
                layer_copy(zb, k, up).start()

    drain.append((functools.partial(layer_copy, 0, 4, 1), far_up))
    drain.append((functools.partial(layer_copy, n_z - 1, 5, -1), far_down))

    g_third = jnp.where(same, g_d, g_y)
    g_fourth = jnp.where(same, g_y, g_d)
    has_up, has_down = z < n_z - 1, z > 0
    halo_up = lambda: remote(
        kv.at[pl.ds(layer_rows, reach)], kv.at[pl.ds(0, reach)], s_h.at[0], r_h.at[0], (sp + 2, tp)
    )
    halo_down = lambda: remote(
        kv.at[pl.ds(reach, reach - 1)], kv.at[pl.ds(reach + layer_rows, reach - 1)],
        s_h.at[1], r_h.at[1], (sp - 2, tp),
    )

    def incoming(k, flow, g, cond):
        @pl.when(cond)
        def _():
            for h in range(chunks):
                over_y(g, flow, h).wait_recv()
                to_sib(k, g, h).start()

    def shared(k, g, cond):
        @pl.when(cond)
        def _():
            for h in range(chunks):
                from_sib(k, g, h).wait_recv()

    for h in range(chunks):
        drain.append((functools.partial(to_sib, 2, g_y, h), None))
        drain.append((functools.partial(to_sib, 3, g_d, h), None))

    def before(k):
        if k == 0:
            for h in range(chunks):
                from_sib(0, g_own, h).wait_recv()
        if k == 1:
            for h in range(1, chunks):
                relay(h)

            @pl.when(differs)
            def _():
                last_own().start()

            for h in range(chunks):
                from_sib(1, g_x, h).wait_recv()
        if k == 2:
            incoming(2, 0, g_y, differs)
            ctx_relay()
            incoming(3, 1, g_d, same)
            shared(2, g_y, differs)
            shared(3, g_d, same)
        if k == 3:
            incoming(2, 0, g_y, same)
            incoming(3, 1, g_d, differs)
            shared(2, g_y, same)
            shared(3, g_d, differs)

    def project(i, carry):
        for k in range(4):
            @pl.when(i == k)
            def _():
                before(k)

        g = jnp.where(i == 0, g_own, jnp.where(i == 1, g_x, jnp.where(i == 2, g_third, g_fourth)))
        hidden = jnp.concatenate([normed(buf[2 * g + e], x) for e in range(2)], axis=0)
        value = jnp.dot(hidden, wkv[...], preferred_element_type=jnp.float32).astype(jnp.bfloat16)
        kv[pl.ds(reach + group_rows * g, group_rows)] = value.reshape(group_rows, GRID_W, 2 * cols)
        query = jnp.dot(hidden, wq[...], preferred_element_type=jnp.float32)
        query = query.reshape(group_rows, GRID_W, cols)
        query = jnp.concatenate([query[:, GRID_W - half :], query[:, : GRID_W - half]], axis=1)
        qs[pl.ds(group_rows * g, group_rows)] = query.astype(jnp.bfloat16)

        @pl.when((g == 0) & has_down)
        def _():
            halo_down().start()

        @pl.when((g == 3) & has_up)
        def _():
            halo_up().start()

        return carry

    lax.fori_loop(0, 4, project, 0)
    drain.append((halo_down, has_down))
    drain.append((halo_up, has_up))

    for k in range(1, n_z):
        zb = lax.rem(z + k, n_z)
        done = (far_up & (zb == 0)) | (far_down & (zb == n_z - 1))

        @pl.when(jnp.logical_not(done))
        def _():
            layer_copy(zb, 0, 1).wait_recv()

    remote(wo.at[0], wo.at[1], s_w.at[0], r_w.at[0], sib).wait_recv()

    factor = HEAD_DIM ** (-0.5) * LOG2E
    contract = (((1,), (1,)), ((), ()))
    low = lax.broadcasted_iota(jnp.int32, (nq, lanes), 1) < HEAD_DIM
    first_head = lax.broadcasted_iota(jnp.int32, (2 * nq, 1), 0) < nq
    key_rows = nk // span
    ctx_count = ckv.shape[0] * ckv.shape[1]

    def attend(i, g, pair):
        own = pl.ds(pl.multiple_of(pair * lanes, lanes), lanes)
        values_at = pl.ds(pl.multiple_of(cols + pair * lanes, lanes), lanes)
        rows = pl.ds(group_rows * g, key_rows)
        kind = jnp.where(g == 0, 1, jnp.where(g == 3, 2, 0))
        ck = ckv[:, :, own].reshape(ctx_count, lanes)
        cv = ckv[:, :, values_at].reshape(ctx_count, lanes)
        cv = jnp.concatenate([cv, jnp.ones((ctx_count, lanes), jnp.bfloat16)], axis=1)
        ones = jnp.ones((nk, lanes), jnp.bfloat16)
        lift = jnp.where(first_head, far_ref[2 * pair], far_ref[2 * pair + 1]) * LOG2E
        outs = []
        for b in range(GRID_W // WIN_COLS):
            q = qs[pl.ds(group_rows * g, group_rows), WIN_COLS * b : WIN_COLS * (b + 1), own]
            q = q.reshape(nq, lanes)
            zero = jnp.zeros_like(q)
            q = jnp.concatenate([jnp.where(low, q, zero), jnp.where(low, zero, q)], axis=0)

            def keys(part_at):
                if b == 0:
                    got = jnp.concatenate(
                        [kv[rows, GRID_W - WIN_COLS :, part_at], kv[rows, :WIN_COLS, part_at]], axis=1
                    )
                else:
                    got = kv[rows, WIN_COLS * (b - 1) : WIN_COLS * (b + 1), part_at]
                return got.reshape(nk, lanes)

            v = jnp.concatenate([keys(values_at), ones], axis=1)
            near = lax.dot_general(q, keys(own), contract, preferred_element_type=jnp.float32)
            near = near * factor + table[kind, pair, min(b, 1)]
            far = lax.dot_general(q, ck, contract, preferred_element_type=jnp.float32)
            top = jnp.maximum(
                jnp.max(near, axis=-1, keepdims=True),
                jnp.max(far, axis=-1, keepdims=True) * factor + lift,
            )
            near = jnp.exp2(near - top).astype(jnp.bfloat16)
            far = jnp.exp2(far * factor + (lift - top)).astype(jnp.bfloat16)
            summed = jnp.dot(near, v, preferred_element_type=jnp.float32) + jnp.dot(
                far, cv, preferred_element_type=jnp.float32
            )
            mean = summed[:, :lanes] / summed[:, lanes:]
            outs.append(jnp.where(low, mean[:nq], mean[nq:]).reshape(group_rows, WIN_COLS, lanes))
        outs = [outs[0][:, half:]] + outs[1:] + [outs[0][:, :half]]
        att[i, :, :, own] = jnp.concatenate(outs, axis=1).astype(jnp.bfloat16)

    def att_half(i, k):
        return att.at[i, pl.ds(own_rows * k, own_rows)]

    def to_across(i, slot, h):
        part_at = pl.ds(h * size, size)
        return remote(
            parts.at[i, part_at], y_in.at[slot, part_at], s_p.at[slot, h], r_p.at[slot, h], across
        )

    def attention_step(i, carry):
        inner_first = jnp.where(y == 0, 1, 2)
        g = jnp.where(
            i == 0, inner_first, jnp.where(i == 1, 3 - inner_first, jnp.where(i == 2, 3 * (1 - y), 3 * y))
        )

        @pl.when((g == 0) & has_down)
        def _():
            remote(kv.at[pl.ds(0, reach)], kv.at[pl.ds(0, reach)], s_h.at[0], r_h.at[0], (sp - 2, tp)).wait_recv()

        @pl.when((g == 3) & has_up)
        def _():
            there = kv.at[pl.ds(reach + layer_rows, reach - 1)]
            remote(there, there, s_h.at[1], r_h.at[1], (sp + 2, tp)).wait_recv()

        def one(pair, inner_carry):
            attend(i, g, pair)
            return inner_carry

        lax.fori_loop(0, pairs, one, 0)
        give = remote(att_half(i, 1 - c), att_in.at[i], s_a.at[i], r_a.at[i], sib)
        give.start()
        update = jnp.dot(
            att[i, pl.ds(own_rows * c, own_rows)].reshape(tokens, cols), wo[0],
            preferred_element_type=jnp.float32,
        )
        give.wait_recv()
        update = update + jnp.dot(
            att_in[i].reshape(tokens, cols), wo[1], preferred_element_type=jnp.float32
        )
        parts[i] = update.astype(jnp.bfloat16)
        for slot in range(2):
            @pl.when(i == 2 * slot)
            def _():
                for h in range(chunks):
                    to_across(2 * slot, slot, h).start()

        return carry

    lax.fori_loop(0, 4, attention_step, 0)
    to_att = lambda i: remote(att_half(i, 1 - c), att_in.at[i], s_a.at[i], r_a.at[i], sib)
    for i in range(4):
        drain.append((functools.partial(to_att, i), None))

    def to_owner(h):
        part_at = pl.ds(h * size, size)
        return remote(fwd.at[part_at], x_in.at[part_at], s_f.at[h], r_f.at[h], beside)

    def finish(which, h, base, update):
        gate = full[pl.ds(6 + which, 1), :]
        out_ref[which, pl.ds(h * size, size)] = (base.astype(jnp.float32) + gate * update).astype(jnp.bfloat16)

    for slot in range(2):
        final, onward = (differs, same) if slot == 0 else (same, differs)
        for h in range(chunks):
            part_at = pl.ds(h * size, size)
            to_across(2 * slot, slot, h).wait_recv()

            @pl.when(onward)
            def _():
                both = parts[2 * slot + 1, part_at].astype(jnp.float32) + y_in[slot, part_at].astype(jnp.float32)
                fwd[part_at] = both.astype(jnp.bfloat16)
                to_owner(h).start()

            @pl.when(final)
            def _():
                both = parts[2 * slot + 1, part_at].astype(jnp.float32) + y_in[slot, part_at].astype(jnp.float32)
                finish(x, h, buf[2 * g_own + c, part_at], both)

            drain.append((functools.partial(to_across, 2 * slot, slot, h), None))
    for h in range(chunks):
        part_at = pl.ds(h * size, size)
        to_owner(h).wait_recv()
        finish(1 - x, h, other[part_at], x_in[part_at].astype(jnp.float32))
        drain.append((functools.partial(to_owner, h), None))

    for make, cond in drain:
        if cond is None:
            make().wait_send()
        else:
            @pl.when(cond)
            def _():
                make().wait_send()


def on_eight(
    latent, context, cond, ctx_cond, w_shift, w_scale, w_gate, norm_gain,
    w_query, w_key, w_value, w_out, rel_bias, ctx_bias,
):
    n_sp, n_tp = lax.axis_size("sp"), lax.axis_size("tp")
    samples, tokens, width = latent.shape
    ctx_tokens = context.shape[1]
    rows_mod, cols = w_shift.shape
    heads = cols // HEAD_DIM
    pairs = heads // 2
    n_z = n_sp // 2
    own_rows = tokens // GRID_W
    group_rows = 2 * own_rows
    layer_rows = 4 * group_rows
    key_rows = group_rows + WIN_ROWS
    nq, nk = group_rows * WIN_COLS, key_rows * 2 * WIN_COLS
    flat = jnp.pad(rel_bias, ((0, 0), (0, 1), (0, 1))).reshape(heads, -1)
    vmem, hbm = pl.BlockSpec(memory_space=pltpu.VMEM), pl.BlockSpec(memory_space=pl.ANY)
    dma = pltpu.SemaphoreType.DMA
    chunks = 4
    bf16, f32 = jnp.bfloat16, jnp.float32
    mods = (8, cols)
    return pl.pallas_call(
        block_kernel,
        out_shape=jax.ShapeDtypeStruct(latent.shape, bf16),
        in_specs=[pl.BlockSpec(memory_space=pltpu.SMEM)] + [vmem] * 4 + [hbm] * 9,
        out_specs=vmem,
        scratch_shapes=[
            pltpu.VMEM((8, rows_mod), f32),
            pltpu.VMEM((3, rows_mod, cols), bf16),
            pltpu.VMEM(mods, f32),
            pltpu.VMEM((n_sp - 1,) + mods, f32),
            pltpu.VMEM(mods, f32),
            pltpu.VMEM((8, width), f32),
            pltpu.VMEM((8, tokens, width), bf16),
            pltpu.VMEM((tokens, width), bf16),
            pltpu.VMEM((2, ctx_tokens, width), bf16),
            pltpu.VMEM((ctx_tokens // 2, width), bf16),
            pltpu.VMEM((width, cols), bf16),
            pltpu.VMEM((width, 2 * cols), bf16),
            pltpu.VMEM((2, cols, width), bf16),
            pltpu.VMEM((layer_rows + WIN_ROWS, GRID_W, 2 * cols), bf16),
            pltpu.VMEM((layer_rows, GRID_W, cols), bf16),
            pltpu.VMEM((n_z, 2 * ctx_tokens, 2 * cols), bf16),
            pltpu.VMEM((3, pairs, 2, 2 * nq, nk), f32),
            pltpu.VMEM((4, group_rows, GRID_W, cols), bf16),
            pltpu.VMEM((4, own_rows, GRID_W, cols), bf16),
            pltpu.VMEM((4, tokens, width), bf16),
            pltpu.VMEM((2, tokens, width), bf16),
            pltpu.VMEM((tokens, width), bf16),
            pltpu.VMEM((tokens, width), bf16),
            dma((11,)),
            dma((n_sp - 1,)), dma((n_sp - 1,)), dma((n_tp - 1,)), dma((n_tp - 1,)),
            dma((2,)), dma((2,)), dma((chunks,)), dma((chunks,)),
            dma((2, chunks)), dma((2, chunks)), dma((4, chunks)), dma((4, chunks)),
            dma((6,)), dma((n_z,)), dma((2,)), dma((2,)),
            dma((1,)), dma((1,)), dma((4,)), dma((4,)),
            dma((2, chunks)), dma((2, chunks)), dma((chunks,)), dma((chunks,)),
        ],
        compiler_params=pltpu.CompilerParams(
            collective_id=1, has_side_effects=True, vmem_limit_bytes=60 * 2**20
        ),
    )(
        ctx_bias, flat, norm_gain[None, :], cond, ctx_cond[None, :],
        w_shift, w_scale, w_gate, latent, context, w_query, w_key, w_value, w_out,
    )


def solution(mesh):
    shape = dict(mesh.shape)
    quick = shape["tp"] == 4 and shape["sp"] == 8
    return jax.shard_map(
        on_eight if quick else on_device,
        mesh=mesh,
        in_specs=(
            P(None, ("sp", "tp"), None),
            P(None, "sp", None),
            P(),
            P(),
            P("sp", "tp"),
            P("sp", "tp"),
            P("sp", "tp"),
            P(),
            P(None, "tp"),
            P(None, "tp"),
            P(None, "tp"),
            P("tp", None),
            P("tp", None, None),
            P("tp"),
        ),
        out_specs=P(None, ("sp", "tp"), None),
        check_vma=False,
    )
```

```python
import functools

import jax
import jax.numpy as jnp
from jax import lax
from jax.experimental import pallas as pl
from jax.experimental.pallas import tpu as pltpu
from jax.sharding import PartitionSpec as P

HEAD_DIM = 64
GRID_W = 64
WIN_ROWS = 8
WIN_COLS = 16


EPSILON = 1e-06


def extended(shard, sides, width):
    for axis, dim in sides:
        size, length = (lax.axis_size(axis), shard.shape[dim])
        up = [(i, (i + 1) % size) for i in range(size - 1)]
        down = [(j, i) for i, j in up]
        last = lax.slice_in_dim(shard, length - width, length, axis=dim)
        first = lax.slice_in_dim(shard, 0, width, axis=dim)
        before = lax.ppermute(last, axis, up)
        after = lax.ppermute(first, axis, down)
        shard = jnp.concatenate([before, shard, after], axis=dim)
    return shard


def silu_rows(values):
    return jax.nn.silu(values.astype(jnp.float32)).astype(jnp.bfloat16)


def modulate_rows(rows, gain, shift, scale):
    floats = rows.astype(jnp.float32)
    inverse = lax.rsqrt(jnp.mean(floats * floats, axis=-1, keepdims=True) + EPSILON)
    return (floats * inverse * gain * (1.0 + scale) + shift).astype(jnp.bfloat16)

LOG2E = 1.4426950408889634


def attention_kernel(bias_ref, far_ref, q_ref, k_ref, v_ref, ck_ref, cv_ref, out_ref, table):
    pair = pl.program_id(0)
    rows_dev = q_ref.shape[1]
    padded = k_ref.shape[1]
    span = 2 * WIN_COLS
    half = WIN_COLS // 2
    reach = WIN_ROWS // 2
    nq, nk = rows_dev * WIN_COLS, padded * span
    lanes = 2 * HEAD_DIM

    @pl.when(pl.program_id(1) == 0)
    def _():
        sp = lax.axis_index("sp")
        rows_all = rows_dev * lax.axis_size("sp")
        at = lax.broadcasted_iota(jnp.int32, (WIN_COLS, nk), 1)
        p = lax.broadcasted_iota(jnp.int32, (WIN_COLS, nk), 0)
        key_row = sp * rows_dev - reach + at // span
        k = at % span
        inner = (k - p >= 0) & (k - p < WIN_COLS)
        edge = (p < half) == (k < WIN_COLS)
        for r in range(rows_dev):
            row = sp * rows_dev + r
            first = jnp.clip(row - reach, 0, rows_all - WIN_ROWS)
            inside = (key_row >= first) & (key_row < first + WIN_ROWS)
            shift = span * (r + reach - WIN_ROWS + 1) - half + 1
            for h in range(2):
                line = jnp.broadcast_to(bias_ref[0, h : h + 1, :], (WIN_COLS, nk))
                line = pltpu.roll(line, shift % nk, 1, stride=1, stride_axis=0) * LOG2E
                at_rows = pl.ds(r * WIN_COLS, WIN_COLS)
                table[h, 0, at_rows, :] = jnp.where(inside & edge, line, -jnp.inf)
                table[h, 1, at_rows, :] = jnp.where(inside & inner, line, -jnp.inf)

    factor = HEAD_DIM ** (-0.5) * LOG2E
    ck = ck_ref[...].reshape(-1, lanes)
    ctx_count = ck.shape[0]
    cv = jnp.concatenate([cv_ref[...].reshape(-1, lanes), jnp.ones((ctx_count, lanes), jnp.bfloat16)], axis=1)
    ones = jnp.ones((nk, lanes), jnp.bfloat16)
    low = lax.broadcasted_iota(jnp.int32, (nq, lanes), 1) < HEAD_DIM
    contract = (((1,), (1,)), ((), ()))
    every = q_ref[0].astype(jnp.float32)
    outs = []
    for block in range(GRID_W // WIN_COLS):
        if block == 0:
            q = jnp.concatenate([every[:, GRID_W - half :], every[:, :half]], axis=1)
        else:
            q = every[:, WIN_COLS * block - half : WIN_COLS * (block + 1) - half]
        q = q.astype(jnp.bfloat16).reshape(nq, lanes)

        def keys(ref):
            if block == 0:
                got = jnp.concatenate([ref[0, :, GRID_W - WIN_COLS :, :], ref[0, :, :WIN_COLS, :]], 1)
            else:
                got = ref[0, :, WIN_COLS * (block - 1) : WIN_COLS * (block + 1), :]
            return got.reshape(nk, lanes)

        k = keys(k_ref)
        v = jnp.concatenate([keys(v_ref), ones], axis=1)
        halves = []
        for h in range(2):
            mine = low if h == 0 else jnp.logical_not(low)
            one = jnp.where(mine, q, jnp.zeros_like(q))
            near = lax.dot_general(one, k, contract, preferred_element_type=jnp.float32)
            near = near * factor + table[h, min(block, 1)]
            far = lax.dot_general(one, ck, contract, preferred_element_type=jnp.float32)
            far = far * factor + far_ref[2 * pair + h] * LOG2E
            top = jnp.maximum(
                jnp.max(near, axis=-1, keepdims=True), jnp.max(far, axis=-1, keepdims=True)
            )
            near = jnp.exp2(near - top).astype(jnp.bfloat16)
            far = jnp.exp2(far - top).astype(jnp.bfloat16)
            got = jnp.dot(near, v, preferred_element_type=jnp.float32) + jnp.dot(
                far, cv, preferred_element_type=jnp.float32
            )
            halves.append(got[:, :lanes] / got[:, lanes:])
        outs.append(jnp.where(low, halves[0], halves[1]).reshape(rows_dev, WIN_COLS, lanes))
    outs = [outs[0][:, half:]] + outs[1:] + [outs[0][:, :half]]
    out_ref[0] = jnp.concatenate(outs, axis=1).astype(jnp.bfloat16)


def attention(query, pair, ctx_pair, rel_bias, ctx_bias):
    samples, rows_dev, _, cols = query.shape
    padded, ctx_count = pair.shape[1], ctx_pair.shape[0] * ctx_pair.shape[2]
    heads = cols // HEAD_DIM
    lanes = 2 * HEAD_DIM
    pairs = cols // lanes
    nq, nk = rows_dev * WIN_COLS, padded * 2 * WIN_COLS
    flat = jnp.pad(rel_bias, ((0, 0), (0, 1), (0, 1))).reshape(heads, -1)
    flat = jnp.pad(flat, ((0, 0), (0, nk - flat.shape[1]))).reshape(pairs, 2, nk)
    token = lambda at: pl.BlockSpec((1, padded, GRID_W, lanes), lambda p, s: (s, 0, 0, p + at))
    far = lambda at: pl.BlockSpec(
        (ctx_pair.shape[0], 1, ctx_pair.shape[2], lanes), lambda p, s: (0, s, 0, p + at)
    )
    own = pl.BlockSpec((1, rows_dev, GRID_W, lanes), lambda p, s: (s, 0, 0, p))
    scores = samples * heads * 4 * nq * (nk + ctx_count)
    return pl.pallas_call(
        attention_kernel,
        grid=(pairs, samples),
        out_shape=jax.ShapeDtypeStruct(query.shape, jnp.bfloat16),
        in_specs=[
            pl.BlockSpec((1, 2, nk), lambda p, s: (p, 0, 0)),
            pl.BlockSpec(memory_space=pltpu.SMEM),
            own,
            token(0),
            token(pairs),
            far(0),
            far(pairs),
        ],
        out_specs=own,
        scratch_shapes=[pltpu.VMEM((2, 2, nq, nk), jnp.float32)],
        cost_estimate=pl.CostEstimate(
            flops=scores * 512, bytes_accessed=8 * query.size * 2, transcendentals=scores
        ),
    )(flat, ctx_bias, query, pair, pair, ctx_pair, ctx_pair)


def on_device(
    latent,
    context,
    cond,
    ctx_cond,
    w_shift,
    w_scale,
    w_gate,
    norm_gain,
    w_query,
    w_key,
    w_value,
    w_out,
    rel_bias,
    ctx_bias,
):
    samples = latent.shape[0]
    rows_sp = w_shift.shape[0]
    local_cols = w_shift.shape[1]
    sp_index = lax.axis_index("sp")
    ada = silu_rows(jnp.concatenate([cond, ctx_cond[None, :]], axis=0))
    ada_rows = lax.dynamic_slice_in_dim(ada, sp_index * rows_sp, rows_sp, 1)
    partial_value = jnp.stack(
        [
            jnp.dot(ada_rows, weight, preferred_element_type=jnp.float32)
            for weight in (w_shift, w_scale, w_gate)
        ]
    )
    summed = lax.psum(partial_value, "sp")
    modulation = lax.all_gather(summed, "tp", axis=2, tiled=True)
    hidden = modulate_rows(
        latent, norm_gain, modulation[0, :samples, None, :], modulation[1, :samples, None, :]
    )
    w_triple = jnp.concatenate([w_query, w_key, w_value], axis=1)
    triple = jnp.dot(
        lax.all_gather(hidden, "tp", axis=1, tiled=True),
        w_triple,
        preferred_element_type=jnp.float32,
    ).astype(jnp.bfloat16)
    ctx_hidden = modulate_rows(context, norm_gain, modulation[0, samples], modulation[1, samples])
    w_pair = jnp.concatenate([w_key, w_value], axis=1)
    own_pair = jnp.dot(ctx_hidden, w_pair, preferred_element_type=jnp.float32).astype(jnp.bfloat16)
    ctx_pair = lax.all_gather(own_pair, "sp", axis=1, tiled=True)
    heads = local_cols // HEAD_DIM
    tokens_sp = triple.shape[1]
    rows_dev = tokens_sp // GRID_W
    rows_all = rows_dev * lax.axis_size("sp")
    reach = WIN_ROWS // 2
    query = triple[..., :local_cols].reshape(samples, rows_dev, GRID_W, local_cols)
    pair = triple[..., local_cols:].reshape(samples, rows_dev, GRID_W, 2 * local_cols)
    padded_pair = extended(pair, (("sp", 1),), reach)
    mixed = attention(query, padded_pair, ctx_pair[None], rel_bias, ctx_bias)
    attended = mixed.reshape(samples, tokens_sp, local_cols)
    attended = attended.transpose(1, 0, 2)
    update = lax.psum_scatter(
        jnp.einsum("tsc,cd->tsd", attended, w_out, preferred_element_type=jnp.float32).astype(
            jnp.bfloat16
        ),
        "tp",
        scatter_dimension=0,
        tiled=True,
    ).astype(jnp.float32)
    gate = modulation[2, :samples, None, :]
    result = latent.astype(jnp.float32) + gate * update.transpose(1, 0, 2)
    return result.astype(jnp.bfloat16)


MESH = pl.DeviceIdType.MESH


def entry_barrier(peers):
    barrier = pltpu.get_barrier_semaphore()
    for device in peers:
        pl.semaphore_signal(barrier, inc=1, device_id=device, device_id_type=MESH)
    pl.semaphore_wait(barrier, len(peers))


def block_kernel(
    far_ref, bias_ref, gain_ref, cond_ref, ctx_cond_ref,
    ws_ref, wc_ref, wg_ref, latent_ref, ctx_ref, wq_ref, wk_ref, wv_ref, wo_ref,
    out_ref,
    flat, ada, wm, part, got, total, full, buf, other, cx, cs, wq, wkv, wo, kv, qs, ckv, table,
    att, att_in, parts, y_in, fwd, x_in,
    own_sem, s1, r1, s2, r2, s_c, r_c, s_x, r_x, s_y, r_y, s_d, r_d, s_z, r_z, s_h, r_h,
    s_w, r_w, s_a, r_a, s_p, r_p, s_f, r_f,
):
    sp, tp = lax.axis_index("sp"), lax.axis_index("tp")
    n_sp, n_tp = lax.axis_size("sp"), lax.axis_size("tp")
    y, c = tp // 2, lax.rem(tp, 2)
    z, x = sp // 2, lax.rem(sp, 2)
    n_z = n_sp // 2
    same = x == y
    differs = x != y
    tokens, width = other.shape
    cols = wq.shape[1]
    rows_mod = wm.shape[1]
    lanes = 2 * HEAD_DIM
    pairs = cols // lanes
    half = WIN_COLS // 2
    reach = WIN_ROWS // 2
    own_rows = tokens // GRID_W
    group_rows = 2 * own_rows
    layer_rows = 4 * group_rows
    chunks = s_x.shape[0]
    size = tokens // chunks
    over_sp = [lax.rem(sp + k, n_sp) for k in range(1, n_sp)]
    over_tp = [lax.rem(tp + k, n_tp) for k in range(1, n_tp)]
    sib, across = (sp, tp + 1 - 2 * c), (sp, (1 - y) * 2 + c)
    beside = (sp + 1 - 2 * x, tp)
    g_own, g_x, g_y, g_d = 2 * x + y, 2 * (1 - x) + y, 2 * x + 1 - y, 2 * (1 - x) + 1 - y
    drain = []

    def remote(src, dst, s, r, device):
        return pltpu.make_async_remote_copy(
            src_ref=src, dst_ref=dst, send_sem=s, recv_sem=r, device_id=device, device_id_type=MESH
        )

    def begin(make, cond=None):
        drain.append((make, cond))
        if cond is None:
            make().start()
        else:
            @pl.when(cond)
            def _():
                make().start()

    def local(k, src, dst):
        copy = pltpu.make_async_copy(src, dst, own_sem.at[k])
        copy.start()
        return copy

    mod_copies = [local(k, w, wm.at[k]) for k, w in enumerate((ws_ref, wc_ref, wg_ref))]
    other_copy = local(3, latent_ref.at[1 - x], other)
    own_copy = local(4, latent_ref.at[x], buf.at[2 * g_own + c])
    ctx_half = cs.shape[0]
    ctx_part = lambda k: pl.ds(pl.multiple_of(k * ctx_half, ctx_half), ctx_half)
    stage_copy = local(5, ctx_ref.at[1 - x, ctx_part(c)], cs)
    ctx_copy = local(6, ctx_ref.at[x], cx.at[x])
    weight_copies = [
        local(7, wk_ref, wkv.at[:, pl.ds(0, cols)]),
        local(8, wv_ref, wkv.at[:, pl.ds(cols, cols)]),
        local(9, wq_ref, wq),
        local(10, wo_ref, wo.at[0]),
    ]
    entry_barrier([(p, tp) for p in over_sp] + [(sp, p) for p in over_tp])

    def piece(g, h):
        return buf.at[2 * g + c, pl.ds(h * size, size)]

    def to_beside(h):
        return remote(other.at[pl.ds(h * size, size)], piece(g_own, h), s_x.at[h], r_x.at[h], beside)

    def from_beside(h):
        return remote(other.at[pl.ds(h * size, size)], piece(g_x, h), s_x.at[h], r_x.at[h], beside)

    def over_y(g, flow, h):
        return remote(piece(g, h), piece(g, h), s_y.at[flow, h], r_y.at[flow, h], across)

    def to_sib(k, g, h):
        return remote(piece(g, h), piece(g, h), s_d.at[k, h], r_d.at[k, h], sib)

    def from_sib(k, g, h):
        there = buf.at[2 * g + 1 - c, pl.ds(h * size, size)]
        return remote(there, there, s_d.at[k, h], r_d.at[k, h], sib)

    mine = pl.ds(pl.multiple_of(sp * rows_mod, rows_mod), rows_mod)
    ada[...] = jnp.zeros_like(ada)
    ada[0:2, :] = cond_ref[:, mine].astype(jnp.float32)
    ctx_cond = ctx_cond_ref[...].astype(jnp.float32)
    for k in range(n_sp):
        @pl.when(sp == k)
        def _():
            for j in range(rows_mod // 128):
                line = k * (rows_mod // 128) + j
                ada[2:3, 128 * j : 128 * (j + 1)] = ctx_cond[line : line + 1, :]
    values = ada[...]
    values = (values / (1.0 + jnp.exp(-values))).astype(jnp.bfloat16)
    at = 0
    for k, count in enumerate((3, 3, 2)):
        mod_copies[k].wait()
        value = jnp.dot(values, wm[k], preferred_element_type=jnp.float32)
        part[at : at + count, :] = value[:count]
        at += count
    for k, peer in enumerate(over_sp):
        begin(functools.partial(remote, part, got.at[k], s1.at[k], r1.at[k], (peer, tp)))

    stage_copy.wait()
    begin(lambda: remote(cs, cx.at[x, ctx_part(c)], s_c.at[0], r_c.at[0], beside))
    other_copy.wait()
    own_copy.wait()
    for h in range(chunks):
        if h < 2:
            begin(functools.partial(over_y, g_own, 0, h))
        begin(functools.partial(to_beside, h))
    for h in range(chunks):
        begin(functools.partial(to_sib, 0, g_own, h))

    span = 2 * WIN_COLS
    nk = table.shape[-1]
    nq = table.shape[-2] // 2
    rows_all = layer_rows * n_z
    lane = lax.broadcasted_iota(jnp.int32, (WIN_COLS, nk), 1)
    p = lax.broadcasted_iota(jnp.int32, (WIN_COLS, nk), 0)
    k_row, k_col = lane // span, lane % span
    inner = (k_col - p >= 0) & (k_col - p < WIN_COLS)
    edge = (p < half) == (k_col < WIN_COLS)

    flat[...] = jnp.zeros_like(flat)
    for k in range(bias_ref.shape[0]):
        flat[:, span * k : span * k + bias_ref.shape[2]] = bias_ref[k]

    def tables(pair, carry):
        for h in range(2):
            line = flat[pl.ds(2 * pair + h, 1), :]
            line = jnp.broadcast_to(line, (WIN_COLS, line.shape[1]))
            for r in range(group_rows):
                shift = (span * (r + reach - WIN_ROWS + 1) - half + 1) % line.shape[1]
                rolled = pltpu.roll(line, shift, 1, stride=1, stride_axis=0)[:, :nk] * LOG2E
                at_rows = pl.ds(h * nq + r * WIN_COLS, WIN_COLS)
                for kind in range(3):
                    row = z * layer_rows + r + (0, 0, layer_rows - group_rows)[kind]
                    first = row - reach
                    if kind:
                        first = jnp.clip(first, 0, rows_all - WIN_ROWS)
                    key_row = k_row + (row - r - reach)
                    inside = (key_row >= first) & (key_row < first + WIN_ROWS)
                    table[kind, pair, 0, at_rows, :] = jnp.where(inside & edge, rolled, -jnp.inf)
                    table[kind, pair, 1, at_rows, :] = jnp.where(inside & inner, rolled, -jnp.inf)
        return carry

    last_row = kv.shape[0] - 1
    kv[last_row] = jnp.zeros(kv.shape[1:], jnp.bfloat16)

    @pl.when(z == 0)
    def _():
        kv[0:reach] = jnp.zeros((reach,) + kv.shape[1:], jnp.bfloat16)

    @pl.when(z == n_z - 1)
    def _():
        kv[last_row - reach + 1 : last_row] = jnp.zeros((reach - 1,) + kv.shape[1:], jnp.bfloat16)

    lax.fori_loop(0, pairs // 2, tables, 0)

    value = part[...]
    for k, peer in enumerate(over_sp):
        remote(part, got.at[k], s1.at[k], r1.at[k], (peer, tp)).wait_recv()
        value = value + got[k]
    total[...] = value
    columns = pl.ds(pl.multiple_of(tp * cols, cols), cols)
    full[:, columns] = value
    for k, peer in enumerate(over_tp):
        begin(
            functools.partial(remote, total, full.at[:, columns], s2.at[k], r2.at[k], (sp, peer))
        )
    begin(functools.partial(over_y, g_own, 0, 2))
    last_own = functools.partial(over_y, g_own, 0, 3)
    drain.append((last_own, None))

    @pl.when(same)
    def _():
        last_own().start()

    remote(cs, cx.at[1 - x, ctx_part(c)], s_c.at[0], r_c.at[0], beside).wait_recv()
    ctx_sib = lambda k: remote(
        cx.at[1 - x, ctx_part(k)], cx.at[1 - x, ctx_part(k)], s_c.at[1], r_c.at[1], sib
    )
    begin(lambda: ctx_sib(c))
    lax.fori_loop(pairs // 2, pairs, tables, 0)
    ctx_copy.wait()
    ctx_sib(1 - c).wait_recv()
    for copy in weight_copies:
        copy.wait()
    for k, peer in enumerate(over_tp):
        there = pl.ds(pl.multiple_of(peer * cols, cols), cols)
        remote(total, full.at[:, there], s2.at[k], r2.at[k], (sp, peer)).wait_recv()
    begin(lambda: remote(wo.at[0], wo.at[1], s_w.at[0], r_w.at[0], sib))

    def relay(h):
        from_beside(h).wait_recv()
        over_y(g_x, 1, h).start()
        to_sib(1, g_x, h).start()

    for h in range(chunks):
        drain.append((functools.partial(over_y, g_x, 1, h), None))
        drain.append((functools.partial(to_sib, 1, g_x, h), None))
    relay(0)

    def normed(rows, which):
        rows = rows.astype(jnp.float32)
        inverse = lax.rsqrt(jnp.mean(rows * rows, axis=-1, keepdims=True) + EPSILON)
        lift = gain_ref[...] * (1.0 + full[pl.ds(3 + which, 1), :])
        return (rows * inverse * lift + full[pl.ds(which, 1), :]).astype(jnp.bfloat16)

    hidden = jnp.concatenate([normed(cx[0], 2), normed(cx[1], 2)], axis=0)
    ckv[z] = jnp.dot(hidden, wkv[...], preferred_element_type=jnp.float32).astype(jnp.bfloat16)

    def layer_copy(zb, k, up):
        return remote(ckv.at[zb], ckv.at[zb], s_z.at[k], r_z.at[zb], (sp + 2 * up, tp))

    for k, up in enumerate((2, -2, 1, -1)):
        begin(functools.partial(layer_copy, z, k, up), (z + up >= 0) & (z + up < n_z))
    far_up, far_down = z == n_z - 2, z == 1
    relays = far_up | far_down

    def ctx_relay():
        for cond, zb, k, up in ((far_up, 0, 4, 1), (far_down, n_z - 1, 5, -1)):
            @pl.when(cond)
            def _():
                layer_copy(zb, k, up).wait_recv()
                layer_copy(zb, k, up).start()

    drain.append((functools.partial(layer_copy, 0, 4, 1), far_up))
    drain.append((functools.partial(layer_copy, n_z - 1, 5, -1), far_down))

    g_third = jnp.where(same, g_d, g_y)
    g_fourth = jnp.where(same, g_y, g_d)
    has_up, has_down = z < n_z - 1, z > 0
    halo_up = lambda: remote(
        kv.at[pl.ds(layer_rows, reach)], kv.at[pl.ds(0, reach)], s_h.at[0], r_h.at[0], (sp + 2, tp)
    )
    halo_down = lambda: remote(
        kv.at[pl.ds(reach, reach - 1)], kv.at[pl.ds(reach + layer_rows, reach - 1)],
        s_h.at[1], r_h.at[1], (sp - 2, tp),
    )

    def incoming(k, flow, g, cond):
        @pl.when(cond)
        def _():
            for h in range(chunks):
                over_y(g, flow, h).wait_recv()
                to_sib(k, g, h).start()

    def shared(k, g, cond):
        @pl.when(cond)
        def _():
            for h in range(chunks):
                from_sib(k, g, h).wait_recv()

    for h in range(chunks):
        drain.append((functools.partial(to_sib, 2, g_y, h), None))
        drain.append((functools.partial(to_sib, 3, g_d, h), None))

    def before(k):
        if k == 0:
            for h in range(chunks):
                from_sib(0, g_own, h).wait_recv()
        if k == 1:
            for h in range(1, chunks):
                relay(h)

            @pl.when(differs)
            def _():
                last_own().start()

            for h in range(chunks):
                from_sib(1, g_x, h).wait_recv()
        if k == 2:
            incoming(2, 0, g_y, differs)
            incoming(3, 1, g_d, same)
            shared(2, g_y, differs)
            shared(3, g_d, same)
        if k == 3:
            ctx_relay()

            @pl.when(relays & has_down)
            def _():
                halo_down().start()

            @pl.when(relays & has_up)
            def _():
                halo_up().start()

            incoming(2, 0, g_y, same)
            incoming(3, 1, g_d, differs)
            shared(2, g_y, same)
            shared(3, g_d, differs)

    def project(i, carry):
        for k in range(4):
            @pl.when(i == k)
            def _():
                before(k)

        g = jnp.where(i == 0, g_own, jnp.where(i == 1, g_x, jnp.where(i == 2, g_third, g_fourth)))
        hidden = jnp.concatenate([normed(buf[2 * g + e], x) for e in range(2)], axis=0)
        value = jnp.dot(hidden, wkv[...], preferred_element_type=jnp.float32).astype(jnp.bfloat16)
        kv[pl.ds(reach + group_rows * g, group_rows)] = value.reshape(group_rows, GRID_W, 2 * cols)
        query = jnp.dot(hidden, wq[...], preferred_element_type=jnp.float32)
        query = query.reshape(group_rows, GRID_W, cols)
        query = jnp.concatenate([query[:, GRID_W - half :], query[:, : GRID_W - half]], axis=1)
        qs[pl.ds(group_rows * g, group_rows)] = query.astype(jnp.bfloat16)

        @pl.when((g == 0) & has_down & jnp.logical_not(relays))
        def _():
            halo_down().start()

        @pl.when((g == 3) & has_up & jnp.logical_not(relays))
        def _():
            halo_up().start()

        return carry

    lax.fori_loop(0, 4, project, 0)
    drain.append((halo_down, has_down))
    drain.append((halo_up, has_up))

    for k in range(1, n_z):
        zb = lax.rem(z + k, n_z)
        done = (far_up & (zb == 0)) | (far_down & (zb == n_z - 1))

        @pl.when(jnp.logical_not(done))
        def _():
            layer_copy(zb, 0, 1).wait_recv()

    remote(wo.at[0], wo.at[1], s_w.at[0], r_w.at[0], sib).wait_recv()

    factor = HEAD_DIM ** (-0.5) * LOG2E
    contract = (((1,), (1,)), ((), ()))
    low = lax.broadcasted_iota(jnp.int32, (nq, lanes), 1) < HEAD_DIM
    first_head = lax.broadcasted_iota(jnp.int32, (2 * nq, 1), 0) < nq
    key_rows = nk // span
    ctx_count = ckv.shape[0] * ckv.shape[1]

    def attend(i, g, pair, blocks):
        own = pl.ds(pair * lanes, lanes)
        values_at = pl.ds(cols + pair * lanes, lanes)
        rows = pl.ds(group_rows * g, key_rows)
        kind = jnp.where(g == 0, 1, jnp.where(g == 3, 2, 0))
        ck = ckv[:, :, own].reshape(ctx_count, lanes)
        cv = ckv[:, :, values_at].reshape(ctx_count, lanes)
        cv = jnp.concatenate([cv, jnp.ones((ctx_count, lanes), jnp.bfloat16)], axis=1)
        ones = jnp.ones((nk, lanes), jnp.bfloat16)
        lift = jnp.where(first_head, far_ref[2 * pair], far_ref[2 * pair + 1]) * LOG2E
        for b in blocks:
            q = qs[pl.ds(group_rows * g, group_rows), WIN_COLS * b : WIN_COLS * (b + 1), own]
            q = q.reshape(nq, lanes)
            zero = jnp.zeros_like(q)
            q = jnp.concatenate([jnp.where(low, q, zero), jnp.where(low, zero, q)], axis=0)

            def keys(part_at):
                if b == 0:
                    got = jnp.concatenate(
                        [kv[rows, GRID_W - WIN_COLS :, part_at], kv[rows, :WIN_COLS, part_at]], axis=1
                    )
                else:
                    got = kv[rows, WIN_COLS * (b - 1) : WIN_COLS * (b + 1), part_at]
                return got.reshape(nk, lanes)

            v = jnp.concatenate([keys(values_at), ones], axis=1)
            near = lax.dot_general(q, keys(own), contract, preferred_element_type=jnp.float32)
            near = near * factor + table[kind, pair, min(b, 1)]
            far = lax.dot_general(q, ck, contract, preferred_element_type=jnp.float32)
            top = jnp.maximum(
                jnp.max(near, axis=-1, keepdims=True),
                jnp.max(far, axis=-1, keepdims=True) * factor + lift,
            )
            near = jnp.exp2(near - top).astype(jnp.bfloat16)
            far = jnp.exp2(far * factor + (lift - top)).astype(jnp.bfloat16)
            summed = jnp.dot(near, v, preferred_element_type=jnp.float32) + jnp.dot(
                far, cv, preferred_element_type=jnp.float32
            )
            mean = summed[:, :lanes] / summed[:, lanes:]
            mean = jnp.where(low, mean[:nq], mean[nq:]).reshape(group_rows, WIN_COLS, lanes)
            att[i, :, WIN_COLS * b : WIN_COLS * (b + 1), own] = mean.astype(jnp.bfloat16)

    def give(i, batch, begins, count):
        at = pl.ds(begins, count)
        return remote(
            att.at[i, pl.ds(own_rows * (1 - c), own_rows), at], att_in.at[i, :, at],
            s_a.at[batch], r_a.at[batch], sib,
        )

    def to_across(i, slot, h):
        part_at = pl.ds(h * size, size)
        return remote(
            parts.at[i, part_at], y_in.at[slot, part_at], s_p.at[slot, h], r_p.at[slot, h], across
        )

    def to_owner(h):
        part_at = pl.ds(h * size, size)
        return remote(fwd.at[part_at], x_in.at[part_at], s_f.at[h], r_f.at[h], beside)

    def sum_at(i, slot, h):
        part_at = pl.ds(h * size, size)
        return parts[i, part_at].astype(jnp.float32) + y_in[slot, part_at].astype(jnp.float32)

    def forward(slot):
        for h in range(chunks):
            to_across(slot, slot, h).wait_recv()
            fwd[pl.ds(h * size, size)] = sum_at(2, slot, h).astype(jnp.bfloat16)
            to_owner(h).start()

    def group_of(i):
        first = jnp.where(y == 0, 1, 2)
        return jnp.where(i == 0, first, jnp.where(i == 1, 3 * (1 - y), jnp.where(i == 2, g_x, g_own)))

    def attention_block(i, batch, begins, count):
        g = group_of(i)
        blocks = range(begins // WIN_COLS, (begins + count) // WIN_COLS)

        for pair in range(pairs):
            attend(i, g, pair, blocks)
        give(i, batch, begins, count).start()
        at = pl.ds(begins, count)
        update = jnp.dot(
            att[i, pl.ds(own_rows * c, own_rows), at].reshape(own_rows * count, cols), wo[0],
            preferred_element_type=jnp.float32,
        )
        give(i, batch, begins, count).wait_recv()
        update = update + jnp.dot(
            att_in[i, :, at].reshape(own_rows * count, cols), wo[1], preferred_element_type=jnp.float32
        )
        for r in range(own_rows):
            parts[i, GRID_W * r + begins : GRID_W * r + begins + count] = update[
                count * r : count * (r + 1)
            ].astype(jnp.bfloat16)

    for part_of in range(2):
        attention_block(0, part_of, size * part_of, size)
        for r in range(own_rows):
            to_across(0, 0, 2 * r + part_of).start()

    def attention_step(i, carry):
        g = group_of(i)

        @pl.when((g == 0) & has_down)
        def _():
            there = kv.at[pl.ds(0, reach)]
            remote(there, there, s_h.at[0], r_h.at[0], (sp - 2, tp)).wait_recv()

        @pl.when((g == 3) & has_up)
        def _():
            there = kv.at[pl.ds(reach + layer_rows, reach - 1)]
            remote(there, there, s_h.at[1], r_h.at[1], (sp + 2, tp)).wait_recv()

        attention_block(i, i + 1, 0, GRID_W)

        @pl.when(i == 1)
        def _():
            for h in range(chunks):
                to_across(1, 1, h).start()

        @pl.when((i == 2) & same)
        def _():
            forward(0)

        return carry

    lax.fori_loop(1, 4, attention_step, 0)
    for part_of in range(2):
        drain.append((functools.partial(give, 0, part_of, size * part_of, size), None))
    for i in range(1, 4):
        drain.append((functools.partial(give, i, i + 1, 0, GRID_W), None))

    def finish(which, h, update):
        value = full[pl.ds(6 + which, 1), :] * update
        if h % 2 == 0:
            row = GRID_W * (h // 2)
            out_ref[which, row + GRID_W - half : row + GRID_W] = value[:half]
            out_ref[which, row : row + size - half] = value[half:]
        else:
            row = GRID_W * (h // 2) + size - half
            out_ref[which, row : row + size] = value

    def own(slot):
        for h in range(chunks):
            to_across(slot, slot, h).wait_recv()
            finish(x, h, sum_at(3, slot, h))

    @pl.when(differs)
    def _():
        forward(1)
        own(0)

    @pl.when(same)
    def _():
        own(1)

    for h in range(chunks):
        to_owner(h).wait_recv()
        finish(1 - x, h, x_in[h * size : (h + 1) * size].astype(jnp.float32))
        drain.append((functools.partial(to_owner, h), None))
        for slot in range(2):
            drain.append((functools.partial(to_across, slot, slot, h), None))

    for make, cond in drain:
        if cond is None:
            make().wait_send()
        else:
            @pl.when(cond)
            def _():
                make().wait_send()


def on_eight(
    latent, context, cond, ctx_cond, w_shift, w_scale, w_gate, norm_gain,
    w_query, w_key, w_value, w_out, rel_bias, ctx_bias,
):
    n_sp, n_tp = lax.axis_size("sp"), lax.axis_size("tp")
    samples, tokens, width = latent.shape
    ctx_tokens = context.shape[1]
    rows_mod, cols = w_shift.shape
    heads = cols // HEAD_DIM
    pairs = heads // 2
    n_z = n_sp // 2
    own_rows = tokens // GRID_W
    group_rows = 2 * own_rows
    layer_rows = 4 * group_rows
    key_rows = group_rows + WIN_ROWS
    nq, nk = group_rows * WIN_COLS, key_rows * 2 * WIN_COLS
    vmem, hbm = pl.BlockSpec(memory_space=pltpu.VMEM), pl.BlockSpec(memory_space=pltpu.HBM)
    dma = pltpu.SemaphoreType.DMA
    chunks = 4
    bf16, f32 = jnp.bfloat16, jnp.float32
    mods = (8, cols)
    delta = pl.pallas_call(
        block_kernel,
        out_shape=jax.ShapeDtypeStruct(latent.shape, f32),
        in_specs=[pl.BlockSpec(memory_space=pltpu.SMEM)] + [vmem] * 4 + [hbm] * 9,
        out_specs=vmem,
        scratch_shapes=[
            pltpu.VMEM((heads, 2 * WIN_ROWS * 2 * WIN_COLS), f32),
            pltpu.VMEM((8, rows_mod), f32),
            pltpu.VMEM((3, rows_mod, cols), bf16),
            pltpu.VMEM(mods, f32),
            pltpu.VMEM((n_sp - 1,) + mods, f32),
            pltpu.VMEM(mods, f32),
            pltpu.VMEM((8, width), f32),
            pltpu.VMEM((8, tokens, width), bf16),
            pltpu.VMEM((tokens, width), bf16),
            pltpu.VMEM((2, ctx_tokens, width), bf16),
            pltpu.VMEM((ctx_tokens // 2, width), bf16),
            pltpu.VMEM((width, cols), bf16),
            pltpu.VMEM((width, 2 * cols), bf16),
            pltpu.VMEM((2, cols, width), bf16),
            pltpu.VMEM((layer_rows + WIN_ROWS, GRID_W, 2 * cols), bf16),
            pltpu.VMEM((layer_rows, GRID_W, cols), bf16),
            pltpu.VMEM((n_z, 2 * ctx_tokens, 2 * cols), bf16),
            pltpu.VMEM((3, pairs, 2, 2 * nq, nk), f32),
            pltpu.VMEM((4, group_rows, GRID_W, cols), bf16),
            pltpu.VMEM((4, own_rows, GRID_W, cols), bf16),
            pltpu.VMEM((4, tokens, width), bf16),
            pltpu.VMEM((2, tokens, width), bf16),
            pltpu.VMEM((tokens, width), bf16),
            pltpu.VMEM((tokens, width), bf16),
            dma((11,)),
            dma((n_sp - 1,)), dma((n_sp - 1,)), dma((n_tp - 1,)), dma((n_tp - 1,)),
            dma((2,)), dma((2,)), dma((chunks,)), dma((chunks,)),
            dma((2, chunks)), dma((2, chunks)), dma((4, chunks)), dma((4, chunks)),
            dma((6,)), dma((n_z,)), dma((2,)), dma((2,)),
            dma((1,)), dma((1,)), dma((5,)), dma((5,)),
            dma((2, chunks)), dma((2, chunks)), dma((chunks,)), dma((chunks,)),
        ],
        compiler_params=pltpu.CompilerParams(
            collective_id=1, has_side_effects=True, vmem_limit_bytes=48 * 2**20
        ),
    )(
        *[
            pltpu.with_memory_space_constraint(v, pltpu.HBM)
            for v in (
                ctx_bias, rel_bias.transpose(1, 0, 2), norm_gain[None, :], cond, ctx_cond.reshape(-1, 128),
                w_shift, w_scale, w_gate, latent, context, w_query, w_key, w_value, w_out,
            )
        ]
    )
    return (latent.astype(f32) + delta).astype(bf16)


def solution(mesh):
    shape = dict(mesh.shape)
    quick = shape["tp"] == 4 and shape["sp"] == 8
    return jax.shard_map(
        on_eight if quick else on_device,
        mesh=mesh,
        in_specs=(
            P(None, ("sp", "tp"), None),
            P(None, "sp", None),
            P(),
            P(),
            P("sp", "tp"),
            P("sp", "tp"),
            P("sp", "tp"),
            P(),
            P(None, "tp"),
            P(None, "tp"),
            P(None, "tp"),
            P("tp", None),
            P("tp", None, None),
            P("tp"),
        ),
        out_specs=P(None, ("sp", "tp"), None),
        check_vma=False,
    )
```

```python
import functools

import jax
import jax.numpy as jnp
from jax import lax
from jax.experimental import pallas as pl
from jax.experimental.pallas import tpu as pltpu
from jax.sharding import PartitionSpec as P

HEAD_DIM = 64
GRID_W = 64
WIN_ROWS = 8
WIN_COLS = 16


EPSILON = 1e-06


def extended(shard, sides, width):
    for axis, dim in sides:
        size, length = (lax.axis_size(axis), shard.shape[dim])
        up = [(i, (i + 1) % size) for i in range(size - 1)]
        down = [(j, i) for i, j in up]
        last = lax.slice_in_dim(shard, length - width, length, axis=dim)
        first = lax.slice_in_dim(shard, 0, width, axis=dim)
        before = lax.ppermute(last, axis, up)
        after = lax.ppermute(first, axis, down)
        shard = jnp.concatenate([before, shard, after], axis=dim)
    return shard


def silu_rows(values):
    return jax.nn.silu(values.astype(jnp.float32)).astype(jnp.bfloat16)


def modulate_rows(rows, gain, shift, scale):
    floats = rows.astype(jnp.float32)
    inverse = lax.rsqrt(jnp.mean(floats * floats, axis=-1, keepdims=True) + EPSILON)
    return (floats * inverse * gain * (1.0 + scale) + shift).astype(jnp.bfloat16)

LOG2E = 1.4426950408889634


def attention_kernel(bias_ref, far_ref, q_ref, k_ref, v_ref, ck_ref, cv_ref, out_ref, table):
    pair = pl.program_id(0)
    rows_dev = q_ref.shape[1]
    padded = k_ref.shape[1]
    span = 2 * WIN_COLS
    half = WIN_COLS // 2
    reach = WIN_ROWS // 2
    nq, nk = rows_dev * WIN_COLS, padded * span
    lanes = 2 * HEAD_DIM

    @pl.when(pl.program_id(1) == 0)
    def _():
        sp = lax.axis_index("sp")
        rows_all = rows_dev * lax.axis_size("sp")
        at = lax.broadcasted_iota(jnp.int32, (WIN_COLS, nk), 1)
        p = lax.broadcasted_iota(jnp.int32, (WIN_COLS, nk), 0)
        key_row = sp * rows_dev - reach + at // span
        k = at % span
        inner = (k - p >= 0) & (k - p < WIN_COLS)
        edge = (p < half) == (k < WIN_COLS)
        for r in range(rows_dev):
            row = sp * rows_dev + r
            first = jnp.clip(row - reach, 0, rows_all - WIN_ROWS)
            inside = (key_row >= first) & (key_row < first + WIN_ROWS)
            shift = span * (r + reach - WIN_ROWS + 1) - half + 1
            for h in range(2):
                line = jnp.broadcast_to(bias_ref[0, h : h + 1, :], (WIN_COLS, nk))
                line = pltpu.roll(line, shift % nk, 1, stride=1, stride_axis=0) * LOG2E
                at_rows = pl.ds(r * WIN_COLS, WIN_COLS)
                table[h, 0, at_rows, :] = jnp.where(inside & edge, line, -jnp.inf)
                table[h, 1, at_rows, :] = jnp.where(inside & inner, line, -jnp.inf)

    factor = HEAD_DIM ** (-0.5) * LOG2E
    ck = ck_ref[...].reshape(-1, lanes)
    ctx_count = ck.shape[0]
    cv = jnp.concatenate([cv_ref[...].reshape(-1, lanes), jnp.ones((ctx_count, lanes), jnp.bfloat16)], axis=1)
    ones = jnp.ones((nk, lanes), jnp.bfloat16)
    low = lax.broadcasted_iota(jnp.int32, (nq, lanes), 1) < HEAD_DIM
    contract = (((1,), (1,)), ((), ()))
    every = q_ref[0].astype(jnp.float32)
    outs = []
    for block in range(GRID_W // WIN_COLS):
        if block == 0:
            q = jnp.concatenate([every[:, GRID_W - half :], every[:, :half]], axis=1)
        else:
            q = every[:, WIN_COLS * block - half : WIN_COLS * (block + 1) - half]
        q = q.astype(jnp.bfloat16).reshape(nq, lanes)

        def keys(ref):
            if block == 0:
                got = jnp.concatenate([ref[0, :, GRID_W - WIN_COLS :, :], ref[0, :, :WIN_COLS, :]], 1)
            else:
                got = ref[0, :, WIN_COLS * (block - 1) : WIN_COLS * (block + 1), :]
            return got.reshape(nk, lanes)

        k = keys(k_ref)
        v = jnp.concatenate([keys(v_ref), ones], axis=1)
        halves = []
        for h in range(2):
            mine = low if h == 0 else jnp.logical_not(low)
            one = jnp.where(mine, q, jnp.zeros_like(q))
            near = lax.dot_general(one, k, contract, preferred_element_type=jnp.float32)
            near = near * factor + table[h, min(block, 1)]
            far = lax.dot_general(one, ck, contract, preferred_element_type=jnp.float32)
            far = far * factor + far_ref[2 * pair + h] * LOG2E
            top = jnp.maximum(
                jnp.max(near, axis=-1, keepdims=True), jnp.max(far, axis=-1, keepdims=True)
            )
            near = jnp.exp2(near - top).astype(jnp.bfloat16)
            far = jnp.exp2(far - top).astype(jnp.bfloat16)
            got = jnp.dot(near, v, preferred_element_type=jnp.float32) + jnp.dot(
                far, cv, preferred_element_type=jnp.float32
            )
            halves.append(got[:, :lanes] / got[:, lanes:])
        outs.append(jnp.where(low, halves[0], halves[1]).reshape(rows_dev, WIN_COLS, lanes))
    outs = [outs[0][:, half:]] + outs[1:] + [outs[0][:, :half]]
    out_ref[0] = jnp.concatenate(outs, axis=1).astype(jnp.bfloat16)


def attention(query, pair, ctx_pair, rel_bias, ctx_bias):
    samples, rows_dev, _, cols = query.shape
    padded, ctx_count = pair.shape[1], ctx_pair.shape[0] * ctx_pair.shape[2]
    heads = cols // HEAD_DIM
    lanes = 2 * HEAD_DIM
    pairs = cols // lanes
    nq, nk = rows_dev * WIN_COLS, padded * 2 * WIN_COLS
    flat = jnp.pad(rel_bias, ((0, 0), (0, 1), (0, 1))).reshape(heads, -1)
    flat = jnp.pad(flat, ((0, 0), (0, nk - flat.shape[1]))).reshape(pairs, 2, nk)
    token = lambda at: pl.BlockSpec((1, padded, GRID_W, lanes), lambda p, s: (s, 0, 0, p + at))
    far = lambda at: pl.BlockSpec(
        (ctx_pair.shape[0], 1, ctx_pair.shape[2], lanes), lambda p, s: (0, s, 0, p + at)
    )
    own = pl.BlockSpec((1, rows_dev, GRID_W, lanes), lambda p, s: (s, 0, 0, p))
    scores = samples * heads * 4 * nq * (nk + ctx_count)
    return pl.pallas_call(
        attention_kernel,
        grid=(pairs, samples),
        out_shape=jax.ShapeDtypeStruct(query.shape, jnp.bfloat16),
        in_specs=[
            pl.BlockSpec((1, 2, nk), lambda p, s: (p, 0, 0)),
            pl.BlockSpec(memory_space=pltpu.SMEM),
            own,
            token(0),
            token(pairs),
            far(0),
            far(pairs),
        ],
        out_specs=own,
        scratch_shapes=[pltpu.VMEM((2, 2, nq, nk), jnp.float32)],
        cost_estimate=pl.CostEstimate(
            flops=scores * 512, bytes_accessed=8 * query.size * 2, transcendentals=scores
        ),
    )(flat, ctx_bias, query, pair, pair, ctx_pair, ctx_pair)


def on_device(
    latent,
    context,
    cond,
    ctx_cond,
    w_shift,
    w_scale,
    w_gate,
    norm_gain,
    w_query,
    w_key,
    w_value,
    w_out,
    rel_bias,
    ctx_bias,
):
    samples = latent.shape[0]
    rows_sp = w_shift.shape[0]
    local_cols = w_shift.shape[1]
    sp_index = lax.axis_index("sp")
    ada = silu_rows(jnp.concatenate([cond, ctx_cond[None, :]], axis=0))
    ada_rows = lax.dynamic_slice_in_dim(ada, sp_index * rows_sp, rows_sp, 1)
    partial_value = jnp.stack(
        [
            jnp.dot(ada_rows, weight, preferred_element_type=jnp.float32)
            for weight in (w_shift, w_scale, w_gate)
        ]
    )
    summed = lax.psum(partial_value, "sp")
    modulation = lax.all_gather(summed, "tp", axis=2, tiled=True)
    hidden = modulate_rows(
        latent, norm_gain, modulation[0, :samples, None, :], modulation[1, :samples, None, :]
    )
    w_triple = jnp.concatenate([w_query, w_key, w_value], axis=1)
    triple = jnp.dot(
        lax.all_gather(hidden, "tp", axis=1, tiled=True),
        w_triple,
        preferred_element_type=jnp.float32,
    ).astype(jnp.bfloat16)
    ctx_hidden = modulate_rows(context, norm_gain, modulation[0, samples], modulation[1, samples])
    w_pair = jnp.concatenate([w_key, w_value], axis=1)
    own_pair = jnp.dot(ctx_hidden, w_pair, preferred_element_type=jnp.float32).astype(jnp.bfloat16)
    ctx_pair = lax.all_gather(own_pair, "sp", axis=1, tiled=True)
    heads = local_cols // HEAD_DIM
    tokens_sp = triple.shape[1]
    rows_dev = tokens_sp // GRID_W
    rows_all = rows_dev * lax.axis_size("sp")
    reach = WIN_ROWS // 2
    query = triple[..., :local_cols].reshape(samples, rows_dev, GRID_W, local_cols)
    pair = triple[..., local_cols:].reshape(samples, rows_dev, GRID_W, 2 * local_cols)
    padded_pair = extended(pair, (("sp", 1),), reach)
    mixed = attention(query, padded_pair, ctx_pair[None], rel_bias, ctx_bias)
    attended = mixed.reshape(samples, tokens_sp, local_cols)
    attended = attended.transpose(1, 0, 2)
    update = lax.psum_scatter(
        jnp.einsum("tsc,cd->tsd", attended, w_out, preferred_element_type=jnp.float32).astype(
            jnp.bfloat16
        ),
        "tp",
        scatter_dimension=0,
        tiled=True,
    ).astype(jnp.float32)
    gate = modulation[2, :samples, None, :]
    result = latent.astype(jnp.float32) + gate * update.transpose(1, 0, 2)
    return result.astype(jnp.bfloat16)


MESH = pl.DeviceIdType.MESH


def block_kernel(
    far_hbm, bias_hbm, gain_hbm, cond_hbm, ctx_cond_hbm,
    ws_ref, wc_ref, wg_ref, latent_ref, ctx_ref, wq_ref, wk_ref, wv_ref, wo_ref,
    out_ref,
    far_ref, bias_ref, gain_ref, cond_ref, ctx_cond_ref, acc,
    flat, ada, wm, part, got, total, full, buf, other, cx, cs, wq, wkv, wo, kv, qs, ckv, table,
    att, att_in, parts, y_in, fwd, x_in,
    own_sem, s1, r1, s2, r2, s_c, r_c, s_x, r_x, s_y, r_y, s_d, r_d, s_z, r_z, s_h, r_h,
    s_w, r_w, s_a, r_a, s_p, r_p, s_f, r_f,
):
    sp, tp = lax.axis_index("sp"), lax.axis_index("tp")
    n_sp, n_tp = lax.axis_size("sp"), lax.axis_size("tp")
    y, c = tp // 2, lax.rem(tp, 2)
    z, x = sp // 2, lax.rem(sp, 2)
    n_z = n_sp // 2
    same = x == y
    differs = x != y
    tokens, width = other.shape
    cols = wq.shape[1]
    rows_mod = wm.shape[1]
    lanes = 2 * HEAD_DIM
    pairs = cols // lanes
    half = WIN_COLS // 2
    reach = WIN_ROWS // 2
    own_rows = tokens // GRID_W
    group_rows = 2 * own_rows
    layer_rows = 4 * group_rows
    chunks = s_x.shape[0]
    size = tokens // chunks
    over_sp = [lax.rem(sp + k, n_sp) for k in range(1, n_sp)]
    over_tp = [lax.rem(tp + k, n_tp) for k in range(1, n_tp)]
    sib, across = (sp, tp + 1 - 2 * c), (sp, (1 - y) * 2 + c)
    beside = (sp + 1 - 2 * x, tp)
    g_own, g_x, g_y, g_d = 2 * x + y, 2 * (1 - x) + y, 2 * x + 1 - y, 2 * (1 - x) + 1 - y
    drain = []

    def remote(src, dst, s, r, device):
        return pltpu.make_async_remote_copy(
            src_ref=src, dst_ref=dst, send_sem=s, recv_sem=r, device_id=device, device_id_type=MESH
        )

    def begin(make, cond=None):
        drain.append((make, cond))
        if cond is None:
            make().start()
        else:
            @pl.when(cond)
            def _():
                make().start()

    def local(k, src, dst):
        copy = pltpu.make_async_copy(src, dst, own_sem.at[k])
        copy.start()
        return copy

    small_copies = [
        local(11 + k, src, dst)
        for k, (src, dst) in enumerate((
            (cond_hbm, cond_ref), (ctx_cond_hbm, ctx_cond_ref), (bias_hbm, bias_ref),
            (gain_hbm, gain_ref), (far_hbm, far_ref),
        ))
    ]
    mod_copies = [local(k, w, wm.at[k]) for k, w in enumerate((ws_ref, wc_ref, wg_ref))]
    other_copy = local(3, latent_ref.at[1 - x], other)
    own_copy = local(4, latent_ref.at[x], buf.at[2 * g_own + c])
    ctx_half = cs.shape[0]
    ctx_part = lambda k: pl.ds(pl.multiple_of(k * ctx_half, ctx_half), ctx_half)
    stage_copy = local(5, ctx_ref.at[1 - x, ctx_part(c)], cs)
    ctx_copy = local(6, ctx_ref.at[x], cx.at[x])
    weight_copies = [
        local(7, wk_ref, wkv.at[:, pl.ds(0, cols)]),
        local(8, wv_ref, wkv.at[:, pl.ds(cols, cols)]),
        local(9, wq_ref, wq),
        local(10, wo_ref, wo.at[0]),
    ]
    barrier = pltpu.get_barrier_semaphore()
    peers = [(p, tp) for p in over_sp] + [(sp, p) for p in over_tp]
    for device in peers:
        pl.semaphore_signal(barrier, inc=1, device_id=device, device_id_type=MESH)

    def piece(g, h):
        return buf.at[2 * g + c, pl.ds(h * size, size)]

    def to_beside(h):
        return remote(other.at[pl.ds(h * size, size)], piece(g_own, h), s_x.at[h], r_x.at[h], beside)

    def from_beside(h):
        return remote(other.at[pl.ds(h * size, size)], piece(g_x, h), s_x.at[h], r_x.at[h], beside)

    def over_y(g, flow, h):
        return remote(piece(g, h), piece(g, h), s_y.at[flow, h], r_y.at[flow, h], across)

    def to_sib(k, g, h):
        return remote(piece(g, h), piece(g, h), s_d.at[k, h], r_d.at[k, h], sib)

    def from_sib(k, g, h):
        there = buf.at[2 * g + 1 - c, pl.ds(h * size, size)]
        return remote(there, there, s_d.at[k, h], r_d.at[k, h], sib)

    mine = pl.ds(pl.multiple_of(sp * rows_mod, rows_mod), rows_mod)
    small_copies[0].wait()
    small_copies[1].wait()
    ada[...] = jnp.zeros_like(ada)
    ada[0:2, :] = cond_ref[:, mine].astype(jnp.float32)
    ctx_cond = ctx_cond_ref[...].astype(jnp.float32)
    for k in range(n_sp):
        @pl.when(sp == k)
        def _():
            for j in range(rows_mod // 128):
                line = k * (rows_mod // 128) + j
                ada[2:3, 128 * j : 128 * (j + 1)] = ctx_cond[line : line + 1, :]
    values = ada[...]
    values = (values / (1.0 + jnp.exp(-values))).astype(jnp.bfloat16)
    at = 0
    for k, count in enumerate((3, 3, 2)):
        mod_copies[k].wait()
        value = jnp.dot(values, wm[k], preferred_element_type=jnp.float32)
        part[at : at + count, :] = value[:count]
        at += count
    stage_copy.wait()
    other_copy.wait()
    own_copy.wait()
    pl.semaphore_wait(barrier, len(peers))
    for k, peer in enumerate(over_sp):
        begin(functools.partial(remote, part, got.at[k], s1.at[k], r1.at[k], (peer, tp)))

    begin(lambda: remote(cs, cx.at[x, ctx_part(c)], s_c.at[0], r_c.at[0], beside))
    upfront, between = 3 * chunks // 8, 5 * chunks // 8
    for h in range(chunks):
        if h < upfront:
            begin(functools.partial(over_y, g_own, 0, h))
        begin(functools.partial(to_beside, h))
    for h in range(chunks):
        begin(functools.partial(to_sib, 0, g_own, h))

    span = 2 * WIN_COLS
    nk = table.shape[-1]
    nq = table.shape[-2] // 2
    rows_all = layer_rows * n_z
    lane = lax.broadcasted_iota(jnp.int32, (WIN_COLS, nk), 1)
    p = lax.broadcasted_iota(jnp.int32, (WIN_COLS, nk), 0)
    k_row, k_col = lane // span, lane % span
    inner = (k_col - p >= 0) & (k_col - p < WIN_COLS)
    edge = (p < half) == (k_col < WIN_COLS)

    small_copies[2].wait()
    flat[...] = jnp.zeros_like(flat)
    for k in range(bias_ref.shape[0]):
        flat[:, span * k : span * k + bias_ref.shape[2]] = bias_ref[k]

    def tables(pair, carry):
        for h in range(2):
            line = flat[pl.ds(2 * pair + h, 1), :]
            line = jnp.broadcast_to(line, (WIN_COLS, line.shape[1]))
            for r in range(group_rows):
                shift = (span * (r + reach - WIN_ROWS + 1) - half + 1) % line.shape[1]
                rolled = pltpu.roll(line, shift, 1, stride=1, stride_axis=0)[:, :nk] * LOG2E
                at_rows = pl.ds(h * nq + r * WIN_COLS, WIN_COLS)
                for kind in range(3):
                    row = z * layer_rows + r + (0, 0, layer_rows - group_rows)[kind]
                    first = row - reach
                    if kind:
                        first = jnp.clip(first, 0, rows_all - WIN_ROWS)
                    key_row = k_row + (row - r - reach)
                    inside = (key_row >= first) & (key_row < first + WIN_ROWS)
                    table[kind, pair, 0, at_rows, :] = jnp.where(inside & edge, rolled, -jnp.inf)
                    table[kind, pair, 1, at_rows, :] = jnp.where(inside & inner, rolled, -jnp.inf)
        return carry

    last_row = kv.shape[0] - 1
    kv[last_row] = jnp.zeros(kv.shape[1:], jnp.bfloat16)

    @pl.when(z == 0)
    def _():
        kv[0:reach] = jnp.zeros((reach,) + kv.shape[1:], jnp.bfloat16)

    @pl.when(z == n_z - 1)
    def _():
        kv[last_row - reach + 1 : last_row] = jnp.zeros((reach - 1,) + kv.shape[1:], jnp.bfloat16)

    lax.fori_loop(0, pairs // 2, tables, 0)

    value = part[...]
    for k, peer in enumerate(over_sp):
        remote(part, got.at[k], s1.at[k], r1.at[k], (peer, tp)).wait_recv()
        value = value + got[k]
    total[...] = value
    columns = pl.ds(pl.multiple_of(tp * cols, cols), cols)
    full[:, columns] = value
    for k, peer in enumerate(over_tp):
        begin(
            functools.partial(remote, total, full.at[:, columns], s2.at[k], r2.at[k], (sp, peer))
        )
    for h in range(upfront, between):
        begin(functools.partial(over_y, g_own, 0, h))

    def rest_own():
        for h in range(between, chunks):
            over_y(g_own, 0, h).start()

    for h in range(between, chunks):
        drain.append((functools.partial(over_y, g_own, 0, h), None))

    @pl.when(same)
    def _():
        rest_own()

    remote(cs, cx.at[1 - x, ctx_part(c)], s_c.at[0], r_c.at[0], beside).wait_recv()
    ctx_sib = lambda k: remote(
        cx.at[1 - x, ctx_part(k)], cx.at[1 - x, ctx_part(k)], s_c.at[1], r_c.at[1], sib
    )
    begin(lambda: ctx_sib(c))
    lax.fori_loop(pairs // 2, pairs, tables, 0)
    def relay(h):
        from_beside(h).wait_recv()
        over_y(g_x, 1, h).start()
        to_sib(1, g_x, h).start()

    for h in range(chunks):
        drain.append((functools.partial(over_y, g_x, 1, h), None))
        drain.append((functools.partial(to_sib, 1, g_x, h), None))
    relay(0)
    ctx_copy.wait()
    ctx_sib(1 - c).wait_recv()
    for copy in weight_copies + small_copies[3:]:
        copy.wait()
    for k, peer in enumerate(over_tp):
        there = pl.ds(pl.multiple_of(peer * cols, cols), cols)
        remote(total, full.at[:, there], s2.at[k], r2.at[k], (sp, peer)).wait_recv()
    begin(lambda: remote(wo.at[0], wo.at[1], s_w.at[0], r_w.at[0], sib))

    def normed(rows, which):
        rows = rows.astype(jnp.float32)
        inverse = lax.rsqrt(jnp.mean(rows * rows, axis=-1, keepdims=True) + EPSILON)
        lift = gain_ref[...] * (1.0 + full[pl.ds(3 + which, 1), :])
        return (rows * inverse * lift + full[pl.ds(which, 1), :]).astype(jnp.bfloat16)

    hidden = jnp.concatenate([normed(cx[0], 2), normed(cx[1], 2)], axis=0)
    ckv[z] = jnp.dot(hidden, wkv[...], preferred_element_type=jnp.float32).astype(jnp.bfloat16)

    def layer_copy(zb, k, up):
        return remote(ckv.at[zb], ckv.at[zb], s_z.at[k], r_z.at[zb], (sp + 2 * up, tp))

    layer_sends = []
    for k, up in enumerate((2, -2, 1, -1)):
        ahead = (z + up >= 0) & (z + up < n_z)
        middle = (z > 0) & (z + 1 < n_z - 1) if up > 0 else (z < n_z - 1) & (z - 1 > 0)
        layer_sends.append((functools.partial(layer_copy, z, k, up), ahead, middle))
        drain.append((functools.partial(layer_copy, z, k, up), ahead))

    def send_layer(late):
        for make, ahead, middle in layer_sends:
            @pl.when(ahead & (middle if late else jnp.logical_not(middle)))
            def _():
                make().start()

    send_layer(False)
    relay(1)
    far_up, far_down = z == n_z - 2, z == 1
    relays = far_up | far_down

    def ctx_relay():
        for cond, zb, k, up in ((far_up, 0, 4, 1), (far_down, n_z - 1, 5, -1)):
            @pl.when(cond)
            def _():
                layer_copy(zb, k, up).wait_recv()
                layer_copy(zb, k, up).start()

    drain.append((functools.partial(layer_copy, 0, 4, 1), far_up))
    drain.append((functools.partial(layer_copy, n_z - 1, 5, -1), far_down))

    g_third = jnp.where(same, g_d, g_y)
    g_fourth = jnp.where(same, g_y, g_d)
    has_up, has_down = z < n_z - 1, z > 0
    halo_up = lambda: remote(
        kv.at[pl.ds(layer_rows, reach)], kv.at[pl.ds(0, reach)], s_h.at[0], r_h.at[0], (sp + 2, tp)
    )
    halo_down = lambda: remote(
        kv.at[pl.ds(reach, reach - 1)], kv.at[pl.ds(reach + layer_rows, reach - 1)],
        s_h.at[1], r_h.at[1], (sp - 2, tp),
    )

    def incoming(k, flow, g, cond):
        @pl.when(cond)
        def _():
            for h in range(chunks):
                over_y(g, flow, h).wait_recv()
                to_sib(k, g, h).start()

    def shared(k, g, cond):
        @pl.when(cond)
        def _():
            for h in range(chunks):
                from_sib(k, g, h).wait_recv()

    for h in range(chunks):
        drain.append((functools.partial(to_sib, 2, g_y, h), None))
        drain.append((functools.partial(to_sib, 3, g_d, h), None))

    def before(k):
        if k == 0:
            for h in range(chunks):
                from_sib(0, g_own, h).wait_recv()
        if k == 1:
            for h in range(2, chunks):
                relay(h)

            @pl.when(differs)
            def _():
                rest_own()

            send_layer(True)
            incoming(2, 0, g_y, differs)
            for h in range(chunks):
                from_sib(1, g_x, h).wait_recv()
        if k == 2:
            ctx_relay()

            @pl.when(relays & has_down & differs & (g_x == 0))
            def _():
                halo_down().start()

            @pl.when(relays & has_up & differs & (g_x == 3))
            def _():
                halo_up().start()

            @pl.when(relays & has_down & same & (g_own == 0))
            def _():
                halo_down().start()

            @pl.when(relays & has_up & same & (g_own == 3))
            def _():
                halo_up().start()

            incoming(3, 1, g_d, same)
            shared(2, g_y, differs)
            shared(3, g_d, same)
        if k == 3:
            incoming(2, 0, g_y, same)
            incoming(3, 1, g_d, differs)
            shared(2, g_y, same)
            shared(3, g_d, differs)

    def project(i, carry):
        for k in range(4):
            @pl.when(i == k)
            def _():
                before(k)

        g = jnp.where(i == 0, g_own, jnp.where(i == 1, g_x, jnp.where(i == 2, g_third, g_fourth)))
        hidden = jnp.concatenate([normed(buf[2 * g + e], x) for e in range(2)], axis=0)
        value = jnp.dot(hidden, wkv[...], preferred_element_type=jnp.float32).astype(jnp.bfloat16)
        kv[pl.ds(reach + group_rows * g, group_rows)] = value.reshape(group_rows, GRID_W, 2 * cols)
        query = jnp.dot(hidden, wq[...], preferred_element_type=jnp.float32)
        query = query.reshape(group_rows, GRID_W, cols)
        query = jnp.concatenate([query[:, GRID_W - half :], query[:, : GRID_W - half]], axis=1)
        qs[pl.ds(group_rows * g, group_rows)] = query.astype(jnp.bfloat16)

        open_now = jnp.logical_not(relays) | (i >= 2)

        @pl.when((g == 0) & has_down & open_now)
        def _():
            halo_down().start()

        @pl.when((g == 3) & has_up & open_now)
        def _():
            halo_up().start()

        return carry

    lax.fori_loop(0, 4, project, 0)
    drain.append((halo_down, has_down))
    drain.append((halo_up, has_up))

    for k in range(1, n_z):
        zb = lax.rem(z + k, n_z)
        done = (far_up & (zb == 0)) | (far_down & (zb == n_z - 1))

        @pl.when(jnp.logical_not(done))
        def _():
            layer_copy(zb, 0, 1).wait_recv()

    remote(wo.at[0], wo.at[1], s_w.at[0], r_w.at[0], sib).wait_recv()

    factor = HEAD_DIM ** (-0.5) * LOG2E
    contract = (((1,), (1,)), ((), ()))
    low = lax.broadcasted_iota(jnp.int32, (nq, lanes), 1) < HEAD_DIM
    first_head = lax.broadcasted_iota(jnp.int32, (2 * nq, 1), 0) < nq
    key_rows = nk // span
    ctx_count = ckv.shape[0] * ckv.shape[1]

    def attend(i, g, pair, blocks):
        own = pl.ds(pl.multiple_of(pair * lanes, lanes), lanes)
        values_at = pl.ds(pl.multiple_of(cols + pair * lanes, lanes), lanes)
        rows = pl.ds(group_rows * g, key_rows)
        kind = jnp.where(g == 0, 1, jnp.where(g == 3, 2, 0))
        ck = ckv[:, :, own].reshape(ctx_count, lanes)
        cv = ckv[:, :, values_at].reshape(ctx_count, lanes)
        cv = jnp.concatenate([cv, jnp.ones((ctx_count, lanes), jnp.bfloat16)], axis=1)
        ones = jnp.ones((nk, lanes), jnp.bfloat16)
        lift = jnp.where(first_head, far_ref[2 * pair], far_ref[2 * pair + 1]) * LOG2E
        for b in blocks:
            q = qs[pl.ds(group_rows * g, group_rows), WIN_COLS * b : WIN_COLS * (b + 1), own]
            q = q.reshape(nq, lanes)
            zero = jnp.zeros_like(q)
            q = jnp.concatenate([jnp.where(low, q, zero), jnp.where(low, zero, q)], axis=0)

            def keys(part_at):
                if b == 0:
                    got = jnp.concatenate(
                        [kv[rows, GRID_W - WIN_COLS :, part_at], kv[rows, :WIN_COLS, part_at]], axis=1
                    )
                else:
                    got = kv[rows, WIN_COLS * (b - 1) : WIN_COLS * (b + 1), part_at]
                return got.reshape(nk, lanes)

            v = jnp.concatenate([keys(values_at), ones], axis=1)
            near = lax.dot_general(q, keys(own), contract, preferred_element_type=jnp.float32)
            near = near * factor + table[kind, pair, min(b, 1)]
            far = lax.dot_general(q, ck, contract, preferred_element_type=jnp.float32)
            top = jnp.maximum(
                jnp.max(near, axis=-1, keepdims=True),
                jnp.max(far, axis=-1, keepdims=True) * factor + lift,
            )
            near = jnp.exp2(near - top).astype(jnp.bfloat16)
            far = jnp.exp2(far * factor + (lift - top)).astype(jnp.bfloat16)
            summed = jnp.dot(near, v, preferred_element_type=jnp.float32) + jnp.dot(
                far, cv, preferred_element_type=jnp.float32
            )
            mean = summed[:, :lanes] / summed[:, lanes:]
            mean = jnp.where(low, mean[:nq], mean[nq:]).reshape(group_rows, WIN_COLS, lanes)
            att[i, :, WIN_COLS * b : WIN_COLS * (b + 1), own] = mean.astype(jnp.bfloat16)

    def give(i, batch, begins, count):
        at = pl.ds(begins, count)
        return remote(
            att.at[i, pl.ds(own_rows * (1 - c), own_rows), at], att_in.at[i, :, at],
            s_a.at[batch], r_a.at[batch], sib,
        )

    def to_across(i, slot, h):
        part_at = pl.ds(pl.multiple_of(h * size, size), size)
        return remote(
            parts.at[i, part_at], y_in.at[slot, part_at], s_p.at[slot, h], r_p.at[slot, h], across
        )

    def chunk(h):
        return pl.ds(pl.multiple_of(h * size, size), size)

    def to_owner(h):
        return remote(fwd.at[chunk(h)], x_in.at[chunk(h)], s_f.at[h], r_f.at[h], beside)

    def sum_at(i, slot, h):
        return parts[i, chunk(h)].astype(jnp.float32) + y_in[slot, chunk(h)].astype(jnp.float32)

    def forward(slot, h):
        to_across(slot, slot, h).wait_recv()
        fwd[chunk(h)] = sum_at(2, slot, h).astype(jnp.bfloat16)
        to_owner(h).start()

    def group_of(i):
        first = jnp.where(y == 0, 1, 2)
        return jnp.where(i == 0, first, jnp.where(i == 1, 3 * (1 - y), jnp.where(i == 2, g_x, g_own)))

    def attention_block(i, batch, begins, count, between_pairs=None):
        g = group_of(i)
        blocks = range(begins // WIN_COLS, (begins + count) // WIN_COLS)

        if between_pairs is None:
            for pair in range(pairs):
                attend(i, g, pair, blocks)
        else:
            def one(pair, carry):
                attend(i, g, pair, blocks)
                between_pairs(pair)
                return carry

            lax.fori_loop(0, pairs, one, 0)
        give(i, batch, begins, count).start()
        at = pl.ds(begins, count)
        acc[: own_rows * count] = jnp.dot(
            att[i, pl.ds(own_rows * c, own_rows), at].reshape(own_rows * count, cols), wo[0],
            preferred_element_type=jnp.float32,
        )
        give(i, batch, begins, count).wait_recv()
        update = acc[: own_rows * count] + jnp.dot(
            att_in[i, :, at].reshape(own_rows * count, cols), wo[1], preferred_element_type=jnp.float32
        )
        for r in range(own_rows):
            parts[i, GRID_W * r + begins : GRID_W * r + begins + count] = update[
                count * r : count * (r + 1)
            ].astype(jnp.bfloat16)

    per_row = chunks // own_rows
    for part_of in range(2):
        attention_block(0, part_of, GRID_W // 2 * part_of, GRID_W // 2)
        for r in range(own_rows):
            for k in range(per_row // 2):
                to_across(0, 0, per_row * r + per_row // 2 * part_of + k).start()

    def wait_halo(g):
        @pl.when((g == 0) & has_down)
        def _():
            there = kv.at[pl.ds(0, reach)]
            remote(there, there, s_h.at[0], r_h.at[0], (sp - 2, tp)).wait_recv()

        @pl.when((g == 3) & has_up)
        def _():
            there = kv.at[pl.ds(reach + layer_rows, reach - 1)]
            remote(there, there, s_h.at[1], r_h.at[1], (sp + 2, tp)).wait_recv()

    def attention_step(i, carry):
        g = group_of(i)

        wait_halo(g)
        attention_block(i, i + 1, 0, GRID_W)

        @pl.when(i == 1)
        def _():
            for h in range(chunks):
                to_across(1, 1, h).start()

        return carry

    lax.fori_loop(1, 3, attention_step, 0)
    early = chunks - 2 - pairs

    @pl.when(same)
    def _():
        for h in range(chunks):
            forward(0, h)

    @pl.when(differs)
    def _():
        for h in range(early):
            forward(1, h)

    def between_pairs(pair):
        @pl.when(differs)
        def _():
            forward(1, early + pair)

    wait_halo(g_own)
    attention_block(3, 4, 0, GRID_W, between_pairs)
    for part_of in range(2):
        drain.append((functools.partial(give, 0, part_of, GRID_W // 2 * part_of, GRID_W // 2), None))
    for i in range(1, 4):
        drain.append((functools.partial(give, i, i + 1, 0, GRID_W), None))

    def finish(which, h, update):
        value = full[pl.ds(6 + which, 1), :] * update
        row, place = GRID_W * (h // per_row), size * (h % per_row)
        if place == 0:
            out_ref[which, row + GRID_W - half : row + GRID_W] = value[:half]
            out_ref[which, row : row + size - half] = value[half:]
        else:
            out_ref[which, row + place - half : row + place - half + size] = value

    def own(slot):
        for h in range(chunks):
            to_across(slot, slot, h).wait_recv()
            finish(x, h, sum_at(3, slot, h))

    @pl.when(differs)
    def _():
        for h in range(early + pairs, chunks):
            forward(1, h)
        own(0)

    @pl.when(same)
    def _():
        own(1)

    for h in range(chunks):
        to_owner(h).wait_recv()
        finish(1 - x, h, x_in[h * size : (h + 1) * size].astype(jnp.float32))
        drain.append((functools.partial(to_owner, h), None))
        for slot in range(2):
            drain.append((functools.partial(to_across, slot, slot, h), None))

    for make, cond in drain:
        if cond is None:
            make().wait_send()
        else:
            @pl.when(cond)
            def _():
                make().wait_send()


def on_eight(
    latent, context, cond, ctx_cond, w_shift, w_scale, w_gate, norm_gain,
    w_query, w_key, w_value, w_out, rel_bias, ctx_bias,
):
    n_sp, n_tp = lax.axis_size("sp"), lax.axis_size("tp")
    samples, tokens, width = latent.shape
    ctx_tokens = context.shape[1]
    rows_mod, cols = w_shift.shape
    heads = cols // HEAD_DIM
    pairs = heads // 2
    n_z = n_sp // 2
    own_rows = tokens // GRID_W
    group_rows = 2 * own_rows
    layer_rows = 4 * group_rows
    key_rows = group_rows + WIN_ROWS
    nq, nk = group_rows * WIN_COLS, key_rows * 2 * WIN_COLS
    vmem, hbm = pl.BlockSpec(memory_space=pltpu.VMEM), pl.BlockSpec(memory_space=pltpu.HBM)
    dma = pltpu.SemaphoreType.DMA
    chunks = 8
    bf16, f32 = jnp.bfloat16, jnp.float32
    mods = (8, cols)
    delta = pl.pallas_call(
        block_kernel,
        out_shape=jax.ShapeDtypeStruct(latent.shape, f32),
        in_specs=[hbm] * 14,
        out_specs=vmem,
        scratch_shapes=[
            pltpu.SMEM(ctx_bias.shape, f32),
            pltpu.VMEM((rel_bias.shape[1], heads, rel_bias.shape[2]), f32),
            pltpu.VMEM((1, width), f32),
            pltpu.VMEM(cond.shape, bf16),
            pltpu.VMEM((width // 128, 128), bf16),
            pltpu.VMEM((tokens, width), f32),
            pltpu.VMEM((heads, 2 * WIN_ROWS * 2 * WIN_COLS), f32),
            pltpu.VMEM((8, rows_mod), f32),
            pltpu.VMEM((3, rows_mod, cols), bf16),
            pltpu.VMEM(mods, f32),
            pltpu.VMEM((n_sp - 1,) + mods, f32),
            pltpu.VMEM(mods, f32),
            pltpu.VMEM((8, width), f32),
            pltpu.VMEM((8, tokens, width), bf16),
            pltpu.VMEM((tokens, width), bf16),
            pltpu.VMEM((2, ctx_tokens, width), bf16),
            pltpu.VMEM((ctx_tokens // 2, width), bf16),
            pltpu.VMEM((width, cols), bf16),
            pltpu.VMEM((width, 2 * cols), bf16),
            pltpu.VMEM((2, cols, width), bf16),
            pltpu.VMEM((layer_rows + WIN_ROWS, GRID_W, 2 * cols), bf16),
            pltpu.VMEM((layer_rows, GRID_W, cols), bf16),
            pltpu.VMEM((n_z, 2 * ctx_tokens, 2 * cols), bf16),
            pltpu.VMEM((3, pairs, 2, 2 * nq, nk), f32),
            pltpu.VMEM((4, group_rows, GRID_W, cols), bf16),
            pltpu.VMEM((4, own_rows, GRID_W, cols), bf16),
            pltpu.VMEM((4, tokens, width), bf16),
            pltpu.VMEM((2, tokens, width), bf16),
            pltpu.VMEM((tokens, width), bf16),
            pltpu.VMEM((tokens, width), bf16),
            dma((16,)),
            dma((n_sp - 1,)), dma((n_sp - 1,)), dma((n_tp - 1,)), dma((n_tp - 1,)),
            dma((2,)), dma((2,)), dma((chunks,)), dma((chunks,)),
            dma((2, chunks)), dma((2, chunks)), dma((4, chunks)), dma((4, chunks)),
            dma((6,)), dma((n_z,)), dma((2,)), dma((2,)),
            dma((1,)), dma((1,)), dma((5,)), dma((5,)),
            dma((2, chunks)), dma((2, chunks)), dma((chunks,)), dma((chunks,)),
        ],
        compiler_params=pltpu.CompilerParams(
            collective_id=1, has_side_effects=True, vmem_limit_bytes=48 * 2**20
        ),
    )(
        *[
            pltpu.with_memory_space_constraint(v, pltpu.HBM)
            for v in (
                ctx_bias, rel_bias.transpose(1, 0, 2), norm_gain[None, :], cond, ctx_cond.reshape(-1, 128),
                w_shift, w_scale, w_gate, latent, context, w_query, w_key, w_value, w_out,
            )
        ]
    )
    return (latent.astype(f32) + delta).astype(bf16)


def solution(mesh):
    shape = dict(mesh.shape)
    quick = shape["tp"] == 4 and shape["sp"] == 8
    return jax.shard_map(
        on_eight if quick else on_device,
        mesh=mesh,
        in_specs=(
            P(None, ("sp", "tp"), None),
            P(None, "sp", None),
            P(),
            P(),
            P("sp", "tp"),
            P("sp", "tp"),
            P("sp", "tp"),
            P(),
            P(None, "tp"),
            P(None, "tp"),
            P(None, "tp"),
            P("tp", None),
            P("tp", None, None),
            P("tp"),
        ),
        out_specs=P(None, ("sp", "tp"), None),
        check_vma=False,
    )
```

```python
import functools

import jax
import jax.numpy as jnp
from jax import lax
from jax.experimental import pallas as pl
from jax.experimental.pallas import tpu as pltpu
from jax.sharding import PartitionSpec as P

HEAD_DIM = 64
GRID_W = 64
WIN_ROWS = 8
WIN_COLS = 16


EPSILON = 1e-06


def extended(shard, sides, width):
    for axis, dim in sides:
        size, length = (lax.axis_size(axis), shard.shape[dim])
        up = [(i, (i + 1) % size) for i in range(size - 1)]
        down = [(j, i) for i, j in up]
        last = lax.slice_in_dim(shard, length - width, length, axis=dim)
        first = lax.slice_in_dim(shard, 0, width, axis=dim)
        before = lax.ppermute(last, axis, up)
        after = lax.ppermute(first, axis, down)
        shard = jnp.concatenate([before, shard, after], axis=dim)
    return shard


def silu_rows(values):
    return jax.nn.silu(values.astype(jnp.float32)).astype(jnp.bfloat16)


def modulate_rows(rows, gain, shift, scale):
    floats = rows.astype(jnp.float32)
    inverse = lax.rsqrt(jnp.mean(floats * floats, axis=-1, keepdims=True) + EPSILON)
    return (floats * inverse * gain * (1.0 + scale) + shift).astype(jnp.bfloat16)

LOG2E = 1.4426950408889634


def attention_kernel(bias_ref, far_ref, q_ref, k_ref, v_ref, ck_ref, cv_ref, out_ref, table):
    pair = pl.program_id(0)
    rows_dev = q_ref.shape[1]
    padded = k_ref.shape[1]
    span = 2 * WIN_COLS
    half = WIN_COLS // 2
    reach = WIN_ROWS // 2
    nq, nk = rows_dev * WIN_COLS, padded * span
    lanes = 2 * HEAD_DIM

    @pl.when(pl.program_id(1) == 0)
    def _():
        sp = lax.axis_index("sp")
        rows_all = rows_dev * lax.axis_size("sp")
        at = lax.broadcasted_iota(jnp.int32, (WIN_COLS, nk), 1)
        p = lax.broadcasted_iota(jnp.int32, (WIN_COLS, nk), 0)
        key_row = sp * rows_dev - reach + at // span
        k = at % span
        inner = (k - p >= 0) & (k - p < WIN_COLS)
        edge = (p < half) == (k < WIN_COLS)
        for r in range(rows_dev):
            row = sp * rows_dev + r
            first = jnp.clip(row - reach, 0, rows_all - WIN_ROWS)
            inside = (key_row >= first) & (key_row < first + WIN_ROWS)
            shift = span * (r + reach - WIN_ROWS + 1) - half + 1
            for h in range(2):
                line = jnp.broadcast_to(bias_ref[0, h : h + 1, :], (WIN_COLS, nk))
                line = pltpu.roll(line, shift % nk, 1, stride=1, stride_axis=0) * LOG2E
                at_rows = pl.ds(r * WIN_COLS, WIN_COLS)
                table[h, 0, at_rows, :] = jnp.where(inside & edge, line, -jnp.inf)
                table[h, 1, at_rows, :] = jnp.where(inside & inner, line, -jnp.inf)

    factor = HEAD_DIM ** (-0.5) * LOG2E
    ck = ck_ref[...].reshape(-1, lanes)
    ctx_count = ck.shape[0]
    cv = jnp.concatenate([cv_ref[...].reshape(-1, lanes), jnp.ones((ctx_count, lanes), jnp.bfloat16)], axis=1)
    ones = jnp.ones((nk, lanes), jnp.bfloat16)
    low = lax.broadcasted_iota(jnp.int32, (nq, lanes), 1) < HEAD_DIM
    contract = (((1,), (1,)), ((), ()))
    every = q_ref[0].astype(jnp.float32)
    outs = []
    for block in range(GRID_W // WIN_COLS):
        if block == 0:
            q = jnp.concatenate([every[:, GRID_W - half :], every[:, :half]], axis=1)
        else:
            q = every[:, WIN_COLS * block - half : WIN_COLS * (block + 1) - half]
        q = q.astype(jnp.bfloat16).reshape(nq, lanes)

        def keys(ref):
            if block == 0:
                got = jnp.concatenate([ref[0, :, GRID_W - WIN_COLS :, :], ref[0, :, :WIN_COLS, :]], 1)
            else:
                got = ref[0, :, WIN_COLS * (block - 1) : WIN_COLS * (block + 1), :]
            return got.reshape(nk, lanes)

        k = keys(k_ref)
        v = jnp.concatenate([keys(v_ref), ones], axis=1)
        halves = []
        for h in range(2):
            mine = low if h == 0 else jnp.logical_not(low)
            one = jnp.where(mine, q, jnp.zeros_like(q))
            near = lax.dot_general(one, k, contract, preferred_element_type=jnp.float32)
            near = near * factor + table[h, min(block, 1)]
            far = lax.dot_general(one, ck, contract, preferred_element_type=jnp.float32)
            far = far * factor + far_ref[2 * pair + h] * LOG2E
            top = jnp.maximum(
                jnp.max(near, axis=-1, keepdims=True), jnp.max(far, axis=-1, keepdims=True)
            )
            near = jnp.exp2(near - top).astype(jnp.bfloat16)
            far = jnp.exp2(far - top).astype(jnp.bfloat16)
            got = jnp.dot(near, v, preferred_element_type=jnp.float32) + jnp.dot(
                far, cv, preferred_element_type=jnp.float32
            )
            halves.append(got[:, :lanes] / got[:, lanes:])
        outs.append(jnp.where(low, halves[0], halves[1]).reshape(rows_dev, WIN_COLS, lanes))
    outs = [outs[0][:, half:]] + outs[1:] + [outs[0][:, :half]]
    out_ref[0] = jnp.concatenate(outs, axis=1).astype(jnp.bfloat16)


def attention(query, pair, ctx_pair, rel_bias, ctx_bias):
    samples, rows_dev, _, cols = query.shape
    padded, ctx_count = pair.shape[1], ctx_pair.shape[0] * ctx_pair.shape[2]
    heads = cols // HEAD_DIM
    lanes = 2 * HEAD_DIM
    pairs = cols // lanes
    nq, nk = rows_dev * WIN_COLS, padded * 2 * WIN_COLS
    flat = jnp.pad(rel_bias, ((0, 0), (0, 1), (0, 1))).reshape(heads, -1)
    flat = jnp.pad(flat, ((0, 0), (0, nk - flat.shape[1]))).reshape(pairs, 2, nk)
    token = lambda at: pl.BlockSpec((1, padded, GRID_W, lanes), lambda p, s: (s, 0, 0, p + at))
    far = lambda at: pl.BlockSpec(
        (ctx_pair.shape[0], 1, ctx_pair.shape[2], lanes), lambda p, s: (0, s, 0, p + at)
    )
    own = pl.BlockSpec((1, rows_dev, GRID_W, lanes), lambda p, s: (s, 0, 0, p))
    scores = samples * heads * 4 * nq * (nk + ctx_count)
    return pl.pallas_call(
        attention_kernel,
        grid=(pairs, samples),
        out_shape=jax.ShapeDtypeStruct(query.shape, jnp.bfloat16),
        in_specs=[
            pl.BlockSpec((1, 2, nk), lambda p, s: (p, 0, 0)),
            pl.BlockSpec(memory_space=pltpu.SMEM),
            own,
            token(0),
            token(pairs),
            far(0),
            far(pairs),
        ],
        out_specs=own,
        scratch_shapes=[pltpu.VMEM((2, 2, nq, nk), jnp.float32)],
        cost_estimate=pl.CostEstimate(
            flops=scores * 512, bytes_accessed=8 * query.size * 2, transcendentals=scores
        ),
    )(flat, ctx_bias, query, pair, pair, ctx_pair, ctx_pair)


def on_device(
    latent,
    context,
    cond,
    ctx_cond,
    w_shift,
    w_scale,
    w_gate,
    norm_gain,
    w_query,
    w_key,
    w_value,
    w_out,
    rel_bias,
    ctx_bias,
):
    samples = latent.shape[0]
    rows_sp = w_shift.shape[0]
    local_cols = w_shift.shape[1]
    sp_index = lax.axis_index("sp")
    ada = silu_rows(jnp.concatenate([cond, ctx_cond[None, :]], axis=0))
    ada_rows = lax.dynamic_slice_in_dim(ada, sp_index * rows_sp, rows_sp, 1)
    partial_value = jnp.stack(
        [
            jnp.dot(ada_rows, weight, preferred_element_type=jnp.float32)
            for weight in (w_shift, w_scale, w_gate)
        ]
    )
    summed = lax.psum(partial_value, "sp")
    modulation = lax.all_gather(summed, "tp", axis=2, tiled=True)
    hidden = modulate_rows(
        latent, norm_gain, modulation[0, :samples, None, :], modulation[1, :samples, None, :]
    )
    w_triple = jnp.concatenate([w_query, w_key, w_value], axis=1)
    triple = jnp.dot(
        lax.all_gather(hidden, "tp", axis=1, tiled=True),
        w_triple,
        preferred_element_type=jnp.float32,
    ).astype(jnp.bfloat16)
    ctx_hidden = modulate_rows(context, norm_gain, modulation[0, samples], modulation[1, samples])
    w_pair = jnp.concatenate([w_key, w_value], axis=1)
    own_pair = jnp.dot(ctx_hidden, w_pair, preferred_element_type=jnp.float32).astype(jnp.bfloat16)
    ctx_pair = lax.all_gather(own_pair, "sp", axis=1, tiled=True)
    heads = local_cols // HEAD_DIM
    tokens_sp = triple.shape[1]
    rows_dev = tokens_sp // GRID_W
    rows_all = rows_dev * lax.axis_size("sp")
    reach = WIN_ROWS // 2
    query = triple[..., :local_cols].reshape(samples, rows_dev, GRID_W, local_cols)
    pair = triple[..., local_cols:].reshape(samples, rows_dev, GRID_W, 2 * local_cols)
    padded_pair = extended(pair, (("sp", 1),), reach)
    mixed = attention(query, padded_pair, ctx_pair[None], rel_bias, ctx_bias)
    attended = mixed.reshape(samples, tokens_sp, local_cols)
    attended = attended.transpose(1, 0, 2)
    update = lax.psum_scatter(
        jnp.einsum("tsc,cd->tsd", attended, w_out, preferred_element_type=jnp.float32).astype(
            jnp.bfloat16
        ),
        "tp",
        scatter_dimension=0,
        tiled=True,
    ).astype(jnp.float32)
    gate = modulation[2, :samples, None, :]
    result = latent.astype(jnp.float32) + gate * update.transpose(1, 0, 2)
    return result.astype(jnp.bfloat16)


MESH = pl.DeviceIdType.MESH


def block_kernel(
    far_hbm, bias_hbm, gain_hbm, cond_hbm, ctx_cond_hbm,
    ws_ref, wc_ref, wg_ref, latent_ref, ctx_ref, wq_ref, wk_ref, wv_ref, wo_ref,
    out_ref,
    far_ref, bias_ref, gain_ref, cond_ref, ctx_cond_ref, acc,
    flat, ada, wm, part, got, total, full, buf, other, cx, cs, wq, wkv, wo, kv, qs, ckv, table,
    att, att_in, parts, y_in, fwd, x_in,
    own_sem, s1, r1, s2, r2, s_c, r_c, s_x, r_x, s_y, r_y, s_d, r_d, s_z, r_z, s_h, r_h,
    s_w, r_w, s_a, r_a, s_p, r_p, s_f, r_f,
):
    sp, tp = lax.axis_index("sp"), lax.axis_index("tp")
    n_sp, n_tp = lax.axis_size("sp"), lax.axis_size("tp")
    y, c = tp // 2, lax.rem(tp, 2)
    z, x = sp // 2, lax.rem(sp, 2)
    n_z = n_sp // 2
    same = x == y
    differs = x != y
    always = sp >= 0
    tokens, width = other.shape
    cols = wq.shape[1]
    rows_mod = wm.shape[1]
    lanes = 2 * HEAD_DIM
    pairs = cols // lanes
    half = WIN_COLS // 2
    reach = WIN_ROWS // 2
    own_rows = tokens // GRID_W
    group_rows = 2 * own_rows
    layer_rows = 4 * group_rows
    chunks = r_x.shape[0]
    per_row = chunks // own_rows
    size = tokens // chunks
    over_sp = [lax.rem(sp + k, n_sp) for k in range(1, n_sp)]
    over_tp = [lax.rem(tp + k, n_tp) for k in range(1, n_tp)]
    sib, across = (sp, tp + 1 - 2 * c), (sp, (1 - y) * 2 + c)
    beside = (sp + 1 - 2 * x, tp)
    g_own, g_x, g_y, g_d = 2 * x + y, 2 * (1 - x) + y, 2 * x + 1 - y, 2 * (1 - x) + 1 - y
    drain = []

    def remote(src, dst, s, r, device):
        return pltpu.make_async_remote_copy(
            src_ref=src, dst_ref=dst, send_sem=s, recv_sem=r, device_id=device, device_id_type=MESH
        )

    def begin(make, cond=None):
        drain.append((make, cond))
        if cond is None:
            make().start()
        else:
            @pl.when(cond)
            def _():
                make().start()

    def local(k, src, dst):
        copy = pltpu.make_async_copy(src, dst, own_sem.at[k])
        copy.start()
        return copy

    small_copies = [
        local(11 + k, src, dst)
        for k, (src, dst) in enumerate((
            (cond_hbm, cond_ref), (ctx_cond_hbm, ctx_cond_ref), (bias_hbm, bias_ref),
            (gain_hbm, gain_ref), (far_hbm, far_ref),
        ))
    ]
    mod_copies = [local(k, w, wm.at[k]) for k, w in enumerate((ws_ref, wc_ref, wg_ref))]
    other_copy = local(3, latent_ref.at[1 - x], other)
    own_copy = local(4, latent_ref.at[x], buf.at[2 * g_own + c])
    ctx_half = cs.shape[0]
    ctx_part = lambda k: pl.ds(pl.multiple_of(k * ctx_half, ctx_half), ctx_half)
    stage_copy = local(5, ctx_ref.at[1 - x, ctx_part(c)], cs)
    ctx_copy = local(6, ctx_ref.at[x], cx.at[x])
    weight_copies = [
        local(7, wk_ref, wkv.at[:, pl.ds(0, cols)]),
        local(8, wv_ref, wkv.at[:, pl.ds(cols, cols)]),
        local(9, wq_ref, wq),
        local(10, wo_ref, wo.at[0]),
    ]
    barrier = pltpu.get_barrier_semaphore()
    peers = [(p, tp) for p in over_sp] + [(sp, p) for p in over_tp]
    for device in peers:
        pl.semaphore_signal(barrier, inc=1, device_id=device, device_id_type=MESH)

    def piece(g, h):
        return buf.at[2 * g + c, pl.ds(pl.multiple_of(h * size, size), size)]

    def to_beside(h):
        return remote(other.at[pl.ds(h * size, size)], piece(g_own, h), s_x.at[0], r_x.at[h], beside)

    def from_beside(h):
        return remote(other.at[pl.ds(h * size, size)], piece(g_x, h), s_x.at[0], r_x.at[h], beside)

    def over_y(g, flow, h):
        return remote(piece(g, h), piece(g, h), s_y.at[flow], r_y.at[flow, h], across)

    def to_sib(k, g, h):
        return remote(piece(g, h), piece(g, h), s_d.at[k], r_d.at[k, h // per_row], sib)

    def from_sib(k, g, r):
        there = buf.at[2 * g + 1 - c, pl.ds(pl.multiple_of(GRID_W * r, GRID_W), GRID_W)]
        return remote(there, there, s_d.at[k], r_d.at[k, r], sib)

    def sent(ref, sem):
        drain.append((lambda: remote(ref, ref, sem, sem, sib), None))

    mine = pl.ds(pl.multiple_of(sp * rows_mod, rows_mod), rows_mod)
    small_copies[0].wait()
    small_copies[1].wait()
    ada[...] = jnp.zeros_like(ada)
    ada[0:2, :] = cond_ref[:, mine].astype(jnp.float32)
    ctx_cond = ctx_cond_ref[...].astype(jnp.float32)
    for k in range(n_sp):
        @pl.when(sp == k)
        def _():
            for j in range(rows_mod // 128):
                line = k * (rows_mod // 128) + j
                ada[2:3, 128 * j : 128 * (j + 1)] = ctx_cond[line : line + 1, :]
    values = ada[...]
    values = (values / (1.0 + jnp.exp(-values))).astype(jnp.bfloat16)
    at = 0
    for k, count in enumerate((3, 3, 2)):
        mod_copies[k].wait()
        value = jnp.dot(values, wm[k], preferred_element_type=jnp.float32)
        part[at : at + count, :] = value[:count]
        at += count
    stage_copy.wait()
    other_copy.wait()
    own_copy.wait()
    pl.semaphore_wait(barrier, len(peers))
    for k, peer in enumerate(over_sp):
        remote(part, got.at[k], s1.at[0], r1.at[0], (peer, tp)).start()
    sent(got, s1.at[0])

    begin(lambda: remote(cs, cx.at[x, ctx_part(c)], s_c.at[0], r_c.at[0], beside))
    upfront, between = 3 * chunks // 8, 5 * chunks // 8
    for h in range(chunks):
        if h < upfront:
            over_y(g_own, 0, h).start()
        to_beside(h).start()
    for h in range(chunks):
        to_sib(0, g_own, h).start()
    sent(other, s_x.at[0])
    for k in range(2):
        sent(other, s_y.at[k])
        sent(other, s_p.at[k])
    for k in range(4):
        sent(other, s_d.at[k])
    sent(fwd, s_f.at[0])

    span = 2 * WIN_COLS
    nk = table.shape[-1]
    nq = table.shape[-2] // 2
    rows_all = layer_rows * n_z
    lane = lax.broadcasted_iota(jnp.int32, (WIN_COLS, nk), 1)
    p = lax.broadcasted_iota(jnp.int32, (WIN_COLS, nk), 0)
    k_row, k_col = lane // span, lane % span
    inner = (k_col - p >= 0) & (k_col - p < WIN_COLS)
    edge = (p < half) == (k_col < WIN_COLS)

    small_copies[2].wait()
    flat[...] = jnp.zeros_like(flat)
    for k in range(bias_ref.shape[0]):
        flat[:, span * k : span * k + bias_ref.shape[2]] = bias_ref[k]

    def tables(pair, carry):
        for h in range(2):
            line = flat[pl.ds(2 * pair + h, 1), :]
            line = jnp.broadcast_to(line, (WIN_COLS, line.shape[1]))
            for r in range(group_rows):
                shift = (span * (r + reach - WIN_ROWS + 1) - half + 1) % line.shape[1]
                rolled = pltpu.roll(line, shift, 1, stride=1, stride_axis=0)[:, :nk] * LOG2E
                at_rows = pl.ds(h * nq + r * WIN_COLS, WIN_COLS)
                for kind in range(3):
                    row = z * layer_rows + r + (0, 0, layer_rows - group_rows)[kind]
                    first = row - reach
                    if kind:
                        first = jnp.clip(first, 0, rows_all - WIN_ROWS)
                    key_row = k_row + (row - r - reach)
                    inside = (key_row >= first) & (key_row < first + WIN_ROWS)
                    table[kind, pair, 0, at_rows, :] = jnp.where(inside & edge, rolled, -jnp.inf)
                    table[kind, pair, 1, at_rows, :] = jnp.where(inside & inner, rolled, -jnp.inf)
        return carry

    last_row = kv.shape[0] - 1
    kv[last_row] = jnp.zeros(kv.shape[1:], jnp.bfloat16)

    @pl.when(z == 0)
    def _():
        kv[0:reach] = jnp.zeros((reach,) + kv.shape[1:], jnp.bfloat16)

    @pl.when(z == n_z - 1)
    def _():
        kv[last_row - reach + 1 : last_row] = jnp.zeros((reach - 1,) + kv.shape[1:], jnp.bfloat16)

    lax.fori_loop(0, pairs // 2, tables, 0)

    value = part[...]
    remote(got, got, s1.at[0], r1.at[0], sib).wait_recv()
    for k in range(len(over_sp)):
        value = value + got[k]
    total[...] = value
    columns = pl.ds(pl.multiple_of(tp * cols, cols), cols)
    full[:, columns] = value
    for peer in over_tp:
        remote(total, full.at[:, columns], s2.at[0], r2.at[0], (sp, peer)).start()
    sent(got.at[pl.ds(0, len(over_tp))], s2.at[0])
    for h in range(upfront, between):
        over_y(g_own, 0, h).start()

    def rest_own():
        for h in range(between, chunks):
            over_y(g_own, 0, h).start()

    @pl.when(same)
    def _():
        rest_own()

    remote(cs, cx.at[1 - x, ctx_part(c)], s_c.at[0], r_c.at[0], beside).wait_recv()
    ctx_sib = lambda k: remote(
        cx.at[1 - x, ctx_part(k)], cx.at[1 - x, ctx_part(k)], s_c.at[1], r_c.at[1], sib
    )
    begin(lambda: ctx_sib(c))
    lax.fori_loop(pairs // 2, pairs, tables, 0)
    def relay(h):
        from_beside(h).wait_recv()
        over_y(g_x, 1, h).start()
        to_sib(1, g_x, h).start()

    relay(0)
    ctx_copy.wait()
    ctx_sib(1 - c).wait_recv()
    for copy in weight_copies + small_copies[3:]:
        copy.wait()
    several = got.at[pl.ds(0, len(over_tp))]
    remote(several, several, s2.at[0], r2.at[0], sib).wait_recv()
    begin(lambda: remote(wo.at[0], wo.at[1], s_w.at[0], r_w.at[0], sib))

    def normed(rows, which):
        rows = rows.astype(jnp.float32)
        inverse = lax.rsqrt(jnp.mean(rows * rows, axis=-1, keepdims=True) + EPSILON)
        lift = gain_ref[...] * (1.0 + full[pl.ds(3 + which, 1), :])
        return (rows * inverse * lift + full[pl.ds(which, 1), :]).astype(jnp.bfloat16)

    hidden = jnp.concatenate([normed(cx[0], 2), normed(cx[1], 2)], axis=0)
    ckv[z] = jnp.dot(hidden, wkv[...], preferred_element_type=jnp.float32).astype(jnp.bfloat16)

    def layer_copy(zb, k, up):
        return remote(ckv.at[zb], ckv.at[zb], s_z.at[k], r_z.at[zb], (sp + 2 * up, tp))

    layer_sends = []
    for k, up in enumerate((2, -2, 1, -1)):
        ahead = (z + up >= 0) & (z + up < n_z)
        middle = (z > 0) & (z + 1 < n_z - 1) if up > 0 else (z < n_z - 1) & (z - 1 > 0)
        layer_sends.append((functools.partial(layer_copy, z, k, up), ahead, middle))
        drain.append((functools.partial(layer_copy, z, k, up), ahead))

    def send_layer(late):
        for make, ahead, middle in layer_sends:
            @pl.when(ahead & (middle if late else jnp.logical_not(middle)))
            def _():
                make().start()

    send_layer(False)
    relay(1)
    far_up, far_down = z == n_z - 2, z == 1
    relays = far_up | far_down

    def ctx_relay():
        for cond, zb, k, up in ((far_up, 0, 4, 1), (far_down, n_z - 1, 5, -1)):
            @pl.when(cond)
            def _():
                layer_copy(zb, k, up).wait_recv()
                layer_copy(zb, k, up).start()

    drain.append((functools.partial(layer_copy, 0, 4, 1), far_up))
    drain.append((functools.partial(layer_copy, n_z - 1, 5, -1), far_down))

    g_third = jnp.where(same, g_d, g_y)
    g_fourth = jnp.where(same, g_y, g_d)
    has_up, has_down = z < n_z - 1, z > 0
    halo_up = lambda: remote(
        kv.at[pl.ds(layer_rows, reach)], kv.at[pl.ds(0, reach)], s_h.at[0], r_h.at[0], (sp + 2, tp)
    )
    halo_down = lambda: remote(
        kv.at[pl.ds(reach, reach - 1)], kv.at[pl.ds(reach + layer_rows, reach - 1)],
        s_h.at[1], r_h.at[1], (sp - 2, tp),
    )

    def incoming(k, flow, g, cond):
        @pl.when(cond)
        def _():
            for h in range(chunks):
                over_y(g, flow, h).wait_recv()
                to_sib(k, g, h).start()

    def shared(k, g, cond=always, rows=range(own_rows)):
        @pl.when(cond)
        def _():
            for r in rows:
                from_sib(k, g, r).wait_recv()

    def before(k):
        if k == 0:
            shared(0, g_own)
        if k == 1:
            for h in range(2, chunks):
                relay(h)
                if h == chunks - 2:
                    send_layer(True)

            @pl.when(differs)
            def _():
                rest_own()

            incoming(2, 0, g_y, differs)
            shared(1, g_x)
        if k == 2:
            ctx_relay()
            for critical, g in ((differs, g_x), (same, g_own)):
                @pl.when(relays & has_down & critical & (g == 0))
                def _():
                    halo_down().start()

                @pl.when(relays & has_up & critical & (g == 3))
                def _():
                    halo_up().start()

            incoming(3, 1, g_d, same)
            shared(2, g_y, differs)
            shared(3, g_d, same)

    def queries(hidden, count):
        query = jnp.dot(hidden, wq[...], preferred_element_type=jnp.float32)
        query = query.reshape(count, GRID_W, cols)
        query = jnp.concatenate([query[:, GRID_W - half :], query[:, : GRID_W - half]], axis=1)
        return query.astype(jnp.bfloat16)

    def project(i, carry):
        for k in range(3):
            @pl.when(i == k)
            def _():
                before(k)

        g = jnp.where(i == 0, g_own, jnp.where(i == 1, g_x, g_third))
        hidden = jnp.concatenate([normed(buf[2 * g + e], x) for e in range(2)], axis=0)
        value = jnp.dot(hidden, wkv[...], preferred_element_type=jnp.float32).astype(jnp.bfloat16)
        kv[pl.ds(reach + group_rows * g, group_rows)] = value.reshape(group_rows, GRID_W, 2 * cols)
        qs[pl.ds(group_rows * g, group_rows)] = queries(hidden, group_rows)
        open_now = jnp.logical_not(relays) | (i >= 2)

        @pl.when((g == 0) & has_down & open_now)
        def _():
            halo_down().start()

        @pl.when((g == 3) & has_up & open_now)
        def _():
            halo_up().start()

        return carry

    lax.fori_loop(0, 3, project, 0)

    def project_row(r, carry):
        incoming(2, 0, g_y, same & (r == 0))
        incoming(3, 1, g_d, differs & (r == 0))
        shared(2, g_y, same, [r])
        shared(3, g_d, differs, [r])
        at = pl.ds(pl.multiple_of(GRID_W * r, GRID_W), GRID_W)
        hidden = jnp.concatenate([normed(buf[2 * g_fourth + e, at], x) for e in range(2)], axis=0)
        value = jnp.dot(hidden, wkv[...], preferred_element_type=jnp.float32).astype(jnp.bfloat16)
        query = queries(hidden, 2)
        for e in range(2):
            row = group_rows * g_fourth + own_rows * e + r
            kv[reach + row] = value[GRID_W * e : GRID_W * (e + 1)]
            qs[row] = query[e]
        return carry

    lax.fori_loop(0, own_rows, project_row, 0)
    drain.append((halo_down, has_down))
    drain.append((halo_up, has_up))

    for k in range(1, n_z):
        zb = lax.rem(z + k, n_z)
        done = (far_up & (zb == 0)) | (far_down & (zb == n_z - 1))

        @pl.when(jnp.logical_not(done))
        def _():
            layer_copy(zb, 0, 1).wait_recv()

    remote(wo.at[0], wo.at[1], s_w.at[0], r_w.at[0], sib).wait_recv()

    factor = HEAD_DIM ** (-0.5) * LOG2E
    contract = (((1,), (1,)), ((), ()))
    low = lax.broadcasted_iota(jnp.int32, (nq, lanes), 1) < HEAD_DIM
    first_head = lax.broadcasted_iota(jnp.int32, (2 * nq, 1), 0) < nq
    key_rows = nk // span
    ctx_count = ckv.shape[0] * ckv.shape[1]

    def attend(i, g, pair, blocks):
        own = pl.ds(pl.multiple_of(pair * lanes, lanes), lanes)
        values_at = pl.ds(pl.multiple_of(cols + pair * lanes, lanes), lanes)
        rows = pl.ds(group_rows * g, key_rows)
        kind = jnp.where(g == 0, 1, jnp.where(g == 3, 2, 0))
        ck = ckv[:, :, own].reshape(ctx_count, lanes)
        cv = ckv[:, :, values_at].reshape(ctx_count, lanes)
        cv = jnp.concatenate([cv, jnp.ones((ctx_count, lanes), jnp.bfloat16)], axis=1)
        ones = jnp.ones((nk, lanes), jnp.bfloat16)
        lift = jnp.where(first_head, far_ref[2 * pair], far_ref[2 * pair + 1]) * LOG2E
        for b in blocks:
            q = qs[pl.ds(group_rows * g, group_rows), WIN_COLS * b : WIN_COLS * (b + 1), own]
            q = q.reshape(nq, lanes)
            zero = jnp.zeros_like(q)
            q = jnp.concatenate([jnp.where(low, q, zero), jnp.where(low, zero, q)], axis=0)

            def keys(part_at):
                if b == 0:
                    got = jnp.concatenate(
                        [kv[rows, GRID_W - WIN_COLS :, part_at], kv[rows, :WIN_COLS, part_at]], axis=1
                    )
                else:
                    got = kv[rows, WIN_COLS * (b - 1) : WIN_COLS * (b + 1), part_at]
                return got.reshape(nk, lanes)

            v = jnp.concatenate([keys(values_at), ones], axis=1)
            near = lax.dot_general(q, keys(own), contract, preferred_element_type=jnp.float32)
            near = near * factor + table[kind, pair, min(b, 1)]
            far = lax.dot_general(q, ck, contract, preferred_element_type=jnp.float32)
            top = jnp.maximum(
                jnp.max(near, axis=-1, keepdims=True),
                jnp.max(far, axis=-1, keepdims=True) * factor + lift,
            )
            near = jnp.exp2(near - top).astype(jnp.bfloat16)
            far = jnp.exp2(far * factor + (lift - top)).astype(jnp.bfloat16)
            summed = jnp.dot(near, v, preferred_element_type=jnp.float32) + jnp.dot(
                far, cv, preferred_element_type=jnp.float32
            )
            mean = summed[:, :lanes] / summed[:, lanes:]
            mean = jnp.where(low, mean[:nq], mean[nq:]).reshape(group_rows, WIN_COLS, lanes)
            att[i, :, WIN_COLS * b : WIN_COLS * (b + 1), own] = mean.astype(jnp.bfloat16)

    def give(i, batch, begins, count):
        at = pl.ds(begins, count)
        return remote(
            att.at[i, pl.ds(own_rows * (1 - c), own_rows), at], att_in.at[i, :, at],
            s_a.at[batch], r_a.at[batch], sib,
        )

    def to_across(i, slot, h):
        part_at = pl.ds(pl.multiple_of(h * size, size), size)
        return remote(
            parts.at[i, part_at], y_in.at[slot, part_at], s_p.at[slot], r_p.at[slot, h], across
        )

    def chunk(h):
        return pl.ds(pl.multiple_of(h * size, size), size)

    def to_owner(h):
        return remote(fwd.at[chunk(h)], x_in.at[chunk(h)], s_f.at[0], r_f.at[h], beside)

    def sum_at(i, slot, h):
        return parts[i, chunk(h)].astype(jnp.float32) + y_in[slot, chunk(h)].astype(jnp.float32)

    def forward(slot, h):
        to_across(slot, slot, h).wait_recv()
        fwd[chunk(h)] = sum_at(2, slot, h).astype(jnp.bfloat16)
        to_owner(h).start()

    def group_of(i):
        first = jnp.where(y == 0, 1, 2)
        return jnp.where(i == 0, first, jnp.where(i == 1, 3 * (1 - y), jnp.where(i == 2, g_x, g_own)))

    def attention_block(i, batch, begins, count, between_pairs=None, last_pieces=None):
        g = group_of(i)
        blocks = range(begins // WIN_COLS, (begins + count) // WIN_COLS)

        if between_pairs is None:
            for pair in range(pairs):
                attend(i, g, pair, blocks)
        else:
            def one(pair, carry):
                attend(i, g, pair, blocks)
                between_pairs(pair)
                return carry

            lax.fori_loop(0, pairs, one, 0)
        give(i, batch, begins, count).start()
        at = pl.ds(begins, count)
        acc[: own_rows * count] = jnp.dot(
            att[i, pl.ds(own_rows * c, own_rows), at].reshape(own_rows * count, cols), wo[0],
            preferred_element_type=jnp.float32,
        )
        if last_pieces is not None:
            last_pieces()
        give(i, batch, begins, count).wait_recv()
        update = acc[: own_rows * count] + jnp.dot(
            att_in[i, :, at].reshape(own_rows * count, cols), wo[1], preferred_element_type=jnp.float32
        )
        for r in range(own_rows):
            parts[i, GRID_W * r + begins : GRID_W * r + begins + count] = update[
                count * r : count * (r + 1)
            ].astype(jnp.bfloat16)

    for part_of in range(2):
        attention_block(0, part_of, GRID_W // 2 * part_of, GRID_W // 2)
        for r in range(own_rows):
            for k in range(per_row // 2):
                to_across(0, 0, per_row * r + per_row // 2 * part_of + k).start()

    def wait_halo(g):
        @pl.when((g == 0) & has_down)
        def _():
            there = kv.at[pl.ds(0, reach)]
            remote(there, there, s_h.at[0], r_h.at[0], (sp - 2, tp)).wait_recv()

        @pl.when((g == 3) & has_up)
        def _():
            there = kv.at[pl.ds(reach + layer_rows, reach - 1)]
            remote(there, there, s_h.at[1], r_h.at[1], (sp + 2, tp)).wait_recv()

    def attention_step(i, carry):
        g = group_of(i)

        wait_halo(g)
        attention_block(i, i + 1, 0, GRID_W)

        @pl.when(i == 1)
        def _():
            for h in range(chunks):
                to_across(1, 1, h).start()

        return carry

    lax.fori_loop(1, 3, attention_step, 0)
    early = chunks - 2 - pairs

    @pl.when(same)
    def _():
        for h in range(chunks):
            forward(0, h)

    @pl.when(differs)
    def _():
        for h in range(early):
            forward(1, h)

    def between_pairs(pair):
        @pl.when(differs)
        def _():
            forward(1, early + pair)

    def last_pieces():
        @pl.when(differs)
        def _():
            for h in range(early + pairs, chunks):
                forward(1, h)

    wait_halo(g_own)
    attention_block(3, 4, 0, GRID_W, between_pairs, last_pieces)
    for part_of in range(2):
        drain.append((functools.partial(give, 0, part_of, GRID_W // 2 * part_of, GRID_W // 2), None))
    for i in range(1, 4):
        drain.append((functools.partial(give, i, i + 1, 0, GRID_W), None))

    def finish(which, h, update):
        value = full[pl.ds(6 + which, 1), :] * update
        row, place = GRID_W * (h // per_row), size * (h % per_row)
        if place == 0:
            out_ref[which, row + GRID_W - half : row + GRID_W] = value[:half]
            out_ref[which, row : row + size - half] = value[half:]
        else:
            out_ref[which, row + place - half : row + place - half + size] = value

    def own(slot):
        for h in range(chunks):
            to_across(slot, slot, h).wait_recv()
            finish(x, h, sum_at(3, slot, h))

    @pl.when(differs)
    def _():
        own(0)

    @pl.when(same)
    def _():
        own(1)

    for h in range(chunks):
        to_owner(h).wait_recv()
        finish(1 - x, h, x_in[h * size : (h + 1) * size].astype(jnp.float32))

    for make, cond in drain:
        if cond is None:
            make().wait_send()
        else:
            @pl.when(cond)
            def _():
                make().wait_send()


def on_eight(
    latent, context, cond, ctx_cond, w_shift, w_scale, w_gate, norm_gain,
    w_query, w_key, w_value, w_out, rel_bias, ctx_bias,
):
    n_sp, n_tp = lax.axis_size("sp"), lax.axis_size("tp")
    samples, tokens, width = latent.shape
    ctx_tokens = context.shape[1]
    rows_mod, cols = w_shift.shape
    heads = cols // HEAD_DIM
    pairs = heads // 2
    n_z = n_sp // 2
    own_rows = tokens // GRID_W
    group_rows = 2 * own_rows
    layer_rows = 4 * group_rows
    key_rows = group_rows + WIN_ROWS
    nq, nk = group_rows * WIN_COLS, key_rows * 2 * WIN_COLS
    vmem, hbm = pl.BlockSpec(memory_space=pltpu.VMEM), pl.BlockSpec(memory_space=pltpu.HBM)
    dma = pltpu.SemaphoreType.DMA
    chunks = 8
    bf16, f32 = jnp.bfloat16, jnp.float32
    mods = (8, cols)
    delta = pl.pallas_call(
        block_kernel,
        out_shape=jax.ShapeDtypeStruct(latent.shape, f32),
        in_specs=[hbm] * 14,
        out_specs=vmem,
        scratch_shapes=[
            pltpu.SMEM(ctx_bias.shape, f32),
            pltpu.VMEM((rel_bias.shape[1], heads, rel_bias.shape[2]), f32),
            pltpu.VMEM((1, width), f32),
            pltpu.VMEM(cond.shape, bf16),
            pltpu.VMEM((width // 128, 128), bf16),
            pltpu.VMEM((tokens, width), f32),
            pltpu.VMEM((heads, 2 * WIN_ROWS * 2 * WIN_COLS), f32),
            pltpu.VMEM((8, rows_mod), f32),
            pltpu.VMEM((3, rows_mod, cols), bf16),
            pltpu.VMEM(mods, f32),
            pltpu.VMEM((n_sp - 1,) + mods, f32),
            pltpu.VMEM(mods, f32),
            pltpu.VMEM((8, width), f32),
            pltpu.VMEM((8, tokens, width), bf16),
            pltpu.VMEM((tokens, width), bf16),
            pltpu.VMEM((2, ctx_tokens, width), bf16),
            pltpu.VMEM((ctx_tokens // 2, width), bf16),
            pltpu.VMEM((width, cols), bf16),
            pltpu.VMEM((width, 2 * cols), bf16),
            pltpu.VMEM((2, cols, width), bf16),
            pltpu.VMEM((layer_rows + WIN_ROWS, GRID_W, 2 * cols), bf16),
            pltpu.VMEM((layer_rows, GRID_W, cols), bf16),
            pltpu.VMEM((n_z, 2 * ctx_tokens, 2 * cols), bf16),
            pltpu.VMEM((3, pairs, 2, 2 * nq, nk), f32),
            pltpu.VMEM((4, group_rows, GRID_W, cols), bf16),
            pltpu.VMEM((4, own_rows, GRID_W, cols), bf16),
            pltpu.VMEM((4, tokens, width), bf16),
            pltpu.VMEM((2, tokens, width), bf16),
            pltpu.VMEM((tokens, width), bf16),
            pltpu.VMEM((tokens, width), bf16),
            dma((16,)),
            dma((1,)), dma((1,)), dma((1,)), dma((1,)),
            dma((2,)), dma((2,)), dma((1,)), dma((chunks,)),
            dma((2,)), dma((2, chunks)), dma((4,)), dma((4, own_rows)),
            dma((6,)), dma((n_z,)), dma((2,)), dma((2,)),
            dma((1,)), dma((1,)), dma((5,)), dma((5,)),
            dma((2,)), dma((2, chunks)), dma((1,)), dma((chunks,)),
        ],
        compiler_params=pltpu.CompilerParams(
            collective_id=1, has_side_effects=True, vmem_limit_bytes=48 * 2**20
        ),
    )(
        *[
            pltpu.with_memory_space_constraint(v, pltpu.HBM)
            for v in (
                ctx_bias, rel_bias.transpose(1, 0, 2), norm_gain[None, :], cond, ctx_cond.reshape(-1, 128),
                w_shift, w_scale, w_gate, latent, context, w_query, w_key, w_value, w_out,
            )
        ]
    )
    return (latent.astype(f32) + delta).astype(bf16)


def solution(mesh):
    shape = dict(mesh.shape)
    quick = shape["tp"] == 4 and shape["sp"] == 8
    return jax.shard_map(
        on_eight if quick else on_device,
        mesh=mesh,
        in_specs=(
            P(None, ("sp", "tp"), None),
            P(None, "sp", None),
            P(),
            P(),
            P("sp", "tp"),
            P("sp", "tp"),
            P("sp", "tp"),
            P(),
            P(None, "tp"),
            P(None, "tp"),
            P(None, "tp"),
            P("tp", None),
            P("tp", None, None),
            P("tp"),
        ),
        out_specs=P(None, ("sp", "tp"), None),
        check_vma=False,
    )
```

```python
import functools

import jax
import jax.numpy as jnp
from jax import lax
from jax.experimental import pallas as pl
from jax.experimental.pallas import tpu as pltpu
from jax.sharding import PartitionSpec as P

HEAD_DIM = 64
GRID_W = 64
WIN_ROWS = 8
WIN_COLS = 16


EPSILON = 1e-06


def extended(shard, sides, width):
    for axis, dim in sides:
        size, length = (lax.axis_size(axis), shard.shape[dim])
        up = [(i, (i + 1) % size) for i in range(size - 1)]
        down = [(j, i) for i, j in up]
        last = lax.slice_in_dim(shard, length - width, length, axis=dim)
        first = lax.slice_in_dim(shard, 0, width, axis=dim)
        before = lax.ppermute(last, axis, up)
        after = lax.ppermute(first, axis, down)
        shard = jnp.concatenate([before, shard, after], axis=dim)
    return shard


def silu_rows(values):
    return jax.nn.silu(values.astype(jnp.float32)).astype(jnp.bfloat16)


def modulate_rows(rows, gain, shift, scale):
    floats = rows.astype(jnp.float32)
    inverse = lax.rsqrt(jnp.mean(floats * floats, axis=-1, keepdims=True) + EPSILON)
    return (floats * inverse * gain * (1.0 + scale) + shift).astype(jnp.bfloat16)

LOG2E = 1.4426950408889634


def attention_kernel(bias_ref, far_ref, q_ref, k_ref, v_ref, ck_ref, cv_ref, out_ref, table):
    pair = pl.program_id(0)
    rows_dev = q_ref.shape[1]
    padded = k_ref.shape[1]
    span = 2 * WIN_COLS
    half = WIN_COLS // 2
    reach = WIN_ROWS // 2
    nq, nk = rows_dev * WIN_COLS, padded * span
    lanes = 2 * HEAD_DIM

    @pl.when(pl.program_id(1) == 0)
    def _():
        sp = lax.axis_index("sp")
        rows_all = rows_dev * lax.axis_size("sp")
        at = lax.broadcasted_iota(jnp.int32, (WIN_COLS, nk), 1)
        p = lax.broadcasted_iota(jnp.int32, (WIN_COLS, nk), 0)
        key_row = sp * rows_dev - reach + at // span
        k = at % span
        inner = (k - p >= 0) & (k - p < WIN_COLS)
        edge = (p < half) == (k < WIN_COLS)
        for r in range(rows_dev):
            row = sp * rows_dev + r
            first = jnp.clip(row - reach, 0, rows_all - WIN_ROWS)
            inside = (key_row >= first) & (key_row < first + WIN_ROWS)
            shift = span * (r + reach - WIN_ROWS + 1) - half + 1
            for h in range(2):
                line = jnp.broadcast_to(bias_ref[0, h : h + 1, :], (WIN_COLS, nk))
                line = pltpu.roll(line, shift % nk, 1, stride=1, stride_axis=0) * LOG2E
                at_rows = pl.ds(r * WIN_COLS, WIN_COLS)
                table[h, 0, at_rows, :] = jnp.where(inside & edge, line, -jnp.inf)
                table[h, 1, at_rows, :] = jnp.where(inside & inner, line, -jnp.inf)

    factor = HEAD_DIM ** (-0.5) * LOG2E
    ck = ck_ref[...].reshape(-1, lanes)
    ctx_count = ck.shape[0]
    cv = jnp.concatenate([cv_ref[...].reshape(-1, lanes), jnp.ones((ctx_count, lanes), jnp.bfloat16)], axis=1)
    ones = jnp.ones((nk, lanes), jnp.bfloat16)
    low = lax.broadcasted_iota(jnp.int32, (nq, lanes), 1) < HEAD_DIM
    contract = (((1,), (1,)), ((), ()))
    every = q_ref[0].astype(jnp.float32)
    outs = []
    for block in range(GRID_W // WIN_COLS):
        if block == 0:
            q = jnp.concatenate([every[:, GRID_W - half :], every[:, :half]], axis=1)
        else:
            q = every[:, WIN_COLS * block - half : WIN_COLS * (block + 1) - half]
        q = q.astype(jnp.bfloat16).reshape(nq, lanes)

        def keys(ref):
            if block == 0:
                got = jnp.concatenate([ref[0, :, GRID_W - WIN_COLS :, :], ref[0, :, :WIN_COLS, :]], 1)
            else:
                got = ref[0, :, WIN_COLS * (block - 1) : WIN_COLS * (block + 1), :]
            return got.reshape(nk, lanes)

        k = keys(k_ref)
        v = jnp.concatenate([keys(v_ref), ones], axis=1)
        halves = []
        for h in range(2):
            mine = low if h == 0 else jnp.logical_not(low)
            one = jnp.where(mine, q, jnp.zeros_like(q))
            near = lax.dot_general(one, k, contract, preferred_element_type=jnp.float32)
            near = near * factor + table[h, min(block, 1)]
            far = lax.dot_general(one, ck, contract, preferred_element_type=jnp.float32)
            far = far * factor + far_ref[2 * pair + h] * LOG2E
            top = jnp.maximum(
                jnp.max(near, axis=-1, keepdims=True), jnp.max(far, axis=-1, keepdims=True)
            )
            near = jnp.exp2(near - top).astype(jnp.bfloat16)
            far = jnp.exp2(far - top).astype(jnp.bfloat16)
            got = jnp.dot(near, v, preferred_element_type=jnp.float32) + jnp.dot(
                far, cv, preferred_element_type=jnp.float32
            )
            halves.append(got[:, :lanes] / got[:, lanes:])
        outs.append(jnp.where(low, halves[0], halves[1]).reshape(rows_dev, WIN_COLS, lanes))
    outs = [outs[0][:, half:]] + outs[1:] + [outs[0][:, :half]]
    out_ref[0] = jnp.concatenate(outs, axis=1).astype(jnp.bfloat16)


def attention(query, pair, ctx_pair, rel_bias, ctx_bias):
    samples, rows_dev, _, cols = query.shape
    padded, ctx_count = pair.shape[1], ctx_pair.shape[0] * ctx_pair.shape[2]
    heads = cols // HEAD_DIM
    lanes = 2 * HEAD_DIM
    pairs = cols // lanes
    nq, nk = rows_dev * WIN_COLS, padded * 2 * WIN_COLS
    flat = jnp.pad(rel_bias, ((0, 0), (0, 1), (0, 1))).reshape(heads, -1)
    flat = jnp.pad(flat, ((0, 0), (0, nk - flat.shape[1]))).reshape(pairs, 2, nk)
    token = lambda at: pl.BlockSpec((1, padded, GRID_W, lanes), lambda p, s: (s, 0, 0, p + at))
    far = lambda at: pl.BlockSpec(
        (ctx_pair.shape[0], 1, ctx_pair.shape[2], lanes), lambda p, s: (0, s, 0, p + at)
    )
    own = pl.BlockSpec((1, rows_dev, GRID_W, lanes), lambda p, s: (s, 0, 0, p))
    scores = samples * heads * 4 * nq * (nk + ctx_count)
    return pl.pallas_call(
        attention_kernel,
        grid=(pairs, samples),
        out_shape=jax.ShapeDtypeStruct(query.shape, jnp.bfloat16),
        in_specs=[
            pl.BlockSpec((1, 2, nk), lambda p, s: (p, 0, 0)),
            pl.BlockSpec(memory_space=pltpu.SMEM),
            own,
            token(0),
            token(pairs),
            far(0),
            far(pairs),
        ],
        out_specs=own,
        scratch_shapes=[pltpu.VMEM((2, 2, nq, nk), jnp.float32)],
        cost_estimate=pl.CostEstimate(
            flops=scores * 512, bytes_accessed=8 * query.size * 2, transcendentals=scores
        ),
    )(flat, ctx_bias, query, pair, pair, ctx_pair, ctx_pair)


def on_device(
    latent,
    context,
    cond,
    ctx_cond,
    w_shift,
    w_scale,
    w_gate,
    norm_gain,
    w_query,
    w_key,
    w_value,
    w_out,
    rel_bias,
    ctx_bias,
):
    samples = latent.shape[0]
    rows_sp = w_shift.shape[0]
    local_cols = w_shift.shape[1]
    sp_index = lax.axis_index("sp")
    ada = silu_rows(jnp.concatenate([cond, ctx_cond[None, :]], axis=0))
    ada_rows = lax.dynamic_slice_in_dim(ada, sp_index * rows_sp, rows_sp, 1)
    partial_value = jnp.stack(
        [
            jnp.dot(ada_rows, weight, preferred_element_type=jnp.float32)
            for weight in (w_shift, w_scale, w_gate)
        ]
    )
    summed = lax.psum(partial_value, "sp")
    modulation = lax.all_gather(summed, "tp", axis=2, tiled=True)
    hidden = modulate_rows(
        latent, norm_gain, modulation[0, :samples, None, :], modulation[1, :samples, None, :]
    )
    w_triple = jnp.concatenate([w_query, w_key, w_value], axis=1)
    triple = jnp.dot(
        lax.all_gather(hidden, "tp", axis=1, tiled=True),
        w_triple,
        preferred_element_type=jnp.float32,
    ).astype(jnp.bfloat16)
    ctx_hidden = modulate_rows(context, norm_gain, modulation[0, samples], modulation[1, samples])
    w_pair = jnp.concatenate([w_key, w_value], axis=1)
    own_pair = jnp.dot(ctx_hidden, w_pair, preferred_element_type=jnp.float32).astype(jnp.bfloat16)
    ctx_pair = lax.all_gather(own_pair, "sp", axis=1, tiled=True)
    heads = local_cols // HEAD_DIM
    tokens_sp = triple.shape[1]
    rows_dev = tokens_sp // GRID_W
    rows_all = rows_dev * lax.axis_size("sp")
    reach = WIN_ROWS // 2
    query = triple[..., :local_cols].reshape(samples, rows_dev, GRID_W, local_cols)
    pair = triple[..., local_cols:].reshape(samples, rows_dev, GRID_W, 2 * local_cols)
    padded_pair = extended(pair, (("sp", 1),), reach)
    mixed = attention(query, padded_pair, ctx_pair[None], rel_bias, ctx_bias)
    attended = mixed.reshape(samples, tokens_sp, local_cols)
    attended = attended.transpose(1, 0, 2)
    update = lax.psum_scatter(
        jnp.einsum("tsc,cd->tsd", attended, w_out, preferred_element_type=jnp.float32).astype(
            jnp.bfloat16
        ),
        "tp",
        scatter_dimension=0,
        tiled=True,
    ).astype(jnp.float32)
    gate = modulation[2, :samples, None, :]
    result = latent.astype(jnp.float32) + gate * update.transpose(1, 0, 2)
    return result.astype(jnp.bfloat16)


MESH = pl.DeviceIdType.MESH


def block_kernel(
    far_hbm, bias_hbm, gain_hbm, cond_hbm, ctx_cond_hbm,
    ws_ref, wc_ref, wg_ref, latent_ref, ctx_ref, wq_ref, wk_ref, wv_ref, wo_ref,
    out_ref,
    far_ref, bias_ref, gain_ref, cond_ref, ctx_cond_ref, acc,
    flat, ada, wm, part, got, total, full, buf, other, cx, cs, wq, wkv, wo, kv, qs, ckv, table,
    att, att_in, parts, y_in, fwd, x_in,
    own_sem, s1, r1, s2, r2, s_c, r_c, s_x, r_x, s_y, r_y, s_d, r_d, s_z, r_z, s_h, r_h,
    s_w, r_w, s_a, r_a, s_p, r_p, s_f, r_f,
):
    sp, tp = lax.axis_index("sp"), lax.axis_index("tp")
    n_sp, n_tp = lax.axis_size("sp"), lax.axis_size("tp")
    y, c = tp // 2, lax.rem(tp, 2)
    z, x = sp // 2, lax.rem(sp, 2)
    n_z = n_sp // 2
    same = x == y
    differs = x != y
    always = sp >= 0
    tokens, width = other.shape
    cols = wq.shape[1]
    rows_mod = wm.shape[1]
    lanes = 2 * HEAD_DIM
    pairs = cols // lanes
    half = WIN_COLS // 2
    reach = WIN_ROWS // 2
    own_rows = tokens // GRID_W
    group_rows = 2 * own_rows
    layer_rows = 4 * group_rows
    chunks = r_x.shape[0]
    per_row = chunks // own_rows
    size = tokens // chunks
    over_sp = [lax.rem(sp + k, n_sp) for k in range(1, n_sp)]
    over_tp = [lax.rem(tp + k, n_tp) for k in range(1, n_tp)]
    sib, across = (sp, tp + 1 - 2 * c), (sp, (1 - y) * 2 + c)
    beside = (sp + 1 - 2 * x, tp)
    g_own, g_x, g_y, g_d = 2 * x + y, 2 * (1 - x) + y, 2 * x + 1 - y, 2 * (1 - x) + 1 - y
    drain = []

    def remote(src, dst, s, r, device):
        return pltpu.make_async_remote_copy(
            src_ref=src, dst_ref=dst, send_sem=s, recv_sem=r, device_id=device, device_id_type=MESH
        )

    def begin(make, cond=None):
        drain.append((make, cond))
        if cond is None:
            make().start()
        else:
            @pl.when(cond)
            def _():
                make().start()

    def local(k, src, dst):
        copy = pltpu.make_async_copy(src, dst, own_sem.at[k])
        copy.start()
        return copy

    small_copies = [
        local(11 + k, src, dst)
        for k, (src, dst) in enumerate((
            (cond_hbm, cond_ref), (ctx_cond_hbm, ctx_cond_ref), (bias_hbm, bias_ref),
            (gain_hbm, gain_ref), (far_hbm, far_ref),
        ))
    ]
    mod_copies = [local(k, w, wm.at[k]) for k, w in enumerate((ws_ref, wc_ref, wg_ref))]
    other_copy = local(3, latent_ref.at[1 - x], other)
    own_copy = local(4, latent_ref.at[x], buf.at[2 * g_own + c])
    ctx_half = cs.shape[0]
    ctx_part = lambda k: pl.ds(pl.multiple_of(k * ctx_half, ctx_half), ctx_half)
    stage_copy = local(5, ctx_ref.at[1 - x, ctx_part(c)], cs)
    ctx_copy = local(6, ctx_ref.at[x], cx.at[x])
    weight_copies = [
        local(7, wk_ref, wkv.at[:, pl.ds(0, cols)]),
        local(8, wv_ref, wkv.at[:, pl.ds(cols, cols)]),
        local(9, wq_ref, wq),
        local(10, wo_ref, wo.at[0]),
    ]
    barrier = pltpu.get_barrier_semaphore()
    peers = [(p, tp) for p in over_sp] + [(sp, p) for p in over_tp]
    for device in peers:
        pl.semaphore_signal(barrier, inc=1, device_id=device, device_id_type=MESH)

    def piece(g, h):
        return buf.at[2 * g + c, pl.ds(pl.multiple_of(h * size, size), size)]

    def to_beside(h):
        return remote(other.at[pl.ds(h * size, size)], piece(g_own, h), s_x.at[0], r_x.at[h], beside)

    def from_beside(h):
        return remote(other.at[pl.ds(h * size, size)], piece(g_x, h), s_x.at[0], r_x.at[h], beside)

    def over_y(g, flow, h):
        return remote(piece(g, h), piece(g, h), s_y.at[flow], r_y.at[flow, h], across)

    def to_sib(k, g, h):
        return remote(piece(g, h), piece(g, h), s_d.at[k], r_d.at[k, h // per_row], sib)

    def from_sib(k, g, r):
        there = buf.at[2 * g + 1 - c, pl.ds(pl.multiple_of(GRID_W * r, GRID_W), GRID_W)]
        return remote(there, there, s_d.at[k], r_d.at[k, r], sib)

    def sent(ref, sem):
        drain.append((lambda: remote(ref, ref, sem, sem, sib), None))

    mine = pl.ds(pl.multiple_of(sp * rows_mod, rows_mod), rows_mod)
    small_copies[0].wait()
    small_copies[1].wait()
    ada[...] = jnp.zeros_like(ada)
    ada[0:2, :] = cond_ref[:, mine].astype(jnp.float32)
    ctx_cond = ctx_cond_ref[...].astype(jnp.float32)
    for k in range(n_sp):
        @pl.when(sp == k)
        def _():
            for j in range(rows_mod // 128):
                line = k * (rows_mod // 128) + j
                ada[2:3, 128 * j : 128 * (j + 1)] = ctx_cond[line : line + 1, :]
    values = ada[...]
    values = (values / (1.0 + jnp.exp(-values))).astype(jnp.bfloat16)
    at = 0
    for k, count in enumerate((3, 3, 2)):
        mod_copies[k].wait()
        value = jnp.dot(values, wm[k], preferred_element_type=jnp.float32)
        part[at : at + count, :] = value[:count]
        at += count
    stage_copy.wait()
    other_copy.wait()
    own_copy.wait()
    pl.semaphore_wait(barrier, len(peers))
    for k, peer in enumerate(over_sp):
        remote(part, got.at[k], s1.at[0], r1.at[0], (peer, tp)).start()
    sent(got, s1.at[0])

    begin(lambda: remote(cs, cx.at[x, ctx_part(c)], s_c.at[0], r_c.at[0], beside))
    upfront, between = 3 * chunks // 8, 5 * chunks // 8
    for h in range(chunks):
        if h < upfront:
            over_y(g_own, 0, h).start()
        to_beside(h).start()
    for h in range(chunks):
        to_sib(0, g_own, h).start()
    sent(other, s_x.at[0])
    for k in range(2):
        sent(other, s_y.at[k])
        sent(other, s_p.at[k])
    for k in range(4):
        sent(other, s_d.at[k])
    sent(fwd, s_f.at[0])

    span = 2 * WIN_COLS
    nk = table.shape[-1]
    nq = table.shape[-2] // 2
    rows_all = layer_rows * n_z
    lane = lax.broadcasted_iota(jnp.int32, (WIN_COLS, nk), 1)
    p = lax.broadcasted_iota(jnp.int32, (WIN_COLS, nk), 0)
    k_row, k_col = lane // span, lane % span
    inner = (k_col - p >= 0) & (k_col - p < WIN_COLS)
    edge = (p < half) == (k_col < WIN_COLS)

    small_copies[2].wait()
    flat[...] = jnp.zeros_like(flat)
    for k in range(bias_ref.shape[0]):
        flat[:, span * k : span * k + bias_ref.shape[2]] = bias_ref[k]

    def tables(pair, carry):
        for h in range(2):
            line = flat[pl.ds(2 * pair + h, 1), :]
            line = jnp.broadcast_to(line, (WIN_COLS, line.shape[1]))
            for r in range(group_rows):
                shift = (span * (r + reach - WIN_ROWS + 1) - half + 1) % line.shape[1]
                rolled = pltpu.roll(line, shift, 1, stride=1, stride_axis=0)[:, :nk] * LOG2E
                at_rows = pl.ds(h * nq + r * WIN_COLS, WIN_COLS)
                for kind in range(3):
                    row = z * layer_rows + r + (0, 0, layer_rows - group_rows)[kind]
                    first = row - reach
                    if kind:
                        first = jnp.clip(first, 0, rows_all - WIN_ROWS)
                    key_row = k_row + (row - r - reach)
                    inside = (key_row >= first) & (key_row < first + WIN_ROWS)
                    table[kind, pair, 0, at_rows, :] = jnp.where(inside & edge, rolled, -jnp.inf)
                    table[kind, pair, 1, at_rows, :] = jnp.where(inside & inner, rolled, -jnp.inf)
        return carry

    last_row = kv.shape[0] - 1
    kv[last_row] = jnp.zeros(kv.shape[1:], jnp.bfloat16)

    @pl.when(z == 0)
    def _():
        kv[0:reach] = jnp.zeros((reach,) + kv.shape[1:], jnp.bfloat16)

    @pl.when(z == n_z - 1)
    def _():
        kv[last_row - reach + 1 : last_row] = jnp.zeros((reach - 1,) + kv.shape[1:], jnp.bfloat16)

    lax.fori_loop(0, pairs // 2, tables, 0)

    value = part[...]
    remote(got, got, s1.at[0], r1.at[0], sib).wait_recv()
    for k in range(len(over_sp)):
        value = value + got[k]
    total[...] = value
    columns = pl.ds(pl.multiple_of(tp * cols, cols), cols)
    full[:, columns] = value
    for peer in over_tp:
        remote(total, full.at[:, columns], s2.at[0], r2.at[0], (sp, peer)).start()
    sent(got.at[pl.ds(0, len(over_tp))], s2.at[0])
    for h in range(upfront, between):
        over_y(g_own, 0, h).start()

    def rest_own():
        for h in range(between, chunks):
            over_y(g_own, 0, h).start()

    @pl.when(same)
    def _():
        rest_own()

    remote(cs, cx.at[1 - x, ctx_part(c)], s_c.at[0], r_c.at[0], beside).wait_recv()
    ctx_sib = lambda k: remote(
        cx.at[1 - x, ctx_part(k)], cx.at[1 - x, ctx_part(k)], s_c.at[1], r_c.at[1], sib
    )
    begin(lambda: ctx_sib(c))
    lax.fori_loop(pairs // 2, pairs, tables, 0)
    def relay(h):
        from_beside(h).wait_recv()
        over_y(g_x, 1, h).start()
        to_sib(1, g_x, h).start()

    ctx_copy.wait()
    ctx_sib(1 - c).wait_recv()
    for copy in weight_copies + small_copies[3:]:
        copy.wait()
    several = got.at[pl.ds(0, len(over_tp))]
    remote(several, several, s2.at[0], r2.at[0], sib).wait_recv()
    begin(lambda: remote(wo.at[0], wo.at[1], s_w.at[0], r_w.at[0], sib))

    def normed(rows, which):
        rows = rows.astype(jnp.float32)
        inverse = lax.rsqrt(jnp.mean(rows * rows, axis=-1, keepdims=True) + EPSILON)
        lift = gain_ref[...] * (1.0 + full[pl.ds(3 + which, 1), :])
        return (rows * inverse * lift + full[pl.ds(which, 1), :]).astype(jnp.bfloat16)

    hidden = jnp.concatenate([normed(cx[0], 2), normed(cx[1], 2)], axis=0)
    ckv[z] = jnp.dot(hidden, wkv[...], preferred_element_type=jnp.float32).astype(jnp.bfloat16)

    def layer_copy(zb, k, up):
        return remote(ckv.at[zb], ckv.at[zb], s_z.at[k], r_z.at[zb], (sp + 2 * up, tp))

    layer_sends = []
    for k, up in enumerate((2, -2, 1, -1)):
        ahead = (z + up >= 0) & (z + up < n_z)
        middle = (z > 0) & (z + 1 < n_z - 1) if up > 0 else (z < n_z - 1) & (z - 1 > 0)
        layer_sends.append((functools.partial(layer_copy, z, k, up), ahead, middle))
        drain.append((functools.partial(layer_copy, z, k, up), ahead))

    def send_layer(late):
        for make, ahead, middle in layer_sends:
            @pl.when(ahead & (middle if late else jnp.logical_not(middle)))
            def _():
                make().start()

    send_layer(False)
    relay(0)
    relay(1)
    far_up, far_down = z == n_z - 2, z == 1
    relays = far_up | far_down

    def ctx_relay():
        for cond, zb, k, up in ((far_up, 0, 4, 1), (far_down, n_z - 1, 5, -1)):
            @pl.when(cond)
            def _():
                layer_copy(zb, k, up).wait_recv()
                layer_copy(zb, k, up).start()

    drain.append((functools.partial(layer_copy, 0, 4, 1), far_up))
    drain.append((functools.partial(layer_copy, n_z - 1, 5, -1), far_down))

    g_third = jnp.where(same, g_d, g_y)
    g_fourth = jnp.where(same, g_y, g_d)
    has_up, has_down = z < n_z - 1, z > 0
    halo_up = lambda: remote(
        kv.at[pl.ds(layer_rows, reach)], kv.at[pl.ds(0, reach)], s_h.at[0], r_h.at[0], (sp + 2, tp)
    )
    halo_down = lambda: remote(
        kv.at[pl.ds(reach, reach - 1)], kv.at[pl.ds(reach + layer_rows, reach - 1)],
        s_h.at[1], r_h.at[1], (sp - 2, tp),
    )

    def incoming(k, flow, g, cond):
        @pl.when(cond)
        def _():
            for h in range(chunks):
                over_y(g, flow, h).wait_recv()
                to_sib(k, g, h).start()

    def shared(k, g, cond=always, rows=range(own_rows)):
        @pl.when(cond)
        def _():
            for r in rows:
                from_sib(k, g, r).wait_recv()

    def before(k):
        if k == 0:
            shared(0, g_own)
        if k == 1:
            for h in range(2, chunks):
                relay(h)
                if h == chunks - 2:
                    send_layer(True)

            @pl.when(differs)
            def _():
                rest_own()

            incoming(2, 0, g_y, differs)
            shared(1, g_x)
        if k == 2:
            ctx_relay()
            for critical, g in ((differs, g_x), (same, g_own)):
                @pl.when(relays & has_down & critical & (g == 0))
                def _():
                    halo_down().start()

                @pl.when(relays & has_up & critical & (g == 3))
                def _():
                    halo_up().start()

            incoming(3, 1, g_d, same)
            shared(2, g_y, differs)
            shared(3, g_d, same)

    def queries(hidden, count):
        query = jnp.dot(hidden, wq[...], preferred_element_type=jnp.float32)
        query = query.reshape(count, GRID_W, cols)
        query = jnp.concatenate([query[:, GRID_W - half :], query[:, : GRID_W - half]], axis=1)
        return query.astype(jnp.bfloat16)

    def project(i, carry):
        for k in range(3):
            @pl.when(i == k)
            def _():
                before(k)

        g = jnp.where(i == 0, g_own, jnp.where(i == 1, g_x, g_third))
        hidden = jnp.concatenate([normed(buf[2 * g + e], x) for e in range(2)], axis=0)
        value = jnp.dot(hidden, wkv[...], preferred_element_type=jnp.float32).astype(jnp.bfloat16)
        kv[pl.ds(reach + group_rows * g, group_rows)] = value.reshape(group_rows, GRID_W, 2 * cols)
        qs[pl.ds(group_rows * g, group_rows)] = queries(hidden, group_rows)
        open_now = jnp.logical_not(relays) | (i >= 2)

        @pl.when((g == 0) & has_down & open_now)
        def _():
            halo_down().start()

        @pl.when((g == 3) & has_up & open_now)
        def _():
            halo_up().start()

        return carry

    lax.fori_loop(0, 3, project, 0)

    def project_row(r, carry):
        incoming(2, 0, g_y, same & (r == 0))
        incoming(3, 1, g_d, differs & (r == 0))
        shared(2, g_y, same, [r])
        shared(3, g_d, differs, [r])
        at = pl.ds(pl.multiple_of(GRID_W * r, GRID_W), GRID_W)
        hidden = jnp.concatenate([normed(buf[2 * g_fourth + e, at], x) for e in range(2)], axis=0)
        value = jnp.dot(hidden, wkv[...], preferred_element_type=jnp.float32).astype(jnp.bfloat16)
        query = queries(hidden, 2)
        for e in range(2):
            row = group_rows * g_fourth + own_rows * e + r
            kv[reach + row] = value[GRID_W * e : GRID_W * (e + 1)]
            qs[row] = query[e]
        return carry

    lax.fori_loop(0, own_rows, project_row, 0)
    drain.append((halo_down, has_down))
    drain.append((halo_up, has_up))

    for k in range(1, n_z):
        zb = lax.rem(z + k, n_z)
        done = (far_up & (zb == 0)) | (far_down & (zb == n_z - 1))

        @pl.when(jnp.logical_not(done))
        def _():
            layer_copy(zb, 0, 1).wait_recv()

    remote(wo.at[0], wo.at[1], s_w.at[0], r_w.at[0], sib).wait_recv()

    factor = HEAD_DIM ** (-0.5) * LOG2E
    contract = (((1,), (1,)), ((), ()))
    low = lax.broadcasted_iota(jnp.int32, (nq, lanes), 1) < HEAD_DIM
    first_head = lax.broadcasted_iota(jnp.int32, (2 * nq, 1), 0) < nq
    key_rows = nk // span
    ctx_count = ckv.shape[0] * ckv.shape[1]

    def attend(i, g, pair, blocks):
        own = pl.ds(pl.multiple_of(pair * lanes, lanes), lanes)
        values_at = pl.ds(pl.multiple_of(cols + pair * lanes, lanes), lanes)
        rows = pl.ds(group_rows * g, key_rows)
        kind = jnp.where(g == 0, 1, jnp.where(g == 3, 2, 0))
        ck = ckv[:, :, own].reshape(ctx_count, lanes)
        cv = ckv[:, :, values_at].reshape(ctx_count, lanes)
        cv = jnp.concatenate([cv, jnp.ones((ctx_count, lanes), jnp.bfloat16)], axis=1)
        ones = jnp.ones((nk, lanes), jnp.bfloat16)
        lift = jnp.where(first_head, far_ref[2 * pair], far_ref[2 * pair + 1]) * LOG2E
        for b in blocks:
            q = qs[pl.ds(group_rows * g, group_rows), WIN_COLS * b : WIN_COLS * (b + 1), own]
            q = q.reshape(nq, lanes)
            zero = jnp.zeros_like(q)
            q = jnp.concatenate([jnp.where(low, q, zero), jnp.where(low, zero, q)], axis=0)

            def keys(part_at):
                if b == 0:
                    got = jnp.concatenate(
                        [kv[rows, GRID_W - WIN_COLS :, part_at], kv[rows, :WIN_COLS, part_at]], axis=1
                    )
                else:
                    got = kv[rows, WIN_COLS * (b - 1) : WIN_COLS * (b + 1), part_at]
                return got.reshape(nk, lanes)

            v = jnp.concatenate([keys(values_at), ones], axis=1)
            near = lax.dot_general(q, keys(own), contract, preferred_element_type=jnp.float32)
            near = near * factor + table[kind, pair, min(b, 1)]
            far = lax.dot_general(q, ck, contract, preferred_element_type=jnp.float32)
            top = jnp.maximum(
                jnp.max(near, axis=-1, keepdims=True),
                jnp.max(far, axis=-1, keepdims=True) * factor + lift,
            )
            near = jnp.exp2(near - top).astype(jnp.bfloat16)
            far = jnp.exp2(far * factor + (lift - top)).astype(jnp.bfloat16)
            summed = jnp.dot(near, v, preferred_element_type=jnp.float32) + jnp.dot(
                far, cv, preferred_element_type=jnp.float32
            )
            mean = summed[:, :lanes] / summed[:, lanes:]
            mean = jnp.where(low, mean[:nq], mean[nq:]).reshape(group_rows, WIN_COLS, lanes)
            att[i, :, WIN_COLS * b : WIN_COLS * (b + 1), own] = mean.astype(jnp.bfloat16)

    def give(i, batch, begins, count):
        at = pl.ds(begins, count)
        return remote(
            att.at[i, pl.ds(own_rows * (1 - c), own_rows), at], att_in.at[i, :, at],
            s_a.at[batch], r_a.at[batch], sib,
        )

    def to_across(i, slot, h):
        part_at = pl.ds(pl.multiple_of(h * size, size), size)
        return remote(
            parts.at[i, part_at], y_in.at[slot, part_at], s_p.at[slot], r_p.at[slot, h], across
        )

    def chunk(h):
        return pl.ds(pl.multiple_of(h * size, size), size)

    def to_owner(h):
        return remote(fwd.at[chunk(h)], x_in.at[chunk(h)], s_f.at[0], r_f.at[h], beside)

    def sum_at(i, slot, h):
        return parts[i, chunk(h)].astype(jnp.float32) + y_in[slot, chunk(h)].astype(jnp.float32)

    def forward(slot, h):
        to_across(slot, slot, h).wait_recv()
        fwd[chunk(h)] = sum_at(2, slot, h).astype(jnp.bfloat16)
        to_owner(h).start()

    def group_of(i):
        first = jnp.where(y == 0, 1, 2)
        return jnp.where(i == 0, first, jnp.where(i == 1, 3 * (1 - y), jnp.where(i == 2, g_x, g_own)))

    def attention_block(i, batch, begins, count, between_pairs=None, last_pieces=None):
        g = group_of(i)
        blocks = range(begins // WIN_COLS, (begins + count) // WIN_COLS)

        if between_pairs is None:
            for pair in range(pairs):
                attend(i, g, pair, blocks)
        else:
            def one(pair, carry):
                attend(i, g, pair, blocks)
                between_pairs(pair)
                return carry

            lax.fori_loop(0, pairs, one, 0)
        give(i, batch, begins, count).start()
        at = pl.ds(begins, count)
        acc[: own_rows * count] = jnp.dot(
            att[i, pl.ds(own_rows * c, own_rows), at].reshape(own_rows * count, cols), wo[0],
            preferred_element_type=jnp.float32,
        )
        if last_pieces is not None:
            last_pieces()
        give(i, batch, begins, count).wait_recv()
        update = acc[: own_rows * count] + jnp.dot(
            att_in[i, :, at].reshape(own_rows * count, cols), wo[1], preferred_element_type=jnp.float32
        )
        for r in range(own_rows):
            parts[i, GRID_W * r + begins : GRID_W * r + begins + count] = update[
                count * r : count * (r + 1)
            ].astype(jnp.bfloat16)

    for part_of in range(2):
        attention_block(0, part_of, GRID_W // 2 * part_of, GRID_W // 2)
        for r in range(own_rows):
            for k in range(per_row // 2):
                to_across(0, 0, per_row * r + per_row // 2 * part_of + k).start()

    def wait_halo(g):
        @pl.when((g == 0) & has_down)
        def _():
            there = kv.at[pl.ds(0, reach)]
            remote(there, there, s_h.at[0], r_h.at[0], (sp - 2, tp)).wait_recv()

        @pl.when((g == 3) & has_up)
        def _():
            there = kv.at[pl.ds(reach + layer_rows, reach - 1)]
            remote(there, there, s_h.at[1], r_h.at[1], (sp + 2, tp)).wait_recv()

    def attention_step(i, carry):
        g = group_of(i)

        wait_halo(g)
        attention_block(i, i + 1, 0, GRID_W)

        @pl.when(i == 1)
        def _():
            for h in range(chunks):
                to_across(1, 1, h).start()

        return carry

    lax.fori_loop(1, 3, attention_step, 0)
    early = chunks - 2 - pairs

    @pl.when(same)
    def _():
        for h in range(chunks):
            forward(0, h)

    @pl.when(differs)
    def _():
        for h in range(early):
            forward(1, h)

    def between_pairs(pair):
        @pl.when(differs)
        def _():
            forward(1, early + pair)

    def last_pieces():
        @pl.when(differs)
        def _():
            for h in range(early + pairs, chunks):
                forward(1, h)

    wait_halo(g_own)
    attention_block(3, 4, 0, GRID_W, between_pairs, last_pieces)
    for part_of in range(2):
        drain.append((functools.partial(give, 0, part_of, GRID_W // 2 * part_of, GRID_W // 2), None))
    for i in range(1, 4):
        drain.append((functools.partial(give, i, i + 1, 0, GRID_W), None))

    def finish(which, h, update):
        value = full[pl.ds(6 + which, 1), :] * update
        row, place = GRID_W * (h // per_row), size * (h % per_row)
        if place == 0:
            out_ref[which, row + GRID_W - half : row + GRID_W] = value[:half]
            out_ref[which, row : row + size - half] = value[half:]
        else:
            out_ref[which, row + place - half : row + place - half + size] = value

    def own(slot):
        for h in range(chunks):
            to_across(slot, slot, h).wait_recv()
            finish(x, h, sum_at(3, slot, h))

    @pl.when(differs)
    def _():
        own(0)

    @pl.when(same)
    def _():
        own(1)

    for h in range(chunks):
        to_owner(h).wait_recv()
        finish(1 - x, h, x_in[h * size : (h + 1) * size].astype(jnp.float32))

    for make, cond in drain:
        if cond is None:
            make().wait_send()
        else:
            @pl.when(cond)
            def _():
                make().wait_send()


def on_eight(
    latent, context, cond, ctx_cond, w_shift, w_scale, w_gate, norm_gain,
    w_query, w_key, w_value, w_out, rel_bias, ctx_bias,
):
    n_sp, n_tp = lax.axis_size("sp"), lax.axis_size("tp")
    samples, tokens, width = latent.shape
    ctx_tokens = context.shape[1]
    rows_mod, cols = w_shift.shape
    heads = cols // HEAD_DIM
    pairs = heads // 2
    n_z = n_sp // 2
    own_rows = tokens // GRID_W
    group_rows = 2 * own_rows
    layer_rows = 4 * group_rows
    key_rows = group_rows + WIN_ROWS
    nq, nk = group_rows * WIN_COLS, key_rows * 2 * WIN_COLS
    vmem, hbm = pl.BlockSpec(memory_space=pltpu.VMEM), pl.BlockSpec(memory_space=pltpu.HBM)
    dma = pltpu.SemaphoreType.DMA
    chunks = 8
    bf16, f32 = jnp.bfloat16, jnp.float32
    mods = (8, cols)
    delta = pl.pallas_call(
        block_kernel,
        out_shape=jax.ShapeDtypeStruct(latent.shape, f32),
        in_specs=[hbm] * 14,
        out_specs=vmem,
        scratch_shapes=[
            pltpu.SMEM(ctx_bias.shape, f32),
            pltpu.VMEM((rel_bias.shape[1], heads, rel_bias.shape[2]), f32),
            pltpu.VMEM((1, width), f32),
            pltpu.VMEM(cond.shape, bf16),
            pltpu.VMEM((width // 128, 128), bf16),
            pltpu.VMEM((tokens, width), f32),
            pltpu.VMEM((heads, 2 * WIN_ROWS * 2 * WIN_COLS), f32),
            pltpu.VMEM((8, rows_mod), f32),
            pltpu.VMEM((3, rows_mod, cols), bf16),
            pltpu.VMEM(mods, f32),
            pltpu.VMEM((n_sp - 1,) + mods, f32),
            pltpu.VMEM(mods, f32),
            pltpu.VMEM((8, width), f32),
            pltpu.VMEM((8, tokens, width), bf16),
            pltpu.VMEM((tokens, width), bf16),
            pltpu.VMEM((2, ctx_tokens, width), bf16),
            pltpu.VMEM((ctx_tokens // 2, width), bf16),
            pltpu.VMEM((width, cols), bf16),
            pltpu.VMEM((width, 2 * cols), bf16),
            pltpu.VMEM((2, cols, width), bf16),
            pltpu.VMEM((layer_rows + WIN_ROWS, GRID_W, 2 * cols), bf16),
            pltpu.VMEM((layer_rows, GRID_W, cols), bf16),
            pltpu.VMEM((n_z, 2 * ctx_tokens, 2 * cols), bf16),
            pltpu.VMEM((3, pairs, 2, 2 * nq, nk), f32),
            pltpu.VMEM((4, group_rows, GRID_W, cols), bf16),
            pltpu.VMEM((4, own_rows, GRID_W, cols), bf16),
            pltpu.VMEM((4, tokens, width), bf16),
            pltpu.VMEM((2, tokens, width), bf16),
            pltpu.VMEM((tokens, width), bf16),
            pltpu.VMEM((tokens, width), bf16),
            dma((16,)),
            dma((1,)), dma((1,)), dma((1,)), dma((1,)),
            dma((2,)), dma((2,)), dma((1,)), dma((chunks,)),
            dma((2,)), dma((2, chunks)), dma((4,)), dma((4, own_rows)),
            dma((6,)), dma((n_z,)), dma((2,)), dma((2,)),
            dma((1,)), dma((1,)), dma((5,)), dma((5,)),
            dma((2,)), dma((2, chunks)), dma((1,)), dma((chunks,)),
        ],
        compiler_params=pltpu.CompilerParams(
            collective_id=1, has_side_effects=True, vmem_limit_bytes=48 * 2**20
        ),
    )(
        *[
            pltpu.with_memory_space_constraint(v, pltpu.HBM)
            for v in (
                ctx_bias, rel_bias.transpose(1, 0, 2), norm_gain[None, :], cond, ctx_cond.reshape(-1, 128),
                w_shift, w_scale, w_gate, latent, context, w_query, w_key, w_value, w_out,
            )
        ]
    )
    return (latent.astype(f32) + delta).astype(bf16)


def solution(mesh):
    shape = dict(mesh.shape)
    quick = shape["tp"] == 4 and shape["sp"] == 8
    return jax.shard_map(
        on_eight if quick else on_device,
        mesh=mesh,
        in_specs=(
            P(None, ("sp", "tp"), None),
            P(None, "sp", None),
            P(),
            P(),
            P("sp", "tp"),
            P("sp", "tp"),
            P("sp", "tp"),
            P(),
            P(None, "tp"),
            P(None, "tp"),
            P(None, "tp"),
            P("tp", None),
            P("tp", None, None),
            P("tp"),
        ),
        out_specs=P(None, ("sp", "tp"), None),
        check_vma=False,
    )
```
